32 devices in a mesh: ep: 8 (over z, x), tp: 4 (over y, core).
Axes of the slice: x: 2, y: 2, z: 4, core: 2. Of those that a mesh axis runs over, the one named last changes fastest.
Arguments:
- queries: bfloat16 [8192, 512], P('ep', 'tp'), may hold values from -6 to 6
- head_key_rows: bfloat16 [8192, 512], P('ep', 'tp'), may hold values from -6 to 6
- head_value_rows: bfloat16 [8192, 1024], P('ep', 'tp'), may hold values from -18 to 18
- log_input_gate: float32 [8192, 8], P('ep', 'tp'), may hold values from -6 to 120
- forget_logits: float32 [8192, 8], P('ep', 'tp'), may hold values from -8 to 8
- head_forget_bias: float32 [8], P('tp'), may hold values from 3 to 20
- extra_log_forget: float32 [8192, 8], P('ep', 'tp'), may hold values from -1 to 0
- output_gate_logits: bfloat16 [8192, 1024], P('ep', 'tp'), may hold values from -6 to 6
- head_norm_gain: float32 [1024], P('tp'), may hold values from 0.1 to 1.9
- mixer_output_weight: bfloat16 [1024, 2048], replicated, may hold values from -0.1875 to 0.1875
- second_batch_input: bfloat16 [6144, 2048], P(('ep', 'tp')), may hold values from -6 to 6
- expert_norm_gain: float32 [2048], replicated, may hold values from 0.1 to 1.9
- routed_expert_index: int32 [6144, 2], P(('ep', 'tp')), may hold values from 0 to 31, all different within a row; in each aligned block of 192 rows (0 to 191, 192 to 383, ...) at most 18 rows name the same one
- routed_copy_weight: float32 [6144, 2], P(('ep', 'tp')), may hold values from 0.3 to 1.5
- routed_gate_weight: bfloat16 [32, 2048, 1024], P(('ep', 'tp')), may hold values from -0.125 to 0.125
- routed_up_weight: bfloat16 [32, 2048, 1024], P(('ep', 'tp')), may hold values from -0.125 to 0.125
- routed_down_weight: bfloat16 [32, 1024, 2048], P(('ep', 'tp')), may hold values from -0.1875 to 0.1875
- shared_gate_weight: bfloat16 [2048, 384], replicated, may hold values from -0.125 to 0.125
- shared_up_weight: bfloat16 [2048, 384], replicated, may hold values from -0.125 to 0.125
- shared_down_weight: bfloat16 [384, 2048], replicated, may hold values from -0.3125 to 0.3125
Outputs:
- mixer_first_output: bfloat16 [8192, 2048], P(('ep', 'tp'))
- moe_out: bfloat16 [6144, 2048], P(('ep', 'tp'))
The draws below stay inside these ranges and needn't reach their ends.
Inputs may be any that keep to these rules, and one draw needn't show every extreme that they name: `routed_expert_index`: in each aligned block of 192 rows (the rows of one device) no expert is named by more than 18 rows, and in some blocks one expert is named by exactly 18; every expert is named somewhere.
All inputs are finite; a program needn't handle non-finite values.
Results may differ from the reference program's by a relative error of at most 0.0068.
Values may be sent and summed in bfloat16 or wider, within the bound.
A program may use at most 128 MiB of HBM per device.

```python
import math
from functools import partial
import jax
import jax.numpy as jnp
import numpy as np
from jax import lax

D = 2048
HEADS = 8
DK = 64
DV = 128
BLK = 128
TOPK = 2
FE = 1024
FS = 384
MOE_DEV = 192
EXPERTS = 32
TOK1 = 8192
TOK2 = 6144
CAP = 18


def draw_head_value_rows(key, part):
    key_base = jax.random.fold_in(key, 15)
    head_of_column = jnp.arange(HEADS * DV, dtype=jnp.int32) // DV
    fraction = head_of_column.astype(jnp.float32) / (HEADS - 1)
    base = jnp.clip(jax.random.normal(key_base, (TOK1, HEADS * DV), jnp.float32), -6.0, 6.0)
    column_scale = jnp.exp(fraction * jnp.log(3.0))
    return (base * column_scale[None, :]).astype(jnp.bfloat16)


def draw_head_forget_bias(key, part):
    key_order, key_slow, key_fast = jax.random.split(jax.random.fold_in(key, 11), 3)
    slow_count = HEADS // 2
    ranking = jax.random.permutation(key_order, HEADS)
    is_slow = ranking < slow_count
    slow_rate = jnp.exp(jax.random.uniform(key_slow, (HEADS,), jnp.float32, jnp.log(0.3), jnp.log(1.0))) / TOK1
    fast_rate = jnp.exp(jax.random.uniform(key_fast, (HEADS,), jnp.float32, jnp.log(1.0 / 100.0), jnp.log(1.0 / 30.0)))
    return -jnp.log(jnp.where(is_slow, slow_rate, fast_rate)).astype(jnp.float32)


def draw_forget_logits(key, part):
    key_base, key_offset = jax.random.split(jax.random.fold_in(key, 12), 2)
    base = jnp.clip(jax.random.normal(key_base, (TOK1, HEADS), jnp.float32), -6.0, 6.0)
    offsets = jax.random.uniform(key_offset, (64, HEADS), jnp.float32, -0.7, 0.7)
    return (base + jnp.repeat(offsets, TOK1 // 64, axis=0)).astype(jnp.float32)


def draw_extra_log_forget(key, part):
    key_place, key_value = jax.random.split(jax.random.fold_in(key, 13), 2)
    places = jax.random.randint(key_place, (4, HEADS), 0, TOK1)
    values = jnp.log(jax.random.uniform(key_value, (4, HEADS), jnp.float32, 0.5, 0.8))
    columns = jnp.broadcast_to(jnp.arange(HEADS, dtype=jnp.int32)[None, :], (4, HEADS))
    return jnp.zeros((TOK1, HEADS), jnp.float32).at[places, columns].set(values)


def draw_log_input_gate(key, part):
    key_base = jax.random.fold_in(jax.random.fold_in(key, 14), 0)
    return jnp.clip(jax.random.normal(key_base, (TOK1, HEADS), jnp.float32), -6.0, 6.0)


def steps_of(stream_key, extent, pieces, smallest, top_value):
    def one(axis_at, parts):
        steps = jax.random.uniform(jax.random.fold_in(jax.random.fold_in(stream_key, 6), axis_at), (parts,), jnp.float32, smallest / len(pieces), top_value / len(pieces))
        return jnp.repeat(jnp.exp(steps), extent[axis_at] // parts).reshape((-1,) + (1,) * (len(extent) - axis_at - 1))

    loudness = one(*pieces[0])
    for cut in pieces[1:]:
        loudness = loudness * one(*cut)
    return loudness


def assign_block(own_key, own, number, rows, amount, top, limit, lean):
    order = jax.random.permutation(own_key, amount)
    packed, common = load_shares(amount, rows * top, limit, lean, True), load_shares(amount, rows * top, limit, lean, False)
    places = jnp.arange(amount)

    def named(tallies, turn):
        used = int((tallies > 0).sum())
        fixed = max(1, used // 4)
        passed = fixed + (places - fixed + turn * (used - fixed)) % max(1, amount - fixed)
        return jnp.zeros((amount,), jnp.int32).at[order[jnp.where(places < fixed, places, passed)]].set(jnp.asarray(tallies, jnp.int32))

    tallies = jnp.where(number % 4 == 0, named(packed, number // 4), named(common, number - number // 4 - 1))
    mixed = jax.random.permutation(jax.random.fold_in(own, 3), amount)
    giver, sink = mixed[0:amount // 2 * 2:2], mixed[1:amount // 2 * 2:2]
    margin = jnp.minimum(tallies[giver] - 1, limit - tallies[sink]) // 2
    margin = jnp.where((giver == order[0]) | (sink == order[0]) | (tallies[sink] == 0), 0, jnp.maximum(margin, 0))
    passed = jax.random.randint(jax.random.fold_in(own, 4), (amount // 2,), 0, 1 << 20) % (margin + 1)
    tallies = tallies.at[giver].add(-passed).at[sink].add(passed)
    labels = jnp.searchsorted(jnp.cumsum(tallies), jnp.arange(rows * top), side="right").astype(jnp.int32)
    table = labels.reshape(top, rows).T
    table = table[jax.random.permutation(jax.random.fold_in(own, 1), rows)]
    turn = jax.random.randint(jax.random.fold_in(own, 2), (rows, 1), 0, top)
    return jnp.take_along_axis(table, (jnp.arange(top)[None, :] + turn) % top, axis=1)


def load_shares(amount, total, reach, lean, full):
    loads = [(1 << 20) // math.isqrt(grade ** lean) + 1 for grade in range(1, amount + 1)]
    largest = reach if full else min(reach, max(-(-total // amount), total * loads[0] // sum(loads)))
    least = 1 if total - largest >= amount - 1 else 0
    given, spare = [largest] + [least] * (amount - 1), total - largest - least * (amount - 1)
    while spare > 0:
        free = [i for i in range(1, amount) if given[i] < largest] or [i for i in range(1, amount) if given[i] < reach]
        mass, left = sum([loads[i] for i in free]), spare
        for i in free:
            addition = min(reach - given[i], max(1, left * loads[i] // mass), spare)
            given[i] = given[i] + addition
            spare = spare - addition
    return np.array(given)


def scatter_about(own_key, shape, width, reach, cuts=(), kind=jnp.bfloat16):
    level = steps_of(own_key, shape, cuts, -0.22, 0.18) if cuts else 1.0
    values = jax.random.normal(own_key, shape, jnp.float32) * width * level
    return jnp.minimum(jnp.maximum(values, -reach), reach).astype(kind)


def setup_inputs(seed: int = 0) -> dict:
    seeds = jax.random.split(jax.random.key(seed), 21)
    queries = scatter_about(seeds[0], (TOK1, HEADS * DK), 1.0, 6.0, ((0, 8), (1, 4)))
    head_key_rows = scatter_about(seeds[1], (TOK1, HEADS * DK), 1.0, 6.0, ((0, 8), (1, 4)))
    head_value_rows = draw_head_value_rows(jax.random.fold_in(seeds[20], 71), 0)
    log_input_gate = draw_log_input_gate(jax.random.fold_in(seeds[20], 71), 0)
    forget_logits = draw_forget_logits(jax.random.fold_in(seeds[20], 71), 0)
    head_forget_bias = draw_head_forget_bias(jax.random.fold_in(seeds[20], 71), 0)
    extra_log_forget = draw_extra_log_forget(jax.random.fold_in(seeds[20], 71), 0)
    output_gate_logits = scatter_about(seeds[7], (TOK1, HEADS * DV), 1.0, 6.0, ((0, 8), (1, 4)))
    head_norm_gain = jnp.clip(1.0 + 0.18 * jax.random.normal(seeds[8], (HEADS * DV,), jnp.float32), 0.1, 1.9)
    mixer_output_weight = scatter_about(seeds[9], (HEADS * DV, D), (HEADS * DV) ** -0.5, 0.1875)
    second_batch_input = scatter_about(seeds[10], (TOK2, D), 1.0, 6.0, ((0, 32),))
    expert_norm_gain = jnp.clip(1.0 + 0.18 * jax.random.normal(seeds[11], (D,), jnp.float32), 0.1, 1.9)
    routed_expert_index_keys = jax.random.split(jax.random.fold_in(seeds[12], 1), TOK2 // MOE_DEV)
    routed_expert_index_turns = jax.random.permutation(jax.random.fold_in(seeds[12], 3), TOK2 // MOE_DEV)
    routed_expert_index = jax.vmap(lambda own, number: assign_block(jax.random.fold_in(seeds[12], 2), own, number, MOE_DEV, EXPERTS, TOPK, CAP, 1))(routed_expert_index_keys, routed_expert_index_turns).reshape((TOK2, TOPK))
    routed_copy_weight = jnp.clip(jnp.exp(math.log(1.5) - 1.60943787 * jax.random.uniform(seeds[13], (TOK2, TOPK), jnp.float32) ** steps_of(seeds[13], (TOK2, TOPK), ((0, 32),), -0.2, 0.2)), 0.3, 1.5)
    routed_gate_weight = scatter_about(seeds[14], (EXPERTS, D, FE), D ** -0.5, 0.125, ((0, 32),))
    routed_up_weight = scatter_about(seeds[15], (EXPERTS, D, FE), D ** -0.5, 0.125, ((0, 32),))
    routed_down_weight = scatter_about(seeds[16], (EXPERTS, FE, D), FE ** -0.5, 0.1875, ((0, 32),))
    shared_gate_weight = scatter_about(seeds[17], (D, FS), D ** -0.5, 0.125)
    shared_up_weight = scatter_about(seeds[18], (D, FS), D ** -0.5, 0.125)
    shared_down_weight = scatter_about(seeds[19], (FS, D), FS ** -0.5, 0.3125)
    return {"queries": queries, "head_key_rows": head_key_rows, "head_value_rows": head_value_rows, "log_input_gate": log_input_gate, "forget_logits": forget_logits, "head_forget_bias": head_forget_bias, "extra_log_forget": extra_log_forget, "output_gate_logits": output_gate_logits, "head_norm_gain": head_norm_gain, "mixer_output_weight": mixer_output_weight, "second_batch_input": second_batch_input, "expert_norm_gain": expert_norm_gain, "routed_expert_index": routed_expert_index, "routed_copy_weight": routed_copy_weight, "routed_gate_weight": routed_gate_weight, "routed_up_weight": routed_up_weight, "routed_down_weight": routed_down_weight, "shared_gate_weight": shared_gate_weight, "shared_up_weight": shared_up_weight, "shared_down_weight": shared_down_weight}


exact_einsum = partial(jnp.einsum, precision=lax.Precision.HIGHEST)

def memory_step(carry, inputs):
    memory, normalizer, running_max = carry
    query_block, key_block, value_block, in_block, forget_block = inputs
    cumulative = jnp.cumsum(forget_block, axis=-1)
    lower = jnp.tril(jnp.ones((BLK, BLK), dtype=bool))
    pair_gap = jnp.where(lower, cumulative[:, :, None] - cumulative[:, None, :] + in_block[:, None, :], -jnp.inf)
    carried = cumulative + running_max[:, None]
    stabilizer = jnp.maximum(carried, lax.optimization_barrier(jnp.max(pair_gap, axis=-1)))
    local_weight = jnp.exp(pair_gap - stabilizer[..., None])
    carry_weight = jnp.exp(carried - stabilizer)
    scores = exact_einsum('htd,hsd->hts', query_block, key_block) * local_weight
    numerator = carry_weight[..., None] * exact_einsum('htd,hde->hte', query_block, memory) + exact_einsum('hts,hse->hte', scores, value_block)
    denominator = carry_weight * exact_einsum('htd,hd->ht', query_block, normalizer) + lax.optimization_barrier(jnp.sum(scores, axis=-1))
    hidden = numerator / jnp.maximum(jnp.abs(denominator), jnp.exp(-stabilizer))[..., None]
    block_total = cumulative[:, -1]
    key_gap = block_total[:, None] - cumulative + in_block
    new_max = jnp.maximum(block_total + running_max, lax.optimization_barrier(jnp.max(key_gap, axis=-1)))
    decay_factor = jnp.exp(block_total + running_max - new_max)
    weighted_keys = jnp.exp(key_gap - new_max[:, None])[..., None] * key_block
    memory = decay_factor[:, None, None] * memory + exact_einsum('hsd,hse->hde', weighted_keys, value_block)
    normalizer = decay_factor[:, None] * normalizer + lax.optimization_barrier(jnp.sum(weighted_keys, axis=1))
    return ((memory, normalizer, new_max), hidden)

def mixer_portion(queries, head_key_rows, head_value_rows, log_input_gate, forget_logits, head_forget_bias, extra_log_forget, output_gate_logits, head_norm_gain, mixer_output_weight):
    positions = queries.shape[0]
    block_count = positions // BLK

    def to_blocks(array, size):
        return array.astype(jnp.float32).reshape(block_count, BLK, HEADS, size).transpose(0, 2, 1, 3)

    def gate_block_list(array):
        return array.reshape(block_count, BLK, HEADS).transpose(0, 2, 1)
    query_blocks = to_blocks(queries, DK) * DK ** (-0.5)
    key_blocks = to_blocks(head_key_rows, DK)
    value_blocks = to_blocks(head_value_rows, DV)
    forget_log_value = jax.nn.log_sigmoid(forget_logits + head_forget_bias[None, :]) + extra_log_forget
    start = (jnp.zeros((HEADS, DK, DV), jnp.float32), jnp.zeros((HEADS, DK), jnp.float32), jnp.zeros((HEADS,), jnp.float32))
    _, hidden = lax.scan(memory_step, start, (query_blocks, key_blocks, value_blocks, gate_block_list(log_input_gate), gate_block_list(forget_log_value)))
    hidden = hidden.transpose(0, 2, 1, 3).reshape(positions, HEADS, DV)
    scaled = hidden * lax.rsqrt(lax.optimization_barrier(jnp.mean(hidden * hidden, axis=(1, 2), keepdims=True)) + 1e-06)
    scaled = scaled * head_norm_gain.reshape(HEADS, DV)
    gated = scaled * jax.nn.sigmoid(output_gate_logits.astype(jnp.float32).reshape(positions, HEADS, DV))
    mixed = gated.reshape(positions, HEADS * DV).astype(jnp.bfloat16)
    return jnp.dot(mixed, mixer_output_weight, preferred_element_type=jnp.float32).astype(jnp.bfloat16)

def expert_part(second_batch_input, expert_norm_gain, routed_expert_index, routed_copy_weight, routed_gate_weight, routed_up_weight, routed_down_weight, shared_gate_weight, shared_up_weight, shared_down_weight):
    token_count = second_batch_input.shape[0]
    floats = second_batch_input.astype(jnp.float32)
    normed = (floats * lax.rsqrt(lax.optimization_barrier(jnp.mean(floats * floats, axis=-1, keepdims=True)) + 1e-06) * expert_norm_gain).astype(jnp.bfloat16)
    block_count = token_count // MOE_DEV
    expert_list = routed_expert_index.reshape(block_count, MOE_DEV * TOPK)
    one_hot = (expert_list[..., None] == jnp.arange(EXPERTS, dtype=jnp.int32)).astype(jnp.int32)
    position = lax.optimization_barrier(jnp.sum((jnp.cumsum(one_hot, axis=1) - one_hot) * one_hot, axis=-1))
    slot_index = expert_list * (block_count * CAP) + jnp.arange(block_count, dtype=jnp.int32)[:, None] * CAP + position
    slot_flat = slot_index.reshape(-1)
    slot_table = jnp.full((EXPERTS * block_count * CAP,), token_count, jnp.int32)
    slot_table = slot_table.at[slot_flat].set(jnp.arange(token_count * TOPK, dtype=jnp.int32) // TOPK)
    padded = jnp.concatenate([normed, jnp.zeros((1, D), jnp.bfloat16)], axis=0)

    def one_expert(operands):
        table_row, gate_weight, up_weight, down_weight = operands
        row_block = padded[table_row]
        gate_vals = jnp.dot(row_block, gate_weight, preferred_element_type=jnp.float32)
        up_vals = jnp.dot(row_block, up_weight, preferred_element_type=jnp.float32)
        hidden = (jax.nn.silu(gate_vals) * up_vals).astype(jnp.bfloat16)
        return jnp.dot(hidden, down_weight, preferred_element_type=jnp.float32).astype(jnp.bfloat16)
    results = lax.map(one_expert, (slot_table.reshape(EXPERTS, block_count * CAP), routed_gate_weight, routed_up_weight, routed_down_weight))
    results = results.reshape(EXPERTS * block_count * CAP, D)
    slot_pairs = slot_flat.reshape(token_count, TOPK)
    routed = jnp.zeros((token_count, D), jnp.float32)
    for copy_index in range(TOPK):
        routed = routed + routed_copy_weight[:, copy_index:copy_index + 1] * results[slot_pairs[:, copy_index]].astype(jnp.float32)
    shared_hidden = (jax.nn.silu(jnp.dot(normed, shared_gate_weight, preferred_element_type=jnp.float32)) * jnp.dot(normed, shared_up_weight, preferred_element_type=jnp.float32)).astype(jnp.bfloat16)
    shared = jnp.dot(shared_hidden, shared_down_weight, preferred_element_type=jnp.float32)
    return (routed + shared).astype(jnp.bfloat16)

def reference(queries, head_key_rows, head_value_rows, log_input_gate, forget_logits, head_forget_bias, extra_log_forget, output_gate_logits, head_norm_gain, mixer_output_weight, second_batch_input, expert_norm_gain, routed_expert_index, routed_copy_weight, routed_gate_weight, routed_up_weight, routed_down_weight, shared_gate_weight, shared_up_weight, shared_down_weight):
    mixer_first_output = mixer_portion(queries, head_key_rows, head_value_rows, log_input_gate, forget_logits, head_forget_bias, extra_log_forget, output_gate_logits, head_norm_gain, mixer_output_weight)
    moe_out = expert_part(second_batch_input, expert_norm_gain, routed_expert_index, routed_copy_weight, routed_gate_weight, routed_up_weight, routed_down_weight, shared_gate_weight, shared_up_weight, shared_down_weight)
    return (mixer_first_output, moe_out)
```

```python
import jax
import jax.numpy as jnp
from jax import lax
from jax.experimental import pallas as pl
from jax.experimental.pallas import tpu as pltpu
from jax.sharding import PartitionSpec as P

BLK = 128


F32 = jnp.float32
BF16 = jnp.bfloat16
LANE_ROWS = 16
CORES = 2
PIECES = 2


def mm(left, right):
    return jnp.dot(left, right, preferred_element_type=F32)


def iota(shape, axis):
    return lax.broadcasted_iota(jnp.int32, shape, axis)


class Place:
    def __init__(self, ep_count, tp_count):
        self.side = max(1, tp_count // CORES)
        self.tp_count = tp_count
        self.planes = ep_count // self.side
        self.depth = self.planes // 2
        self.cell = self.side * tp_count
        self.near = self.depth * self.cell
        self.ep_at = lax.axis_index("ep")
        self.tp_at = lax.axis_index("tp")
        plane = self.ep_at // self.side
        self.row = lax.rem(self.ep_at, self.side)
        self.half = plane // self.depth
        self.level = plane - self.half * self.depth
        self.stage = self.half * self.level + (1 - self.half) * (self.depth - 1 - self.level)
        self.spot = self.level * self.cell + self.row * tp_count + self.tp_at
        self.partner = ((self.planes - 1 - plane) * self.side + self.row, self.tp_at)

    def at(self, level, row, tp):
        device = ((self.half * self.depth + level) * self.side + row, tp)
        return device, level * self.cell + row * self.tp_count + tp

    def across(self, step, sign):
        row_step, tp_step = step // self.tp_count, lax.rem(step, self.tp_count)
        row = lax.rem(self.row + sign * row_step + self.side, self.side)
        tp = lax.rem(self.tp_at + sign * tp_step + self.tp_count, self.tp_count)
        return row, tp

    def away(self, distance, sign):
        level_step = distance // self.cell
        level = lax.rem(self.level + sign * level_step + self.depth, self.depth)
        return self.at(level, *self.across(lax.rem(distance, self.cell), sign))

    def level_of(self, stage):
        return self.half * stage + (1 - self.half) * (self.depth - 1 - stage)


def each(low, high, work):
    def turn(step, carry):
        work(step)
        return carry

    lax.fori_loop(low, high, turn, 0)


def rows_of(index):
    return pl.ds(pl.multiple_of(index * LANE_ROWS, LANE_ROWS), LANE_ROWS)


def remote(source, target, send_sem, recv_sem, device):
    return pltpu.make_async_remote_copy(
        src_ref=source, dst_ref=target, send_sem=send_sem, recv_sem=recv_sem,
        device_id=device, device_id_type=pl.DeviceIdType.MESH,
    )


def as_weight(mask):
    return mask.astype(F32).astype(BF16)


class Experts:
    def __init__(self, place, capacity, refs):
        (self.x_ref, self.gain_ref, self.idx_ref, self.weight_ref, wg_hbm, wu_hbm, wd_hbm, sg_hbm,
         su_hbm, sd_hbm, self.out_ref, self.normed, self.meta, self.far_block, self.far_meta,
         self.send_own, self.send_far, self.recv, self.ysend, self.ret_own, self.ret_far,
         self.far_out, self.far_in, self.wg, self.wu, self.wd, self.sg, self.su, self.sd, self.xc,
         self.hc, self.yc, self.total, load_sem, self.go_send, self.go_recv, self.back_send,
         self.back_recv, self.over_send, self.over_recv) = refs
        self.place = place
        self.tokens, self.width = self.x_ref.shape
        self.groups = capacity // LANE_ROWS
        self.tail = capacity - self.groups * LANE_ROWS
        self.parts = LANE_ROWS // self.tail
        self.piece = self.width // self.parts
        self.base = self.groups * self.width
        self.loads = [
            pltpu.make_async_copy(source, target, load_sem.at[number])
            for number, (source, target) in enumerate(
                [(sg_hbm, self.sg), (su_hbm, self.su), (sd_hbm, self.sd),
                 (wg_hbm.at[0], self.wg), (wu_hbm.at[0], self.wu), (wd_hbm.at[0], self.wd)]
            )
        ]

    def open(self):
        place, tokens = self.place, self.tokens
        for load in self.loads:
            load.start()
        barrier = pltpu.get_barrier_semaphore()

        def greet(device):
            pl.semaphore_signal(
                barrier, inc=1, device_id=device, device_id_type=pl.DeviceIdType.MESH
            )

        each(1, place.near, lambda distance: greet(place.away(distance, 1)[0]))
        greet(place.partner)

        floats = self.x_ref[...].astype(F32)
        inverse = lax.rsqrt(jnp.mean(floats * floats, axis=1, keepdims=True) + 1e-6)
        self.normed[...] = (floats * inverse * self.gain_ref[...]).astype(BF16)

        expert_rows = iota((2 * place.near, tokens), 0)
        first, second = self.idx_ref[0:1, :], self.idx_ref[1:2, :]
        hit_first = expert_rows == first
        hit_second = expert_rows == second
        named = as_weight(hit_first | hit_second)
        before = as_weight(iota((tokens, tokens), 0) < iota((tokens, tokens), 1))
        earlier = mm(named, before)
        self.meta[...] = jnp.zeros_like(self.meta)
        self.meta[0:1, :tokens] = first.astype(F32)
        self.meta[1:2, :tokens] = second.astype(F32)
        self.meta[2:3, :tokens] = jnp.sum(jnp.where(hit_first, earlier, 0.0), axis=0, keepdims=True)
        self.meta[3:4, :tokens] = jnp.sum(
            jnp.where(hit_second, earlier, 0.0), axis=0, keepdims=True
        )
        self.meta[4:6, :tokens] = self.weight_ref[...]
        self.slots(self.normed, self.meta, self.send_own)
        pl.semaphore_wait(barrier, place.near)

    def keys(self, first, second, place_first, place_second):
        near, low = self.place.near, self.place.half * self.place.near

        def main(expert, place, group):
            local, near_expert = place - group * LANE_ROWS, expert - low
            inside = (near_expert >= 0) & (near_expert < near)
            inside = inside & (local >= 0) & (local < LANE_ROWS)
            return jnp.where(inside, near_expert * LANE_ROWS + local, -LANE_ROWS)

        def tail(expert, place):
            local, near_expert = place - self.groups * LANE_ROWS, expert - low
            inside = (near_expert >= 0) & (near_expert < near) & (local >= 0)
            return jnp.where(inside, near_expert * LANE_ROWS + local * self.parts, -LANE_ROWS)

        mains = [
            (main(first, place_first, group), main(second, place_second, group))
            for group in range(self.groups)
        ]
        return mains, (tail(first, place_first), tail(second, place_second))

    def slots(self, block, meta, send):
        whole = meta[:, :self.tokens].astype(jnp.int32)
        mains, tails = self.keys(*[whole[row:row + 1, :] for row in range(4)])
        slot_rows = iota((self.place.near * LANE_ROWS, self.tokens), 0)
        step = self.width // 4
        for group, (first, second) in enumerate(mains):
            pick = as_weight((slot_rows == first) | (slot_rows == second))
            for at in range(0, self.width, step):
                send[:, group * self.width + at:group * self.width + at + step] = mm(
                    pick, block[:, at:at + step]
                ).astype(BF16)
        total = jnp.zeros((self.place.near * LANE_ROWS, self.piece), F32)
        for part in range(self.parts):
            pick = as_weight((slot_rows == tails[0] + part) | (slot_rows == tails[1] + part))
            total = total + mm(pick, block[:, part * self.piece:(part + 1) * self.piece])
        send[:, self.base:self.base + self.piece] = total.astype(BF16)

    def over(self, source, target, first):
        step = self.width // PIECES
        return [
            remote(
                source.at[:, number * step:(number + 1) * step],
                target.at[:, number * step:(number + 1) * step],
                self.over_send.at[first + number], self.over_recv.at[first + number],
                self.place.partner,
            )
            for number in range(PIECES)
        ]

    def block_copies(self):
        return [
            remote(
                self.meta, self.far_meta, self.over_send.at[2 * PIECES],
                self.over_recv.at[2 * PIECES], self.place.partner,
            )
        ] + self.over(self.normed, self.far_block, 0)

    def back_copies(self):
        return self.over(self.far_out, self.far_in, PIECES)

    def go_own(self, distance):
        device, spot = self.place.away(distance, 1)
        return remote(
            self.send_own.at[rows_of(spot), :], self.recv.at[rows_of(distance), :],
            self.go_send.at[distance], self.go_recv.at[distance], device,
        )

    def back_own(self, distance):
        device, _ = self.place.away(distance, -1)
        return remote(
            self.ysend.at[rows_of(distance), :], self.ret_own.at[rows_of(self.place.spot), :],
            self.back_send.at[distance], self.back_recv.at[distance], device,
        )

    def go_far(self, turn):
        place = self.place
        level, step = turn // place.cell, lax.rem(turn, place.cell)
        device, spot = place.at(level, *place.across(step, 1))
        slot = place.near + place.stage * place.cell + step
        return remote(
            self.send_far.at[rows_of(spot), :], self.recv.at[rows_of(slot), :],
            self.go_send.at[place.near + turn], self.go_recv.at[slot], device,
        )

    def got_far(self, stage, step):
        slot = self.place.near + stage * self.place.cell + step
        return remote(
            self.send_far.at[rows_of(0), :], self.recv.at[rows_of(slot), :],
            self.go_send.at[slot], self.go_recv.at[slot], self.place.partner,
        )

    def back_far(self, stage, step):
        place = self.place
        device, _ = place.at(place.level_of(stage), *place.across(step, -1))
        slot = place.near + stage * place.cell + step
        return remote(
            self.ysend.at[rows_of(slot), :], self.ret_far.at[rows_of(place.spot), :],
            self.back_send.at[slot],
            self.back_recv.at[place.near + place.level * place.cell + step], device,
        )

    def returned_far(self, turn):
        place = self.place
        level, step = turn // place.cell, lax.rem(turn, place.cell)
        _, spot = place.at(level, *place.across(step, 1))
        return remote(
            self.ysend.at[rows_of(0), :], self.ret_far.at[rows_of(spot), :],
            self.back_send.at[place.near + turn], self.back_recv.at[place.near + turn],
            place.partner,
        )

    def others(self, work):
        own = self.place.level * self.place.cell
        each(0, own, work)
        each(own + 1, self.place.near, work)

    def start(self):
        place = self.place

        @pl.when(place.stage == 0)
        def _():
            for copy in self.block_copies():
                copy.start()

        each(1, place.near, lambda distance: self.go_own(distance).start())
        self.recv[0:LANE_ROWS, :] = self.send_own[rows_of(place.spot), :]

        @pl.when(place.stage > 0)
        def _():
            for copy in self.block_copies():
                copy.start()

    def relay(self, stage):
        place = self.place

        @pl.when(place.stage == stage)
        def _():
            for copy in self.block_copies():
                copy.wait_recv()
            self.slots(self.far_block, self.far_meta, self.send_far)
            self.others(lambda turn: self.go_far(turn).start())
            slot = (place.near + stage * place.cell) * LANE_ROWS
            self.recv[slot:slot + LANE_ROWS, :] = self.send_far[rows_of(place.spot), :]

    def common(self):
        for load in self.loads[:3]:
            load.wait()
        gate = mm(self.normed[...], self.sg[...])
        hidden = (gate * jax.nn.sigmoid(gate) * mm(self.normed[...], self.su[...])).astype(BF16)
        step = self.width // 4
        for at in range(0, self.width, step):
            self.total[:, at:at + step] = mm(hidden, self.sd[:, at:at + step])
        for load in self.loads[3:]:
            load.wait()

    def serve(self, first, sources):
        main_rows, tail_rows = sources * LANE_ROWS, sources * self.tail
        low, width, base, piece = first * LANE_ROWS, self.width, self.base, self.piece
        start = self.groups * main_rows
        rows = start + tail_rows
        recv, ysend, xc, hc, yc = self.recv, self.ysend, self.xc, self.hc, self.yc

        def select(part, transposed):
            shape = (main_rows, tail_rows) if transposed else (tail_rows, main_rows)
            axis = 1 if transposed else 0
            return as_weight(iota(shape, 1 - axis) == iota(shape, axis) * self.parts + part)

        for group in range(self.groups):
            xc[group * main_rows:(group + 1) * main_rows, :] = recv[
                low:low + main_rows, group * width:(group + 1) * width
            ]
        for part in range(self.parts):
            xc[start:rows, part * piece:(part + 1) * piece] = mm(
                select(part, False), recv[low:low + main_rows, base:base + piece]
            ).astype(BF16)

        @pl.loop(0, hc.shape[1] // 256)
        def _(turn):
            columns = pl.ds(pl.multiple_of(turn * 256, 256), 256)
            gate = mm(xc[:rows, :], self.wg[:, columns])
            up = mm(xc[:rows, :], self.wu[:, columns])
            hc[:rows, columns] = (gate * jax.nn.sigmoid(gate) * up).astype(BF16)

        @pl.loop(0, width // 256)
        def _(turn):
            columns = pl.ds(pl.multiple_of(turn * 256, 256), 256)
            yc[:rows, columns] = mm(hc[:rows, :], self.wd[:, columns]).astype(BF16)

        for group in range(self.groups):
            ysend[low:low + main_rows, group * width:(group + 1) * width] = yc[
                group * main_rows:(group + 1) * main_rows, :
            ]
        total = jnp.zeros((main_rows, piece), F32)
        for part in range(self.parts):
            total = total + mm(
                select(part, True), yc[start:rows, part * piece:(part + 1) * piece]
            )
        ysend[low:low + main_rows, base:base + piece] = total.astype(BF16)

    def serve_own(self):
        place = self.place
        each(1, place.near, lambda distance: self.go_own(distance).wait_recv())
        self.serve(0, place.near)
        each(1, place.near, lambda distance: self.back_own(distance).start())
        self.ret_own[rows_of(place.spot), :] = self.ysend[0:LANE_ROWS, :]

    def serve_far(self, stage):
        place = self.place
        low = jnp.where(place.stage == stage, 1, 0)
        each(low, place.cell, lambda step: self.got_far(stage, step).wait_recv())
        first = place.near + stage * place.cell
        self.serve(first, place.cell)
        each(low, place.cell, lambda step: self.back_far(stage, step).start())

        @pl.when(place.stage == stage)
        def _():
            self.ret_far[rows_of(place.spot), :] = self.ysend[
                first * LANE_ROWS:(first + 1) * LANE_ROWS, :
            ]

    def mix(self, meta, ret, wait, store):
        turned = jnp.transpose(meta[...])[:self.tokens, :]
        whole = turned.astype(jnp.int32)
        mains, tails = self.keys(*[whole[:, row:row + 1] for row in range(4)])
        slot_lanes = iota((self.tokens, self.place.near * LANE_ROWS), 1)

        def mixing(first, second):
            values = jnp.where(slot_lanes == first, turned[:, 4:5], 0.0) + jnp.where(
                slot_lanes == second, turned[:, 5:6], 0.0
            )
            return halves(values)

        main_mix = [mixing(first, second) for first, second in mains]
        wait()
        for part in range(self.parts):
            low, high = part * self.piece, (part + 1) * self.piece
            total = jnp.zeros((self.tokens, self.piece), F32)
            for group, (coarse, fine) in enumerate(main_mix):
                values = ret[:, group * self.width + low:group * self.width + high]
                total = total + (mm(coarse, values) + mm(fine, values))
            coarse, fine = mixing(tails[0] + part, tails[1] + part)
            values = ret[:, self.base:self.base + self.piece]
            store(low, high, total + (mm(coarse, values) + mm(fine, values)))

    def mix_own(self):
        place = self.place

        def wait():
            each(1, place.near, lambda distance: self.back_own(distance).wait_recv())

        def store(low, high, value):
            self.total[:, low:high] = self.total[:, low:high] + value

        self.mix(self.meta, self.ret_own, wait, store)

    def mix_far(self, stage):
        @pl.when(self.place.stage == stage)
        def _():
            copies = self.back_copies()
            step = self.width // PIECES

            def wait():
                self.others(lambda turn: self.returned_far(turn).wait_recv())

            def store(low, high, value):
                self.far_out[:, low:high] = value.astype(BF16)
                if high % step == 0:
                    copies[high // step - 1].start()

            self.mix(self.far_meta, self.ret_far, wait, store)

    def close(self):
        step = self.width // PIECES
        for number, copy in enumerate(self.back_copies()):
            copy.wait_recv()
            columns = slice(number * step, (number + 1) * step)
            self.out_ref[:, columns] = (
                self.total[:, columns] + self.far_in[:, columns].astype(F32)
            ).astype(BF16)
        place = self.place
        each(1, place.near, lambda distance: self.go_own(distance).wait_send())
        each(1, place.near, lambda distance: self.back_own(distance).wait_send())
        self.others(lambda turn: self.go_far(turn).wait_send())
        for stage in range(place.depth):
            low = jnp.where(place.stage == stage, 1, 0)
            each(low, place.cell, lambda step: self.back_far(stage, step).wait_send())
        for copy in self.block_copies() + self.back_copies():
            copy.wait_send()


STATE_ROWS = 8


def nt(left, right, precision=None):
    return lax.dot_general(
        left, right, (((1,), (1,)), ((), ())), precision=precision, preferred_element_type=F32
    )


def halves(value):
    high = value.astype(BF16)
    return high, (value - high.astype(F32)).astype(BF16)


def log_one_plus(small):
    series = small * (1.0 - small * (0.5 - small * (1.0 / 3.0 - small * 0.25)))
    return jnp.where(small < 0.01, series, jnp.log(1.0 + small))


def mixer_parts(place_at, ep_count, tp_count, refs):
    (q_ref, k_ref, v_ref, in_ref, forget_ref, bias_ref, extra_ref, gate_ref, gain_ref, wo_hbm,
     out_ref, wo, locals_ref, state_send, state_recv, total_send, total_recv, total_ref,
     total_max, incoming, incoming_max, u_ref, squares_ref,
     u_recv, squares_recv, wo_sem, st_send, st_recv, tot_send, tot_recv, us_send, us_recv, sq_send, sq_recv) = refs
    exact = lax.Precision.HIGHEST
    heads, length = in_ref.shape
    blocks = length // BLK
    key_dim = q_ref.shape[1] // heads
    value_dim = v_ref.shape[1] // heads
    own_width = heads * value_dim
    scale = key_dim ** (-0.5)
    message = key_dim + STATE_ROWS
    share = length // tp_count
    share_blocks = share // BLK
    ep_at, tp_at = place_at.ep_at, place_at.tp_at
    load = pltpu.make_async_copy(wo_hbm, wo, wo_sem)

    def block_rows(ref, transform=lambda value, head: value):
        whole = ref[...]
        return jnp.concatenate(
            [
                transform(whole[head:head + 1, at * BLK:(at + 1) * BLK], head)
                for head in range(heads)
                for at in range(blocks)
            ],
            axis=0,
        )

    def key_block(head, at):
        return k_ref[at * BLK:(at + 1) * BLK, head * key_dim:(head + 1) * key_dim]

    def wide_values(head, at):
        values = v_ref[at * BLK:(at + 1) * BLK, head * value_dim:(head + 1) * value_dim]
        return jnp.concatenate([values, jnp.ones((BLK, value_dim), BF16)], axis=1)

    found = {}

    def grow(state, number):
        memory, top = state
        total = found["total"][number:number + 1, :]
        block_top = found["block_top"][number:number + 1, :]
        new_top = jnp.maximum(top + total, block_top)
        memory = jnp.exp(top + total - new_top) * memory + jnp.exp(
            block_top - new_top
        ) * locals_ref[number]
        return memory, new_top

    def diagonal():
        shape = (key_dim, value_dim)
        return iota(shape, 0) == iota(shape, 1)

    def early():
        load.start()
        logits = block_rows(forget_ref, lambda value, head: value + bias_ref[:, head:head + 1])
        kept = jnp.minimum(logits, 0.0) - log_one_plus(jnp.exp(-jnp.abs(logits)))
        kept = kept + block_rows(extra_ref)
        gates = block_rows(in_ref)
        upper = (iota((BLK, BLK), 0) <= iota((BLK, BLK), 1)).astype(F32)
        cumulative = jnp.dot(kept, upper, precision=exact, preferred_element_type=F32)
        total = cumulative[:, BLK - 1:BLK]
        gap = total - cumulative + gates
        block_top = jnp.max(gap, axis=1, keepdims=True)
        weight = jnp.exp(gap - block_top)
        found["total"], found["block_top"] = total, block_top
        found["cumulative"], found["shift"] = cumulative, gates - cumulative
        eye = (iota((key_dim, key_dim), 0) == iota((key_dim, key_dim), 1)).astype(F32).astype(BF16)
        for head in range(heads):
            state = (
                jnp.zeros((key_dim, 2 * value_dim), F32), jnp.full((1, 1), -1e30, F32)
            )
            decay = jnp.zeros((1, 1), F32)
            for at in range(blocks):
                number = head * blocks + at
                turned = nt(eye, key_block(head, at)) * weight[number:number + 1, :]
                high, low = halves(turned)
                values = wide_values(head, at)
                locals_ref[number] = mm(high, values) + mm(low, values)
                state = grow(state, number)
                decay = decay + total[number:number + 1, :]
            memory, top = state
            low_row = head * message
            state_send[low_row:low_row + key_dim, :] = memory[:, :value_dim]
            norm = jnp.sum(
                jnp.where(diagonal(), memory[:, value_dim:], 0.0), axis=0, keepdims=True
            )
            row = iota((STATE_ROWS, value_dim), 0)
            state_send[low_row + key_dim:low_row + message, :] = jnp.where(
                row == 0, norm, jnp.where(row == 1, top, decay)
            )

    span = place_at.depth * place_at.side
    own_at = lax.rem(ep_at, span)
    lower_half = place_at.half == 0

    def state_copy(distance, sign):
        at = lax.rem(own_at + sign * distance + span, span)
        return remote(
            state_send, state_recv.at[distance], st_send.at[distance], st_recv.at[distance],
            (place_at.half * span + at, tp_at),
        )

    def total_copy():
        return remote(total_send, total_recv, tot_send, tot_recv, place_at.partner)

    def sends_to(distance):
        return lower_half | (own_at + distance < span)

    def takes_from(distance):
        return lower_half | (own_at >= distance)

    def u_copies(target, sender):
        place = pl.ds(pl.multiple_of(sender * own_width, own_width), own_width)
        return [
            remote(
                u_ref.at[target * share:(target + 1) * share, :], u_recv.at[:, place],
                us_send.at[target], us_recv.at[sender], (ep_at, target),
            ),
            remote(
                squares_ref.at[target], squares_recv.at[sender],
                sq_send.at[target], sq_recv.at[sender], (ep_at, target),
            ),
        ]

    def send_states():
        for distance in range(1, span):
            @pl.when(sends_to(distance))
            def _():
                state_copy(distance, 1).start()

    def absorb(memory_ref, max_ref, message_ref):
        for head in range(heads):
            low_row = head * message
            memory = message_ref[low_row:low_row + key_dim, :]
            extra = message_ref[low_row + key_dim:low_row + message, :]
            norm = jnp.sum(jnp.where(diagonal(), extra[0:1, :], 0.0), axis=1, keepdims=True)
            top, decay = extra[1:2, :], extra[2:3, :]
            old_top = max_ref[head, 0:1, :]
            new_top = jnp.maximum(old_top + decay, top)
            left = jnp.exp(old_top + decay - new_top)
            right = jnp.exp(top - new_top)
            memory_ref[head, :, :value_dim] = (
                left * memory_ref[head, :, :value_dim] + right * memory
            )
            memory_ref[head, :, value_dim:] = (
                left * memory_ref[head, :, value_dim:] + right * norm
            )
            max_ref[head] = jnp.broadcast_to(new_top, max_ref.shape[1:])

    def take_states():
        for distance in range(1, span):
            @pl.when(takes_from(distance))
            def _():
                state_copy(distance, 1).wait_recv()

        @pl.when(lower_half)
        def _():
            total_ref[...] = jnp.zeros_like(total_ref)
            total_max[...] = jnp.full_like(total_max, -1e30)
            for distance in range(span - 1, 0, -1):
                @pl.when(own_at >= distance)
                def _():
                    absorb(total_ref, total_max, state_recv.at[distance])
            incoming[...] = total_ref[...]
            incoming_max[...] = total_max[...]
            absorb(total_ref, total_max, state_send)
            for distance in range(span - 1, 0, -1):
                @pl.when(own_at < distance)
                def _():
                    absorb(total_ref, total_max, state_recv.at[distance])
            for head in range(heads):
                low_row = head * message
                total_send[low_row:low_row + key_dim, :] = total_ref[head, :, :value_dim]
                norm = jnp.sum(
                    jnp.where(diagonal(), total_ref[head, :, value_dim:], 0.0),
                    axis=0, keepdims=True,
                )
                row = iota((STATE_ROWS, value_dim), 0)
                total_send[low_row + key_dim:low_row + message, :] = jnp.where(
                    row == 0, norm, jnp.where(row == 1, total_max[head], 0.0)
                )
            total_copy().start()

    def take_total():
        @pl.when(jnp.logical_not(lower_half))
        def _():
            incoming[...] = jnp.zeros_like(incoming)
            incoming_max[...] = jnp.full_like(incoming_max, -1e30)
            total_copy().wait_recv()
            absorb(incoming, incoming_max, total_recv)
            for distance in range(span - 1, 0, -1):
                @pl.when(own_at >= distance)
                def _():
                    absorb(incoming, incoming_max, state_recv.at[distance])

    def walk(low_block, high_block):
        if low_block == 0:
            found["states"] = [
                (incoming[head], incoming_max[head, 0:1, 0:1]) for head in range(heads)
            ]
            found["columns"] = jnp.transpose(found["cumulative"])
        states, columns = found["states"], found["columns"]
        lower = iota((BLK, BLK), 0) >= iota((BLK, BLK), 1)
        ones = jnp.ones((STATE_ROWS, value_dim), F32)
        for at in range(low_block, high_block):
            squares = jnp.zeros((STATE_ROWS, BLK), F32)
            for head in range(heads):
                number = head * blocks + at
                memory, top = states[head]
                query = q_ref[at * BLK:(at + 1) * BLK, head * key_dim:(head + 1) * key_dim]
                column = columns[:, number:number + 1]
                gap = jnp.where(
                    lower, column + found["shift"][number:number + 1, :], -jnp.inf
                )
                carried = column + top
                stabilizer = jnp.maximum(carried, jnp.max(gap, axis=1, keepdims=True))
                scores = nt(query, key_block(head, at)) * scale * jnp.exp(gap - stabilizer)
                high, low = halves(scores)
                values = wide_values(head, at)
                sums = mm(high, values) + mm(low, values)
                high, low = halves(memory)
                sums = sums + (jnp.exp(carried - stabilizer) * scale) * (
                    mm(query, high) + mm(query, low)
                )
                hidden = sums[:, :value_dim] / jnp.maximum(
                    jnp.abs(sums[:, value_dim:]), jnp.exp(-stabilizer)
                )
                squares = squares + nt(ones, hidden * hidden, exact)
                place = slice(head * value_dim, (head + 1) * value_dim)
                gate = gate_ref[at * BLK:(at + 1) * BLK, place].astype(F32)
                u_ref[at * BLK:(at + 1) * BLK, place] = (
                    hidden * gain_ref[:, place] * jax.nn.sigmoid(gate)
                ).astype(BF16)
                states[head] = grow(states[head], number)
            squares_ref[at // share_blocks, at % share_blocks] = squares
            if at % share_blocks == share_blocks - 1:
                target = at // share_blocks

                @pl.when(tp_at != target)
                def _():
                    for copy in u_copies(target, tp_at):
                        copy.start()

                @pl.when(tp_at == target)
                def _():
                    place = pl.ds(pl.multiple_of(tp_at * own_width, own_width), own_width)
                    u_recv[:, place] = u_ref[target * share:(target + 1) * share, :]
                    squares_recv[tp_at] = squares_ref[target]

    def late():
        for sender in range(tp_count):
            @pl.when(tp_at != sender)
            def _():
                for copy in u_copies(0, sender):
                    copy.wait_recv()
        squares = squares_recv[0]
        for sender in range(1, tp_count):
            squares = squares + squares_recv[sender]
        inverse_row = lax.rsqrt(squares / (heads * tp_count * value_dim) + 1e-6)
        eye = (iota((BLK, BLK), 0) == iota((BLK, BLK), 1)).astype(F32)
        load.wait()
        width = wo.shape[1]
        for at in range(share_blocks):
            inverse = nt(eye, inverse_row[at], exact)[:, 0:1]

            @pl.loop(0, width // 512)
            def _(turn):
                place = pl.ds(pl.multiple_of(turn * 512, 512), 512)
                product = mm(u_recv[at * BLK:(at + 1) * BLK, :], wo[:, place])
                out_ref[at * BLK:(at + 1) * BLK, place] = (product * inverse).astype(BF16)


    def close():
        for distance in range(1, span):
            @pl.when(sends_to(distance))
            def _():
                state_copy(distance, 1).wait_send()

        @pl.when(lower_half)
        def _():
            total_copy().wait_send()

        for target in range(tp_count):
            @pl.when(tp_at != target)
            def _():
                for copy in u_copies(target, tp_at):
                    copy.wait_send()

    return early, send_states, take_states, take_total, walk, late, close


def on_device(
    queries,
    head_key_rows,
    head_value_rows,
    log_input_gate,
    forget_logits,
    head_forget_bias,
    extra_log_forget,
    output_gate_logits,
    head_norm_gain,
    mixer_output_weight,
    second_batch_input,
    expert_norm_gain,
    routed_expert_index,
    routed_copy_weight,
    routed_gate_weight,
    routed_up_weight,
    routed_down_weight,
    shared_gate_weight,
    shared_up_weight,
    shared_down_weight,
):
    tokens, width = second_batch_input.shape
    ep_count = lax.axis_size("ep")
    tp_count = lax.axis_size("tp")
    count = ep_count * tp_count
    top_count = routed_expert_index.shape[1]
    capacity = max(2, 3 * tokens * top_count // (2 * count))
    wire = capacity * width // LANE_ROWS
    side = max(1, tp_count // CORES)
    near = count // 2
    span = ep_count // 2
    rows = near * capacity
    padded = -(-tokens // 128) * 128
    hidden_width = routed_gate_weight.shape[2]
    length = queries.shape[0]
    heads = head_forget_bias.shape[0]
    key_dim = queries.shape[1] // heads
    value_dim = head_value_rows.shape[1] // heads
    blocks = length // BLK
    share = length // tp_count
    dma = pltpu.SemaphoreType.DMA
    vmem = pl.BlockSpec(memory_space=pltpu.VMEM)
    hbm = pl.BlockSpec(memory_space=pl.ANY)

    block = pltpu.VMEM((tokens, width), BF16)
    meta = pltpu.VMEM((STATE_ROWS, padded), F32)
    half_slots = pltpu.VMEM((near * LANE_ROWS, wire), BF16)
    slots = pltpu.VMEM((2 * near * LANE_ROWS, wire), BF16)
    moe_scratch = (
        [block, meta, block, meta]
        + [half_slots, half_slots, slots, slots, half_slots, half_slots]
        + [block, block]
        + [
            pltpu.VMEM(array.shape[-2:], BF16)
            for array in (
                routed_gate_weight, routed_up_weight, routed_down_weight,
                shared_gate_weight, shared_up_weight, shared_down_weight,
            )
        ]
        + [
            pltpu.VMEM((rows, width), BF16),
            pltpu.VMEM((rows, hidden_width), BF16),
            pltpu.VMEM((rows, width), BF16),
            pltpu.VMEM((tokens, width), F32),
            dma((6,)), dma((count,)), dma((count,)), dma((count,)), dma((count,)),
            dma((2 * PIECES + 1,)), dma((2 * PIECES + 1,)),
        ]
    )
    message = heads * (key_dim + STATE_ROWS)
    mixer_scratch = [
        pltpu.VMEM(mixer_output_weight.shape, BF16),
        pltpu.VMEM((heads * blocks, key_dim, 2 * value_dim), F32),
        pltpu.VMEM((message, value_dim), F32),
        pltpu.VMEM((span, message, value_dim), F32),
        pltpu.VMEM((message, value_dim), F32),
        pltpu.VMEM((message, value_dim), F32),
        pltpu.VMEM((heads, key_dim, 2 * value_dim), F32),
        pltpu.VMEM((heads, STATE_ROWS, value_dim), F32),
        pltpu.VMEM((heads, key_dim, 2 * value_dim), F32),
        pltpu.VMEM((heads, STATE_ROWS, value_dim), F32),
        pltpu.VMEM((length, heads * value_dim), BF16),
        pltpu.VMEM((tp_count, share // BLK, STATE_ROWS, BLK), F32),
        pltpu.VMEM((share, tp_count * heads * value_dim), BF16),
        pltpu.VMEM((tp_count, share // BLK, STATE_ROWS, BLK), F32),
        dma, dma((span,)), dma((span,)), dma, dma,
        dma((tp_count,)), dma((tp_count,)), dma((tp_count,)), dma((tp_count,)),
    ]

    def kernel(*refs):
        mixer_in, moe_in = refs[:10], refs[10:20]
        mixer_out, moe_out = refs[20], refs[21]
        scratch = refs[22:]
        cut = len(moe_scratch)
        place = Place(ep_count, tp_count)
        early, send_states, take_states, take_total, walk, late, close = mixer_parts(
            place, ep_count, tp_count, (*mixer_in, mixer_out, *scratch[cut:])
        )
        experts = Experts(place, capacity, (*moe_in, moe_out, *scratch[:cut]))
        depth = place.depth
        experts.open()
        experts.start()
        early()
        send_states()
        experts.common()
        experts.relay(0)
        experts.serve_own()
        take_states()
        for stage in range(depth):
            experts.serve_far(stage)
            if stage + 1 < depth:
                experts.relay(stage + 1)
            if stage == 0:
                take_total()
            walk(blocks * stage // depth, blocks * (stage + 1) // depth)
            if stage == 0:
                experts.mix_own()
            experts.mix_far(stage)
        late()
        experts.close()
        close()

    return pl.pallas_call(
        kernel,
        out_shape=(
            jax.ShapeDtypeStruct((share, width), BF16),
            jax.ShapeDtypeStruct((tokens, width), BF16),
        ),
        in_specs=[vmem] * 9 + [hbm] + [vmem] * 4 + [hbm] * 6,
        out_specs=(vmem, vmem),
        scratch_shapes=moe_scratch + mixer_scratch,
        compiler_params=pltpu.CompilerParams(
            collective_id=0, has_side_effects=True, vmem_limit_bytes=62 * 1024 * 1024
        ),
        name="both",
    )(
        queries, head_key_rows, head_value_rows, log_input_gate.T, forget_logits.T,
        head_forget_bias[None, :], extra_log_forget.T, output_gate_logits,
        head_norm_gain[None, :], mixer_output_weight,
        second_batch_input, expert_norm_gain[None, :], routed_expert_index.T,
        routed_copy_weight.T, routed_gate_weight, routed_up_weight,
        routed_down_weight, shared_gate_weight, shared_up_weight, shared_down_weight,
    )


def solution(mesh):
    in_specs = (
        P("ep", "tp"),
        P("ep", "tp"),
        P("ep", "tp"),
        P("ep", "tp"),
        P("ep", "tp"),
        P("tp"),
        P("ep", "tp"),
        P("ep", "tp"),
        P("tp"),
        P(),
        P(("ep", "tp"), None),
        P(),
        P(("ep", "tp"), None),
        P(("ep", "tp"), None),
        P(("ep", "tp"), None, None),
        P(("ep", "tp"), None, None),
        P(("ep", "tp"), None, None),
        P(),
        P(),
        P(),
    )
    out_specs = (P(("ep", "tp"), None), P(("ep", "tp"), None))
    return jax.shard_map(
        on_device, mesh=mesh, in_specs=in_specs, out_specs=out_specs, check_vma=False
    )
```

```python
import jax
import jax.numpy as jnp
from jax import lax
from jax.experimental import pallas as pl
from jax.experimental.pallas import tpu as pltpu
from jax.sharding import PartitionSpec as P

BLK = 128


F32 = jnp.float32
BF16 = jnp.bfloat16
LANE_ROWS = 16
CORES = 2
PIECES = 2


def mm(left, right):
    return jnp.dot(left, right, preferred_element_type=F32)


def iota(shape, axis):
    return lax.broadcasted_iota(jnp.int32, shape, axis)


class Place:
    def __init__(self, ep_count, tp_count):
        self.side = max(1, tp_count // CORES)
        self.tp_count = tp_count
        self.planes = ep_count // self.side
        self.depth = self.planes // 2
        self.cell = self.side * tp_count
        self.near = self.depth * self.cell
        self.ep_at = lax.axis_index("ep")
        self.tp_at = lax.axis_index("tp")
        plane = self.ep_at // self.side
        self.row = lax.rem(self.ep_at, self.side)
        self.half = plane // self.depth
        self.level = plane - self.half * self.depth
        self.stage = self.half * self.level + (1 - self.half) * (self.depth - 1 - self.level)
        self.spot = self.level * self.cell + self.row * tp_count + self.tp_at
        self.inner = self.stage == 0
        self.low = jnp.where(self.inner, 1, 0)
        self.proxy = self.beyond(0)

    def at(self, level, row, tp):
        device = ((self.half * self.depth + level) * self.side + row, tp)
        return device, level * self.cell + row * self.tp_count + tp

    def across(self, step, sign):
        row_step, tp_step = step // self.tp_count, lax.rem(step, self.tp_count)
        row = lax.rem(self.row + sign * row_step + self.side, self.side)
        tp = lax.rem(self.tp_at + sign * tp_step + self.tp_count, self.tp_count)
        return row, tp

    def away(self, distance, sign):
        level_step = distance // self.cell
        level = lax.rem(self.level + sign * level_step + self.depth, self.depth)
        return self.at(level, *self.across(lax.rem(distance, self.cell), sign))

    def beyond(self, stage):
        plane = (1 - self.half) * (self.depth + stage) + self.half * (self.depth - 1 - stage)
        return plane * self.side + self.row, self.tp_at


def each(low, high, work):
    def turn(step, carry):
        work(step)
        return carry

    lax.fori_loop(low, high, turn, 0)


def rows_of(index):
    return pl.ds(pl.multiple_of(index * LANE_ROWS, LANE_ROWS), LANE_ROWS)


def remote(source, target, send_sem, recv_sem, device):
    return pltpu.make_async_remote_copy(
        src_ref=source, dst_ref=target, send_sem=send_sem, recv_sem=recv_sem,
        device_id=device, device_id_type=pl.DeviceIdType.MESH,
    )


def as_weight(mask):
    return mask.astype(F32).astype(BF16)


class Experts:
    def __init__(self, place, capacity, refs):
        (self.x_ref, self.gain_ref, self.idx_ref, self.weight_ref, wg_hbm, wu_hbm, wd_hbm, sg_hbm,
         su_hbm, sd_hbm, self.out_ref, self.normed, self.meta, self.far_block, self.far_meta,
         self.send_own, self.send_far, self.recv, self.ysend, self.ret_own, self.ret_far,
         self.far_out, self.far_in, self.wg, self.wu, self.wd, self.sg, self.su, self.sd, self.xc,
         self.hc, self.yc, self.total, load_sem, self.go_send, self.go_recv, self.far_send,
         self.back_send, self.back_recv, self.far_recv, self.over_send, self.over_recv,
         self.result_send, self.result_recv, self.meta_send, self.meta_recv) = refs
        self.place = place
        self.tokens, self.width = self.x_ref.shape
        self.step = self.width // PIECES
        self.groups = capacity // LANE_ROWS
        self.tail = capacity - self.groups * LANE_ROWS
        self.parts = LANE_ROWS // self.tail
        self.piece = self.step // self.parts
        self.base = self.groups * self.step
        self.wire = self.base + self.piece
        self.loads = [
            pltpu.make_async_copy(source, target, load_sem.at[number])
            for number, (source, target) in enumerate(
                [(sg_hbm, self.sg), (su_hbm, self.su), (sd_hbm, self.sd),
                 (wg_hbm.at[0], self.wg), (wu_hbm.at[0], self.wu), (wd_hbm.at[0], self.wd)]
            )
        ]

    def open(self):
        place, tokens = self.place, self.tokens
        for load in self.loads:
            load.start()
        barrier = pltpu.get_barrier_semaphore()

        def greet(device):
            pl.semaphore_signal(
                barrier, inc=1, device_id=device, device_id_type=pl.DeviceIdType.MESH
            )

        each(1, place.near, lambda distance: greet(place.away(distance, 1)[0]))
        greet(place.proxy)

        @pl.when(place.inner)
        def _():
            for stage in range(1, place.depth):
                greet(place.beyond(stage))

        floats = self.x_ref[...].astype(F32)
        inverse = lax.rsqrt(jnp.mean(floats * floats, axis=1, keepdims=True) + 1e-6)
        self.normed[...] = (floats * inverse * self.gain_ref[...]).astype(BF16)

        expert_rows = iota((2 * place.near, tokens), 0)
        first, second = self.idx_ref[0:1, :], self.idx_ref[1:2, :]
        hit_first = expert_rows == first
        hit_second = expert_rows == second
        named = as_weight(hit_first | hit_second)
        before = as_weight(iota((tokens, tokens), 0) < iota((tokens, tokens), 1))
        earlier = mm(named, before)
        self.meta[...] = jnp.zeros_like(self.meta)
        self.meta[0:1, :tokens] = first.astype(F32)
        self.meta[1:2, :tokens] = second.astype(F32)
        self.meta[2:3, :tokens] = jnp.sum(jnp.where(hit_first, earlier, 0.0), axis=0, keepdims=True)
        self.meta[3:4, :tokens] = jnp.sum(
            jnp.where(hit_second, earlier, 0.0), axis=0, keepdims=True
        )
        self.meta[4:6, :tokens] = self.weight_ref[...]
        for piece in range(PIECES):
            self.slots(piece, self.normed, self.meta, self.send_own)

    def meet(self):
        place = self.place
        pl.semaphore_wait(
            pltpu.get_barrier_semaphore(), place.near - 1 + jnp.where(place.inner, place.depth, 1)
        )

    def keys(self, first, second, place_first, place_second):
        near, low = self.place.near, self.place.half * self.place.near

        def main(expert, place, group):
            local, near_expert = place - group * LANE_ROWS, expert - low
            inside = (near_expert >= 0) & (near_expert < near)
            inside = inside & (local >= 0) & (local < LANE_ROWS)
            return jnp.where(inside, near_expert * LANE_ROWS + local, -LANE_ROWS)

        def tail(expert, place):
            local, near_expert = place - self.groups * LANE_ROWS, expert - low
            inside = (near_expert >= 0) & (near_expert < near) & (local >= 0)
            return jnp.where(inside, near_expert * LANE_ROWS + local * self.parts, -LANE_ROWS)

        mains = [
            (main(first, place_first, group), main(second, place_second, group))
            for group in range(self.groups)
        ]
        return mains, (tail(first, place_first), tail(second, place_second))

    def slots(self, piece, block, meta, send):
        whole = meta[:, :self.tokens].astype(jnp.int32)
        mains, tails = self.keys(*[whole[row:row + 1, :] for row in range(4)])
        slot_rows = iota((self.place.near * LANE_ROWS, self.tokens), 0)
        low, to = piece * self.step, piece * self.wire
        step = self.step // 2
        for group, (first, second) in enumerate(mains):
            pick = as_weight((slot_rows == first) | (slot_rows == second))
            for at in range(0, self.step, step):
                start = to + group * self.step + at
                send[:, start:start + step] = mm(
                    pick, block[:, low + at:low + at + step]
                ).astype(BF16)
        total = jnp.zeros((self.place.near * LANE_ROWS, self.piece), F32)
        for part in range(self.parts):
            pick = as_weight((slot_rows == tails[0] + part) | (slot_rows == tails[1] + part))
            at = low + part * self.piece
            total = total + mm(pick, block[:, at:at + self.piece])
        send[:, to + self.base:to + self.wire] = total.astype(BF16)

    def columns(self, piece):
        return slice(piece * self.step, (piece + 1) * self.step)

    def wires(self, piece):
        return slice(piece * self.wire, (piece + 1) * self.wire)

    def meta_copy(self):
        return remote(
            self.meta, self.far_meta.at[self.place.stage], self.meta_send,
            self.meta_recv.at[self.place.stage], self.place.proxy,
        )

    def meta_from(self, stage):
        return remote(
            self.meta, self.far_meta.at[stage], self.meta_send, self.meta_recv.at[stage],
            self.place.proxy,
        )

    def block_to(self, stage, piece):
        columns = self.columns(piece)
        return remote(
            self.normed.at[:, columns], self.far_block.at[stage, :, columns],
            self.over_send.at[piece], self.over_recv.at[stage, piece], self.place.proxy,
        )

    def result_to(self, stage, piece):
        columns = self.columns(piece)
        return remote(
            self.far_out.at[stage, :, columns], self.far_in.at[:, columns],
            self.result_send.at[stage, piece], self.result_recv.at[piece],
            self.place.beyond(stage),
        )

    def go_own(self, distance, piece):
        device, spot = self.place.away(distance, 1)
        wires = self.wires(piece)
        return remote(
            self.send_own.at[rows_of(spot), wires], self.recv.at[rows_of(distance), wires],
            self.go_send.at[piece, distance], self.go_recv.at[piece, distance], device,
        )

    def back_own(self, distance, piece):
        device, _ = self.place.away(distance, -1)
        wires = self.wires(piece)
        return remote(
            self.ysend.at[rows_of(distance), wires],
            self.ret_own.at[rows_of(self.place.spot), wires],
            self.back_send.at[piece, distance], self.back_recv.at[piece, distance], device,
        )

    def back_here(self, distance, piece):
        _, spot = self.place.away(distance, 1)
        wires = self.wires(piece)
        return remote(
            self.ysend.at[rows_of(distance), wires], self.ret_own.at[rows_of(spot), wires],
            self.back_send.at[piece, distance], self.back_recv.at[piece, distance],
            self.place.proxy,
        )

    def go_far(self, stage, turn, piece):
        place = self.place
        level, step = turn // place.cell, lax.rem(turn, place.cell)
        device, spot = place.at(level, *place.across(step, 1))
        slot = place.near + stage * place.cell + step
        wires = self.wires(piece)
        return remote(
            self.send_far.at[stage, rows_of(spot), wires], self.recv.at[rows_of(slot), wires],
            self.far_send.at[piece, stage * place.near + turn], self.go_recv.at[piece, slot],
            device,
        )

    def got_far(self, stage, step, piece):
        slot = self.place.near + stage * self.place.cell + step
        wires = self.wires(piece)
        return remote(
            self.send_far.at[stage, rows_of(0), wires], self.recv.at[rows_of(slot), wires],
            self.far_send.at[piece, 0], self.go_recv.at[piece, slot], self.place.proxy,
        )

    def back_far(self, stage, step, piece):
        place = self.place
        level = (1 - place.half) * (place.depth - 1)
        device, _ = place.at(level, *place.across(step, -1))
        slot = place.near + stage * place.cell + step
        wires = self.wires(piece)
        return remote(
            self.ysend.at[rows_of(slot), wires],
            self.ret_far.at[stage, rows_of(place.spot), wires],
            self.back_send.at[piece, slot],
            self.far_recv.at[piece, stage * place.near + place.level * place.cell + step],
            device,
        )

    def returned_far(self, stage, turn, piece):
        place = self.place
        level, step = turn // place.cell, lax.rem(turn, place.cell)
        _, spot = place.at(level, *place.across(step, 1))
        wires = self.wires(piece)
        return remote(
            self.ysend.at[rows_of(0), wires], self.ret_far.at[stage, rows_of(spot), wires],
            self.back_send.at[piece, 0], self.far_recv.at[piece, stage * place.near + turn],
            place.proxy,
        )

    def others(self, work):
        own = self.place.level * self.place.cell
        each(0, own, work)
        each(own + 1, self.place.near, work)

    def start(self):
        place = self.place

        @pl.when(place.inner)
        def _():
            self.meta_copy().start()
            for piece in range(PIECES):
                self.block_to(0, piece).start()

        for piece in range(PIECES):
            each(1, place.near, lambda distance: self.go_own(distance, piece).start())
        self.recv[0:LANE_ROWS, :] = self.send_own[rows_of(place.spot), :]

    def start_outer(self):
        place = self.place

        @pl.when(jnp.logical_not(place.inner))
        def _():
            self.meta_copy().start()
            for piece in range(PIECES):
                self.block_to(place.stage, piece).start()

    def relay(self, stage, piece):
        place = self.place

        @pl.when(place.inner)
        def _():
            if piece == 0:
                self.meta_from(stage).wait_recv()
            self.block_to(stage, piece).wait_recv()
            self.slots(piece, self.far_block.at[stage], self.far_meta.at[stage], self.send_far.at[stage])
            self.others(lambda turn: self.go_far(stage, turn, piece).start())
            slot = (place.near + stage * place.cell) * LANE_ROWS
            self.recv[slot:slot + LANE_ROWS, self.wires(piece)] = self.send_far[
                stage, rows_of(place.spot), self.wires(piece)
            ]

    def common(self):
        for load in self.loads[:3]:
            load.wait()
        gate = mm(self.normed[...], self.sg[...])
        hidden = (gate * jax.nn.sigmoid(gate) * mm(self.normed[...], self.su[...])).astype(BF16)
        step = self.width // 4
        for at in range(0, self.width, step):
            self.total[:, at:at + step] = mm(hidden, self.sd[:, at:at + step])
        for load in self.loads[3:]:
            load.wait()

    def serve(self, first, sources, arrive, leave, between):
        main_rows, tail_rows = sources * LANE_ROWS, sources * self.tail
        low, piece = first * LANE_ROWS, self.piece
        start = self.groups * main_rows
        rows = start + tail_rows
        recv, ysend, xc, hc, yc = self.recv, self.ysend, self.xc, self.hc, self.yc

        def select(part, transposed):
            shape = (main_rows, tail_rows) if transposed else (tail_rows, main_rows)
            axis = 1 if transposed else 0
            return as_weight(iota(shape, 1 - axis) == iota(shape, axis) * self.parts + part)

        for number in range(PIECES):
            arrive(number)
            at, to = number * self.wire, number * self.step
            for group in range(self.groups):
                xc[group * main_rows:(group + 1) * main_rows, to:to + self.step] = recv[
                    low:low + main_rows, at + group * self.step:at + (group + 1) * self.step
                ]
            for part in range(self.parts):
                xc[start:rows, to + part * piece:to + (part + 1) * piece] = mm(
                    select(part, False),
                    recv[low:low + main_rows, at + self.base:at + self.wire],
                ).astype(BF16)

        @pl.loop(0, hc.shape[1] // 256)
        def _(turn):
            columns = pl.ds(pl.multiple_of(turn * 256, 256), 256)
            gate = mm(xc[:rows, :], self.wg[:, columns])
            up = mm(xc[:rows, :], self.wu[:, columns])
            hc[:rows, columns] = (gate * jax.nn.sigmoid(gate) * up).astype(BF16)

        between()
        for number in range(PIECES):
            at, to = number * self.wire, number * self.step

            @pl.loop(0, self.step // 256)
            def _(turn):
                columns = pl.ds(pl.multiple_of(to + turn * 256, 256), 256)
                yc[:rows, columns] = mm(hc[:rows, :], self.wd[:, columns]).astype(BF16)

            for group in range(self.groups):
                ysend[
                    low:low + main_rows, at + group * self.step:at + (group + 1) * self.step
                ] = yc[group * main_rows:(group + 1) * main_rows, to:to + self.step]
            total = jnp.zeros((main_rows, piece), F32)
            for part in range(self.parts):
                total = total + mm(
                    select(part, True),
                    yc[start:rows, to + part * piece:to + (part + 1) * piece],
                )
            ysend[low:low + main_rows, at + self.base:at + self.wire] = total.astype(BF16)
            leave(number)

    def serve_own(self):
        place = self.place

        def arrive(piece):
            with jax.named_scope("wait_own"):
                each(1, place.near, lambda distance: self.go_own(distance, piece).wait_recv())

        def leave(piece):
            each(1, place.near, lambda distance: self.back_own(distance, piece).start())
            self.ret_own[rows_of(place.spot), self.wires(piece)] = self.ysend[
                0:LANE_ROWS, self.wires(piece)
            ]

        self.serve(0, place.near, arrive, leave, self.start_outer)

    def serve_far(self, stage):
        place = self.place
        first = place.near + stage * place.cell

        def arrive(piece):
            with jax.named_scope("wait_far"):
                each(
                    place.low, place.cell,
                    lambda step: self.got_far(stage, step, piece).wait_recv(),
                )

        def leave(piece):
            each(place.low, place.cell, lambda step: self.back_far(stage, step, piece).start())

            @pl.when(place.inner)
            def _():
                self.ret_far[stage, rows_of(place.spot), self.wires(piece)] = self.ysend[
                    first * LANE_ROWS:(first + 1) * LANE_ROWS, self.wires(piece)
                ]

        self.serve(first, place.cell, arrive, leave, lambda: None)

    def mix(self, meta, ret, wait, store):
        turned = jnp.transpose(meta[...])[:self.tokens, :]
        whole = turned.astype(jnp.int32)
        mains, tails = self.keys(*[whole[:, row:row + 1] for row in range(4)])
        slot_lanes = iota((self.tokens, self.place.near * LANE_ROWS), 1)

        def mixing(first, second):
            values = jnp.where(slot_lanes == first, turned[:, 4:5], 0.0) + jnp.where(
                slot_lanes == second, turned[:, 5:6], 0.0
            )
            return halves(values)

        main_mix = [mixing(first, second) for first, second in mains]
        tail_mix = [
            mixing(tails[0] + part, tails[1] + part) for part in range(self.parts)
        ]
        for number in range(PIECES):
            wait(number)
            at, to = number * self.wire, number * self.step
            for part in range(self.parts):
                low, high = part * self.piece, (part + 1) * self.piece
                coarse, fine = tail_mix[part]
                values = ret[:, at + self.base:at + self.wire]
                total = mm(coarse, values) + mm(fine, values)
                for group, (coarse, fine) in enumerate(main_mix):
                    start = at + group * self.step
                    values = ret[:, start + low:start + high]
                    total = total + (mm(coarse, values) + mm(fine, values))
                store(number, to + low, to + high, total)

    def mix_own(self):
        place = self.place

        def wait(piece):
            with jax.named_scope("wait_back"):
                each(1, place.near, lambda distance: self.back_here(distance, piece).wait_recv())

        def store(number, low, high, value):
            self.total[:, low:high] = self.total[:, low:high] + value

        self.mix(self.meta, self.ret_own, wait, store)

    def mix_far(self, stage):
        @pl.when(self.place.inner)
        def _():
            def wait(piece):
                with jax.named_scope("wait_ret"):
                    self.others(lambda turn: self.returned_far(stage, turn, piece).wait_recv())

            def store(number, low, high, value):
                self.far_out[stage, :, low:high] = value.astype(BF16)
                if high == (number + 1) * self.step:
                    self.result_to(stage, number).start()

            self.mix(self.far_meta.at[stage], self.ret_far.at[stage], wait, store)

    def close(self):
        place = self.place
        for piece in range(PIECES):
            with jax.named_scope("wait_result"):
                self.result_to(0, piece).wait_recv()
            columns = self.columns(piece)
            self.out_ref[:, columns] = (
                self.total[:, columns] + self.far_in[:, columns].astype(F32)
            ).astype(BF16)
        self.meta_copy().wait_send()
        for piece in range(PIECES):
            self.block_to(0, piece).wait_send()
            each(1, place.near, lambda distance: self.go_own(distance, piece).wait_send())
            each(1, place.near, lambda distance: self.back_own(distance, piece).wait_send())
            for stage in range(place.depth):
                each(
                    place.low, place.cell,
                    lambda step: self.back_far(stage, step, piece).wait_send(),
                )

        @pl.when(place.inner)
        def _():
            for piece in range(PIECES):
                for stage in range(place.depth):
                    self.others(lambda turn: self.go_far(stage, turn, piece).wait_send())
                    self.result_to(stage, piece).wait_send()


STATE_ROWS = 8


def nt(left, right, precision=None):
    return lax.dot_general(
        left, right, (((1,), (1,)), ((), ())), precision=precision, preferred_element_type=F32
    )


def halves(value):
    high = value.astype(BF16)
    return high, (value - high.astype(F32)).astype(BF16)


def log_one_plus(small):
    series = small * (1.0 - small * (0.5 - small * (1.0 / 3.0 - small * 0.25)))
    return jnp.where(small < 0.01, series, jnp.log(1.0 + small))


def mixer_parts(place_at, ep_count, tp_count, refs):
    (q_ref, k_ref, v_ref, in_ref, forget_ref, bias_ref, extra_ref, gate_ref, gain_ref, wo_hbm,
     out_ref, wo, locals_ref, state_send, state_recv, total_send, total_recv, total_ref,
     total_max, incoming, incoming_max, u_ref, squares_ref,
     u_recv, squares_recv, wo_sem, st_send, st_recv, tot_send, tot_recv, us_send, us_recv, sq_send, sq_recv) = refs
    exact = lax.Precision.HIGHEST
    heads, length = in_ref.shape
    blocks = length // BLK
    key_dim = q_ref.shape[1] // heads
    value_dim = v_ref.shape[1] // heads
    own_width = heads * value_dim
    scale = key_dim ** (-0.5)
    message = key_dim + STATE_ROWS
    share = length // tp_count
    share_blocks = share // BLK
    ep_at, tp_at = place_at.ep_at, place_at.tp_at
    load = pltpu.make_async_copy(wo_hbm, wo, wo_sem)

    def block_rows(ref, transform=lambda value, head: value):
        whole = ref[...]
        return jnp.concatenate(
            [
                transform(whole[head:head + 1, at * BLK:(at + 1) * BLK], head)
                for head in range(heads)
                for at in range(blocks)
            ],
            axis=0,
        )

    def key_block(head, at):
        return k_ref[at * BLK:(at + 1) * BLK, head * key_dim:(head + 1) * key_dim]

    def wide_values(head, at):
        values = v_ref[at * BLK:(at + 1) * BLK, head * value_dim:(head + 1) * value_dim]
        return jnp.concatenate([values, jnp.ones((BLK, value_dim), BF16)], axis=1)

    found = {}

    def grow(state, number):
        memory, top = state
        total = found["total"][number:number + 1, :]
        block_top = found["block_top"][number:number + 1, :]
        new_top = jnp.maximum(top + total, block_top)
        memory = jnp.exp(top + total - new_top) * memory + jnp.exp(
            block_top - new_top
        ) * locals_ref[number]
        return memory, new_top

    def diagonal():
        shape = (key_dim, value_dim)
        return iota(shape, 0) == iota(shape, 1)

    def early():
        load.start()
        logits = block_rows(forget_ref, lambda value, head: value + bias_ref[:, head:head + 1])
        kept = jnp.minimum(logits, 0.0) - log_one_plus(jnp.exp(-jnp.abs(logits)))
        kept = kept + block_rows(extra_ref)
        gates = block_rows(in_ref)
        upper = (iota((BLK, BLK), 0) <= iota((BLK, BLK), 1)).astype(F32)
        cumulative = jnp.dot(kept, upper, precision=exact, preferred_element_type=F32)
        total = cumulative[:, BLK - 1:BLK]
        gap = total - cumulative + gates
        block_top = jnp.max(gap, axis=1, keepdims=True)
        weight = jnp.exp(gap - block_top)
        found["total"], found["block_top"] = total, block_top
        found["cumulative"], found["shift"] = cumulative, gates - cumulative
        eye = (iota((key_dim, key_dim), 0) == iota((key_dim, key_dim), 1)).astype(F32).astype(BF16)
        for head in range(heads):
            state = (
                jnp.zeros((key_dim, 2 * value_dim), F32), jnp.full((1, 1), -1e30, F32)
            )
            decay = jnp.zeros((1, 1), F32)
            for at in range(blocks):
                number = head * blocks + at
                turned = nt(eye, key_block(head, at)) * weight[number:number + 1, :]
                high, low = halves(turned)
                values = wide_values(head, at)
                locals_ref[number] = mm(high, values) + mm(low, values)
                state = grow(state, number)
                decay = decay + total[number:number + 1, :]
            memory, top = state
            low_row = head * message
            state_send[low_row:low_row + key_dim, :] = memory[:, :value_dim]
            norm = jnp.sum(
                jnp.where(diagonal(), memory[:, value_dim:], 0.0), axis=0, keepdims=True
            )
            row = iota((STATE_ROWS, value_dim), 0)
            state_send[low_row + key_dim:low_row + message, :] = jnp.where(
                row == 0, norm, jnp.where(row == 1, top, decay)
            )

    span = place_at.depth * place_at.side
    own_at = lax.rem(ep_at, span)
    lower_half = place_at.half == 0

    def state_copy(distance, sign):
        at = lax.rem(own_at + sign * distance + span, span)
        return remote(
            state_send, state_recv.at[distance], st_send.at[distance], st_recv.at[distance],
            (place_at.half * span + at, tp_at),
        )

    low_inner = lower_half & place_at.inner
    first_inner = (place_at.depth - 1) * place_at.side

    def total_copy(stage):
        return remote(
            total_send, total_recv, tot_send.at[stage], tot_recv, place_at.beyond(stage)
        )

    def sends_to(distance):
        at = lax.rem(own_at + distance, span)
        return (own_at + distance < span) | (lower_half & (at >= first_inner))

    def takes_from(distance):
        return (own_at >= distance) | low_inner

    def u_copies(target, sender):
        place = pl.ds(pl.multiple_of(sender * own_width, own_width), own_width)
        return [
            remote(
                u_ref.at[target * share:(target + 1) * share, :], u_recv.at[:, place],
                us_send.at[target], us_recv.at[sender], (ep_at, target),
            ),
            remote(
                squares_ref.at[target], squares_recv.at[sender],
                sq_send.at[target], sq_recv.at[sender], (ep_at, target),
            ),
        ]

    def send_states():
        for distance in range(1, span):
            @pl.when(sends_to(distance))
            def _():
                state_copy(distance, 1).start()

    def absorb(memory_ref, max_ref, message_ref):
        for head in range(heads):
            low_row = head * message
            memory = message_ref[low_row:low_row + key_dim, :]
            extra = message_ref[low_row + key_dim:low_row + message, :]
            norm = jnp.sum(jnp.where(diagonal(), extra[0:1, :], 0.0), axis=1, keepdims=True)
            top, decay = extra[1:2, :], extra[2:3, :]
            old_top = max_ref[head, 0:1, :]
            new_top = jnp.maximum(old_top + decay, top)
            left = jnp.exp(old_top + decay - new_top)
            right = jnp.exp(top - new_top)
            memory_ref[head, :, :value_dim] = (
                left * memory_ref[head, :, :value_dim] + right * memory
            )
            memory_ref[head, :, value_dim:] = (
                left * memory_ref[head, :, value_dim:] + right * norm
            )
            max_ref[head] = jnp.broadcast_to(new_top, max_ref.shape[1:])

    def take_states():
        for distance in range(1, span):
            @pl.when(takes_from(distance))
            def _():
                state_copy(distance, 1).wait_recv()

        @pl.when(lower_half)
        def _():
            total_ref[...] = jnp.zeros_like(total_ref)
            total_max[...] = jnp.full_like(total_max, -1e30)
            for distance in range(span - 1, 0, -1):
                @pl.when(own_at >= distance)
                def _():
                    absorb(total_ref, total_max, state_recv.at[distance])
            incoming[...] = total_ref[...]
            incoming_max[...] = total_max[...]

        @pl.when(low_inner)
        def _():
            absorb(total_ref, total_max, state_send)
            for distance in range(span - 1, 0, -1):
                @pl.when(own_at < distance)
                def _():
                    absorb(total_ref, total_max, state_recv.at[distance])
            for head in range(heads):
                low_row = head * message
                total_send[low_row:low_row + key_dim, :] = total_ref[head, :, :value_dim]
                norm = jnp.sum(
                    jnp.where(diagonal(), total_ref[head, :, value_dim:], 0.0),
                    axis=0, keepdims=True,
                )
                row = iota((STATE_ROWS, value_dim), 0)
                total_send[low_row + key_dim:low_row + message, :] = jnp.where(
                    row == 0, norm, jnp.where(row == 1, total_max[head], 0.0)
                )
            for stage in range(place_at.depth):
                total_copy(stage).start()

    def take_total():
        @pl.when(jnp.logical_not(lower_half))
        def _():
            incoming[...] = jnp.zeros_like(incoming)
            incoming_max[...] = jnp.full_like(incoming_max, -1e30)
            total_copy(0).wait_recv()
            absorb(incoming, incoming_max, total_recv)
            for distance in range(span - 1, 0, -1):
                @pl.when(own_at >= distance)
                def _():
                    absorb(incoming, incoming_max, state_recv.at[distance])

    def walk(low_block, high_block):
        if low_block == 0:
            found["states"] = [
                (incoming[head], incoming_max[head, 0:1, 0:1]) for head in range(heads)
            ]
            found["columns"] = jnp.transpose(found["cumulative"])
        states, columns = found["states"], found["columns"]
        lower = iota((BLK, BLK), 0) >= iota((BLK, BLK), 1)
        ones = jnp.ones((STATE_ROWS, value_dim), F32)
        for at in range(low_block, high_block):
            squares = jnp.zeros((STATE_ROWS, BLK), F32)
            for head in range(heads):
                number = head * blocks + at
                memory, top = states[head]
                query = q_ref[at * BLK:(at + 1) * BLK, head * key_dim:(head + 1) * key_dim]
                column = columns[:, number:number + 1]
                gap = jnp.where(
                    lower, column + found["shift"][number:number + 1, :], -jnp.inf
                )
                carried = column + top
                stabilizer = jnp.maximum(carried, jnp.max(gap, axis=1, keepdims=True))
                scores = nt(query, key_block(head, at)) * scale * jnp.exp(gap - stabilizer)
                high, low = halves(scores)
                values = wide_values(head, at)
                sums = mm(high, values) + mm(low, values)
                high, low = halves(memory)
                sums = sums + (jnp.exp(carried - stabilizer) * scale) * (
                    mm(query, high) + mm(query, low)
                )
                hidden = sums[:, :value_dim] / jnp.maximum(
                    jnp.abs(sums[:, value_dim:]), jnp.exp(-stabilizer)
                )
                squares = squares + nt(ones, hidden * hidden, exact)
                place = slice(head * value_dim, (head + 1) * value_dim)
                gate = gate_ref[at * BLK:(at + 1) * BLK, place].astype(F32)
                u_ref[at * BLK:(at + 1) * BLK, place] = (
                    hidden * gain_ref[:, place] * jax.nn.sigmoid(gate)
                ).astype(BF16)
                states[head] = grow(states[head], number)
            squares_ref[at // share_blocks, at % share_blocks] = squares
            if at % share_blocks == share_blocks - 1:
                target = at // share_blocks

                @pl.when(tp_at != target)
                def _():
                    for copy in u_copies(target, tp_at):
                        copy.start()

                @pl.when(tp_at == target)
                def _():
                    place = pl.ds(pl.multiple_of(tp_at * own_width, own_width), own_width)
                    u_recv[:, place] = u_ref[target * share:(target + 1) * share, :]
                    squares_recv[tp_at] = squares_ref[target]

    def late():
        for sender in range(tp_count):
            @pl.when(tp_at != sender)
            def _():
                for copy in u_copies(0, sender):
                    copy.wait_recv()
        squares = squares_recv[0]
        for sender in range(1, tp_count):
            squares = squares + squares_recv[sender]
        inverse_row = lax.rsqrt(squares / (heads * tp_count * value_dim) + 1e-6)
        eye = (iota((BLK, BLK), 0) == iota((BLK, BLK), 1)).astype(F32)
        load.wait()
        width = wo.shape[1]
        for at in range(share_blocks):
            inverse = nt(eye, inverse_row[at], exact)[:, 0:1]

            @pl.loop(0, width // 512)
            def _(turn):
                place = pl.ds(pl.multiple_of(turn * 512, 512), 512)
                product = mm(u_recv[at * BLK:(at + 1) * BLK, :], wo[:, place])
                out_ref[at * BLK:(at + 1) * BLK, place] = (product * inverse).astype(BF16)


    def close():
        for distance in range(1, span):
            @pl.when(sends_to(distance))
            def _():
                state_copy(distance, 1).wait_send()

        @pl.when(low_inner)
        def _():
            for stage in range(place_at.depth):
                total_copy(stage).wait_send()

        for target in range(tp_count):
            @pl.when(tp_at != target)
            def _():
                for copy in u_copies(target, tp_at):
                    copy.wait_send()

    return early, send_states, take_states, take_total, walk, late, close


def on_device(
    queries,
    head_key_rows,
    head_value_rows,
    log_input_gate,
    forget_logits,
    head_forget_bias,
    extra_log_forget,
    output_gate_logits,
    head_norm_gain,
    mixer_output_weight,
    second_batch_input,
    expert_norm_gain,
    routed_expert_index,
    routed_copy_weight,
    routed_gate_weight,
    routed_up_weight,
    routed_down_weight,
    shared_gate_weight,
    shared_up_weight,
    shared_down_weight,
):
    tokens, width = second_batch_input.shape
    ep_count = lax.axis_size("ep")
    tp_count = lax.axis_size("tp")
    count = ep_count * tp_count
    top_count = routed_expert_index.shape[1]
    capacity = max(2, 3 * tokens * top_count // (2 * count))
    groups = capacity // LANE_ROWS
    step = width // PIECES
    wire = PIECES * (groups * step + step * (capacity - groups * LANE_ROWS) // LANE_ROWS)
    side = max(1, tp_count // CORES)
    near = count // 2
    span = ep_count // 2
    depth = ep_count // side // 2
    rows = near * capacity
    padded = -(-tokens // 128) * 128
    hidden_width = routed_gate_weight.shape[2]
    length = queries.shape[0]
    heads = head_forget_bias.shape[0]
    key_dim = queries.shape[1] // heads
    value_dim = head_value_rows.shape[1] // heads
    blocks = length // BLK
    share = length // tp_count
    dma = pltpu.SemaphoreType.DMA
    vmem = pl.BlockSpec(memory_space=pltpu.VMEM)
    hbm = pl.BlockSpec(memory_space=pl.ANY)

    block = pltpu.VMEM((tokens, width), BF16)
    meta = pltpu.VMEM((STATE_ROWS, padded), F32)
    half_slots = pltpu.VMEM((near * LANE_ROWS, wire), BF16)
    far_slots = pltpu.VMEM((depth, near * LANE_ROWS, wire), BF16)
    far_block = pltpu.VMEM((depth, tokens, width), BF16)
    slots = pltpu.VMEM((2 * near * LANE_ROWS, wire), BF16)
    moe_scratch = (
        [block, meta, far_block, pltpu.VMEM((depth, STATE_ROWS, padded), F32)]
        + [half_slots, far_slots, slots, slots, half_slots, far_slots]
        + [far_block, block]
        + [
            pltpu.VMEM(array.shape[-2:], BF16)
            for array in (
                routed_gate_weight, routed_up_weight, routed_down_weight,
                shared_gate_weight, shared_up_weight, shared_down_weight,
            )
        ]
        + [
            pltpu.VMEM((rows, width), BF16),
            pltpu.VMEM((rows, hidden_width), BF16),
            pltpu.VMEM((rows, width), BF16),
            pltpu.VMEM((tokens, width), F32),
            dma((6,)), dma((PIECES, near)), dma((PIECES, count)), dma((PIECES, depth * near)),
            dma((PIECES, count)), dma((PIECES, near)), dma((PIECES, depth * near)),
            dma((PIECES,)), dma((depth, PIECES)), dma((depth, PIECES)), dma((PIECES,)),
            dma, dma((depth,)),
        ]
    )
    message = heads * (key_dim + STATE_ROWS)
    mixer_scratch = [
        pltpu.VMEM(mixer_output_weight.shape, BF16),
        pltpu.VMEM((heads * blocks, key_dim, 2 * value_dim), F32),
        pltpu.VMEM((message, value_dim), F32),
        pltpu.VMEM((span, message, value_dim), F32),
        pltpu.VMEM((message, value_dim), F32),
        pltpu.VMEM((message, value_dim), F32),
        pltpu.VMEM((heads, key_dim, 2 * value_dim), F32),
        pltpu.VMEM((heads, STATE_ROWS, value_dim), F32),
        pltpu.VMEM((heads, key_dim, 2 * value_dim), F32),
        pltpu.VMEM((heads, STATE_ROWS, value_dim), F32),
        pltpu.VMEM((length, heads * value_dim), BF16),
        pltpu.VMEM((tp_count, share // BLK, STATE_ROWS, BLK), F32),
        pltpu.VMEM((share, tp_count * heads * value_dim), BF16),
        pltpu.VMEM((tp_count, share // BLK, STATE_ROWS, BLK), F32),
        dma, dma((span,)), dma((span,)), dma((depth,)), dma,
        dma((tp_count,)), dma((tp_count,)), dma((tp_count,)), dma((tp_count,)),
    ]

    def kernel(*refs):
        mixer_in, moe_in = refs[:10], refs[10:20]
        mixer_out, moe_out = refs[20], refs[21]
        scratch = refs[22:]
        cut = len(moe_scratch)
        place = Place(ep_count, tp_count)
        early, send_states, take_states, take_total, walk, late, close = mixer_parts(
            place, ep_count, tp_count, (*mixer_in, mixer_out, *scratch[cut:])
        )
        experts = Experts(place, capacity, (*moe_in, moe_out, *scratch[:cut]))
        depth = place.depth
        experts.open()
        early()
        experts.meet()
        experts.start()
        send_states()
        experts.common()
        for piece in range(PIECES):
            experts.relay(0, piece)
        experts.serve_own()
        for stage in range(depth):
            if stage + 1 < depth:
                experts.relay(stage + 1, 0)
            experts.serve_far(stage)
            if stage + 1 < depth:
                for piece in range(1, PIECES):
                    experts.relay(stage + 1, piece)
            if stage == 0:
                take_states()
                take_total()
            walk(blocks * stage // depth, blocks * (stage + 1) // depth)
            experts.mix_far(stage)
            if stage == 0:
                experts.mix_own()
        late()
        experts.close()
        close()

    return pl.pallas_call(
        kernel,
        out_shape=(
            jax.ShapeDtypeStruct((share, width), BF16),
            jax.ShapeDtypeStruct((tokens, width), BF16),
        ),
        in_specs=[vmem] * 9 + [hbm] + [vmem] * 4 + [hbm] * 6,
        out_specs=(vmem, vmem),
        scratch_shapes=moe_scratch + mixer_scratch,
        compiler_params=pltpu.CompilerParams(
            collective_id=0, has_side_effects=True, vmem_limit_bytes=62 * 1024 * 1024
        ),
        name="both",
    )(
        queries, head_key_rows, head_value_rows, log_input_gate.T, forget_logits.T,
        head_forget_bias[None, :], extra_log_forget.T, output_gate_logits,
        head_norm_gain[None, :], mixer_output_weight,
        second_batch_input, expert_norm_gain[None, :], routed_expert_index.T,
        routed_copy_weight.T, routed_gate_weight, routed_up_weight,
        routed_down_weight, shared_gate_weight, shared_up_weight, shared_down_weight,
    )


def solution(mesh):
    in_specs = (
        P("ep", "tp"),
        P("ep", "tp"),
        P("ep", "tp"),
        P("ep", "tp"),
        P("ep", "tp"),
        P("tp"),
        P("ep", "tp"),
        P("ep", "tp"),
        P("tp"),
        P(),
        P(("ep", "tp"), None),
        P(),
        P(("ep", "tp"), None),
        P(("ep", "tp"), None),
        P(("ep", "tp"), None, None),
        P(("ep", "tp"), None, None),
        P(("ep", "tp"), None, None),
        P(),
        P(),
        P(),
    )
    out_specs = (P(("ep", "tp"), None), P(("ep", "tp"), None))
    return jax.shard_map(
        on_device, mesh=mesh, in_specs=in_specs, out_specs=out_specs, check_vma=False
    )
```

```python
import jax
import jax.numpy as jnp
from jax import lax
from jax.experimental import pallas as pl
from jax.experimental.pallas import tpu as pltpu
from jax.sharding import PartitionSpec as P

BLK = 128


F32 = jnp.float32
BF16 = jnp.bfloat16
LANE_ROWS = 16
CORES = 2
PIECES = 2


def mm(left, right):
    return jnp.dot(left, right, preferred_element_type=F32)


def iota(shape, axis):
    return lax.broadcasted_iota(jnp.int32, shape, axis)


class Place:
    def __init__(self, ep_count, tp_count):
        self.side = max(1, tp_count // CORES)
        self.tp_count = tp_count
        self.planes = ep_count // self.side
        self.depth = self.planes // 2
        self.cell = self.side * tp_count
        self.near = self.depth * self.cell
        self.ep_at = lax.axis_index("ep")
        self.tp_at = lax.axis_index("tp")
        plane = self.ep_at // self.side
        self.row = lax.rem(self.ep_at, self.side)
        self.half = plane // self.depth
        self.level = plane - self.half * self.depth
        self.stage = self.half * self.level + (1 - self.half) * (self.depth - 1 - self.level)
        self.spot = self.level * self.cell + self.row * tp_count + self.tp_at
        self.inner = self.stage == 0
        self.low = jnp.where(self.inner, 1, 0)
        self.proxy = self.beyond(0)

    def at(self, level, row, tp):
        device = ((self.half * self.depth + level) * self.side + row, tp)
        return device, level * self.cell + row * self.tp_count + tp

    def across(self, step, sign):
        row_step, tp_step = step // self.tp_count, lax.rem(step, self.tp_count)
        row = lax.rem(self.row + sign * row_step + self.side, self.side)
        tp = lax.rem(self.tp_at + sign * tp_step + self.tp_count, self.tp_count)
        return row, tp

    def away(self, distance, sign):
        level_step = distance // self.cell
        level = lax.rem(self.level + sign * level_step + self.depth, self.depth)
        return self.at(level, *self.across(lax.rem(distance, self.cell), sign))

    def beyond(self, stage):
        plane = (1 - self.half) * (self.depth + stage) + self.half * (self.depth - 1 - stage)
        return plane * self.side + self.row, self.tp_at


def each(low, high, work):
    def turn(step, carry):
        work(step)
        return carry

    lax.fori_loop(low, high, turn, 0)


def rows_of(index):
    return pl.ds(pl.multiple_of(index * LANE_ROWS, LANE_ROWS), LANE_ROWS)


def remote(source, target, send_sem, recv_sem, device):
    return pltpu.make_async_remote_copy(
        src_ref=source, dst_ref=target, send_sem=send_sem, recv_sem=recv_sem,
        device_id=device, device_id_type=pl.DeviceIdType.MESH,
    )


def as_weight(mask):
    return mask.astype(F32).astype(BF16)


class Experts:
    def __init__(self, place, capacity, refs):
        (self.x_ref, self.gain_ref, self.idx_ref, self.weight_ref, wg_hbm, wu_hbm, wd_hbm, sg_hbm,
         su_hbm, sd_hbm, self.out_ref, self.normed, self.meta, self.far_block, self.far_meta,
         self.send_own, self.send_far, self.recv, self.ysend, self.ret_own, self.ret_far,
         self.far_out, self.far_in, self.wg, self.wu, self.wd, self.sg, self.su, self.sd, self.xc,
         self.hc, self.yc, self.gates, self.ups, self.total, self.out, load_sem, self.go_send, self.go_recv, self.far_send,
         self.back_send, self.back_recv, self.far_recv, self.over_send, self.over_recv,
         self.result_send, self.result_recv, self.meta_send, self.meta_recv, self.out_sem) = refs
        self.place = place
        self.tokens, self.width = self.x_ref.shape
        self.step = self.width // PIECES
        self.groups = capacity // LANE_ROWS
        self.tail = capacity - self.groups * LANE_ROWS
        self.parts = LANE_ROWS // self.tail
        self.piece = self.step // self.parts
        self.base = self.groups * self.step
        self.wire = self.base + self.piece
        self.loads = [
            pltpu.make_async_copy(source, target, load_sem.at[number])
            for number, (source, target) in enumerate(
                [(sg_hbm, self.sg), (su_hbm, self.su), (sd_hbm, self.sd),
                 (wg_hbm.at[0], self.wg), (wu_hbm.at[0], self.wu), (wd_hbm.at[0], self.wd)]
            )
        ]

    def open(self):
        place, tokens = self.place, self.tokens
        for load in self.loads:
            load.start()
        barrier = pltpu.get_barrier_semaphore()

        def greet(device):
            pl.semaphore_signal(
                barrier, inc=1, device_id=device, device_id_type=pl.DeviceIdType.MESH
            )

        each(1, place.near, lambda distance: greet(place.away(distance, 1)[0]))
        greet(place.proxy)

        @pl.when(place.inner)
        def _():
            for stage in range(1, place.depth):
                greet(place.beyond(stage))

        floats = self.x_ref[...].astype(F32)
        inverse = lax.rsqrt(jnp.mean(floats * floats, axis=1, keepdims=True) + 1e-6)
        self.normed[...] = (floats * inverse * self.gain_ref[...]).astype(BF16)

        expert_rows = iota((2 * place.near, tokens), 0)
        first, second = self.idx_ref[0:1, :], self.idx_ref[1:2, :]
        hit_first = expert_rows == first
        hit_second = expert_rows == second
        named = as_weight(hit_first | hit_second)
        before = as_weight(iota((tokens, tokens), 0) < iota((tokens, tokens), 1))
        earlier = mm(named, before)
        self.meta[...] = jnp.zeros_like(self.meta)
        self.meta[0:1, :tokens] = first.astype(F32)
        self.meta[1:2, :tokens] = second.astype(F32)
        self.meta[2:3, :tokens] = jnp.sum(jnp.where(hit_first, earlier, 0.0), axis=0, keepdims=True)
        self.meta[3:4, :tokens] = jnp.sum(
            jnp.where(hit_second, earlier, 0.0), axis=0, keepdims=True
        )
        self.meta[4:6, :tokens] = self.weight_ref[...]
    def meet(self):
        place = self.place
        pl.semaphore_wait(
            pltpu.get_barrier_semaphore(), place.near - 1 + jnp.where(place.inner, place.depth, 1)
        )

    def keys(self, first, second, place_first, place_second):
        near, low = self.place.near, self.place.half * self.place.near

        def main(expert, place, group):
            local, near_expert = place - group * LANE_ROWS, expert - low
            inside = (near_expert >= 0) & (near_expert < near)
            inside = inside & (local >= 0) & (local < LANE_ROWS)
            return jnp.where(inside, near_expert * LANE_ROWS + local, -LANE_ROWS)

        def tail(expert, place):
            local, near_expert = place - self.groups * LANE_ROWS, expert - low
            inside = (near_expert >= 0) & (near_expert < near) & (local >= 0)
            return jnp.where(inside, near_expert * LANE_ROWS + local * self.parts, -LANE_ROWS)

        mains = [
            (main(first, place_first, group), main(second, place_second, group))
            for group in range(self.groups)
        ]
        return mains, (tail(first, place_first), tail(second, place_second))

    def slots(self, piece, block, meta, send):
        whole = meta[:, :self.tokens].astype(jnp.int32)
        mains, tails = self.keys(*[whole[row:row + 1, :] for row in range(4)])
        slot_rows = iota((self.place.near * LANE_ROWS, self.tokens), 0)
        low, to = piece * self.step, piece * self.wire
        step = self.step // 2
        for group, (first, second) in enumerate(mains):
            pick = as_weight((slot_rows == first) | (slot_rows == second))
            for at in range(0, self.step, step):
                start = to + group * self.step + at
                send[:, start:start + step] = mm(
                    pick, block[:, low + at:low + at + step]
                ).astype(BF16)
        total = jnp.zeros((self.place.near * LANE_ROWS, self.piece), F32)
        for part in range(self.parts):
            pick = as_weight((slot_rows == tails[0] + part) | (slot_rows == tails[1] + part))
            at = low + part * self.piece
            total = total + mm(pick, block[:, at:at + self.piece])
        send[:, to + self.base:to + self.wire] = total.astype(BF16)

    def columns(self, piece):
        return slice(piece * self.step, (piece + 1) * self.step)

    def wires(self, piece):
        return slice(piece * self.wire, (piece + 1) * self.wire)

    def meta_copy(self):
        return remote(
            self.meta, self.far_meta.at[self.place.stage], self.meta_send,
            self.meta_recv.at[self.place.stage], self.place.proxy,
        )

    def meta_from(self, stage):
        return remote(
            self.meta, self.far_meta.at[stage], self.meta_send, self.meta_recv.at[stage],
            self.place.proxy,
        )

    def block_to(self, stage, piece):
        columns = self.columns(piece)
        return remote(
            self.normed.at[:, columns], self.far_block.at[stage, :, columns],
            self.over_send.at[piece], self.over_recv.at[stage, piece], self.place.proxy,
        )

    def result_to(self, stage, piece):
        columns = self.columns(piece)
        return remote(
            self.far_out.at[stage, :, columns], self.far_in.at[:, columns],
            self.result_send.at[stage, piece], self.result_recv.at[piece],
            self.place.beyond(stage),
        )

    def go_own(self, distance, piece):
        device, spot = self.place.away(distance, 1)
        wires = self.wires(piece)
        return remote(
            self.send_own.at[rows_of(spot), wires], self.recv.at[rows_of(distance), wires],
            self.go_send.at[piece, distance], self.go_recv.at[piece, distance], device,
        )

    def back_own(self, distance, piece):
        device, _ = self.place.away(distance, -1)
        wires = self.wires(piece)
        return remote(
            self.ysend.at[rows_of(distance), wires],
            self.ret_own.at[rows_of(self.place.spot), wires],
            self.back_send.at[piece, distance], self.back_recv.at[piece, distance], device,
        )

    def back_here(self, distance, piece):
        _, spot = self.place.away(distance, 1)
        wires = self.wires(piece)
        return remote(
            self.ysend.at[rows_of(distance), wires], self.ret_own.at[rows_of(spot), wires],
            self.back_send.at[piece, distance], self.back_recv.at[piece, distance],
            self.place.proxy,
        )

    def go_far(self, stage, turn, piece):
        place = self.place
        level, step = turn // place.cell, lax.rem(turn, place.cell)
        device, spot = place.at(level, *place.across(step, 1))
        slot = place.near + stage * place.cell + step
        wires = self.wires(piece)
        return remote(
            self.send_far.at[stage, rows_of(spot), wires], self.recv.at[rows_of(slot), wires],
            self.far_send.at[piece, stage * place.near + turn], self.go_recv.at[piece, slot],
            device,
        )

    def got_far(self, stage, step, piece):
        slot = self.place.near + stage * self.place.cell + step
        wires = self.wires(piece)
        return remote(
            self.send_far.at[stage, rows_of(0), wires], self.recv.at[rows_of(slot), wires],
            self.far_send.at[piece, 0], self.go_recv.at[piece, slot], self.place.proxy,
        )

    def back_far(self, stage, step, piece):
        place = self.place
        level = (1 - place.half) * (place.depth - 1)
        device, _ = place.at(level, *place.across(step, -1))
        slot = place.near + stage * place.cell + step
        wires = self.wires(piece)
        return remote(
            self.ysend.at[rows_of(slot), wires],
            self.ret_far.at[stage, rows_of(place.spot), wires],
            self.back_send.at[piece, slot],
            self.far_recv.at[piece, stage * place.near + place.level * place.cell + step],
            device,
        )

    def returned_far(self, stage, turn, piece):
        place = self.place
        level, step = turn // place.cell, lax.rem(turn, place.cell)
        _, spot = place.at(level, *place.across(step, 1))
        wires = self.wires(piece)
        return remote(
            self.ysend.at[rows_of(0), wires], self.ret_far.at[stage, rows_of(spot), wires],
            self.back_send.at[piece, 0], self.far_recv.at[piece, stage * place.near + turn],
            place.proxy,
        )

    def others(self, work):
        own = self.place.level * self.place.cell
        each(0, own, work)
        each(own + 1, self.place.near, work)

    def start(self):
        place = self.place

        @pl.when(place.inner)
        def _():
            self.meta_copy().start()
            for piece in range(PIECES):
                self.block_to(0, piece).start()

        for piece in range(PIECES):
            self.slots(piece, self.normed, self.meta, self.send_own)
            each(1, place.near, lambda distance: self.go_own(distance, piece).start())
        self.recv[0:LANE_ROWS, :] = self.send_own[rows_of(place.spot), :]

    def start_outer(self):
        place = self.place

        @pl.when(jnp.logical_not(place.inner))
        def _():
            self.meta_copy().start()
            for piece in range(PIECES):
                self.block_to(place.stage, piece).start()

    def relay(self, stage, piece):
        place = self.place

        @pl.when(place.inner)
        def _():
            if piece == 0:
                self.meta_from(stage).wait_recv()
            self.block_to(stage, piece).wait_recv()
            self.slots(piece, self.far_block.at[stage], self.far_meta.at[stage], self.send_far.at[stage])
            self.others(lambda turn: self.go_far(stage, turn, piece).start())
            slot = (place.near + stage * place.cell) * LANE_ROWS
            self.recv[slot:slot + LANE_ROWS, self.wires(piece)] = self.send_far[
                stage, rows_of(place.spot), self.wires(piece)
            ]

    def common(self):
        for load in self.loads[:3]:
            load.wait()
        gate = mm(self.normed[...], self.sg[...])
        hidden = (gate * jax.nn.sigmoid(gate) * mm(self.normed[...], self.su[...])).astype(BF16)
        step = self.width // 4
        for at in range(0, self.width, step):
            self.total[:, at:at + step] = mm(hidden, self.sd[:, at:at + step])
        for load in self.loads[3:]:
            load.wait()

    def serve(self, first, sources, arrive, leave):
        main_rows, tail_rows = sources * LANE_ROWS, sources * self.tail
        low, piece = first * LANE_ROWS, self.piece
        start = self.groups * main_rows
        rows = start + tail_rows
        recv, ysend, xc, hc, yc = self.recv, self.ysend, self.xc, self.hc, self.yc

        def select(part, transposed):
            shape = (main_rows, tail_rows) if transposed else (tail_rows, main_rows)
            axis = 1 if transposed else 0
            return as_weight(iota(shape, 1 - axis) == iota(shape, axis) * self.parts + part)

        for number in range(PIECES):
            arrive(number)
            at, to = number * self.wire, number * self.step
            for group in range(self.groups):
                xc[group * main_rows:(group + 1) * main_rows, to:to + self.step] = recv[
                    low:low + main_rows, at + group * self.step:at + (group + 1) * self.step
                ]
            for part in range(self.parts):
                xc[start:rows, to + part * piece:to + (part + 1) * piece] = mm(
                    select(part, False),
                    recv[low:low + main_rows, at + self.base:at + self.wire],
                ).astype(BF16)
            last = number == PIECES - 1

            @pl.loop(0, hc.shape[1] // 256)
            def _(turn):
                columns = pl.ds(pl.multiple_of(turn * 256, 256), 256)
                gate = mm(xc[:rows, to:to + self.step], self.wg[to:to + self.step, columns])
                up = mm(xc[:rows, to:to + self.step], self.wu[to:to + self.step, columns])
                if number:
                    gate = gate + self.gates[:rows, columns]
                    up = up + self.ups[:rows, columns]
                if last:
                    hc[:rows, columns] = (gate * jax.nn.sigmoid(gate) * up).astype(BF16)
                else:
                    self.gates[:rows, columns] = gate
                    self.ups[:rows, columns] = up

        for number in range(PIECES):
            at, to = number * self.wire, number * self.step

            @pl.loop(0, self.step // 256)
            def _(turn):
                columns = pl.ds(pl.multiple_of(to + turn * 256, 256), 256)
                yc[:rows, columns] = mm(hc[:rows, :], self.wd[:, columns]).astype(BF16)

            for group in range(self.groups):
                ysend[
                    low:low + main_rows, at + group * self.step:at + (group + 1) * self.step
                ] = yc[group * main_rows:(group + 1) * main_rows, to:to + self.step]
            total = jnp.zeros((main_rows, piece), F32)
            for part in range(self.parts):
                total = total + mm(
                    select(part, True),
                    yc[start:rows, to + part * piece:to + (part + 1) * piece],
                )
            ysend[low:low + main_rows, at + self.base:at + self.wire] = total.astype(BF16)
            leave(number)

    def serve_own(self):
        place = self.place

        def arrive(piece):
            with jax.named_scope("wait_own"):
                each(1, place.near, lambda distance: self.go_own(distance, piece).wait_recv())

        def leave(piece):
            if piece == 0:
                self.start_outer()

        self.serve(0, place.near, arrive, leave)

    def return_own(self, low, high):
        for piece in range(PIECES):
            each(low, high, lambda distance: self.back_own(distance, piece).start())

    def return_plane(self):
        place = self.place
        self.return_own(1, place.cell)
        self.ret_own[rows_of(place.spot), :] = self.ysend[0:LANE_ROWS, :]

    def return_planes(self, chosen):
        @pl.when(chosen)
        def _():
            self.return_own(self.place.cell, self.place.near)

    def serve_far(self, stage):
        place = self.place
        first = place.near + stage * place.cell

        def arrive(piece):
            with jax.named_scope("wait_far"):
                each(
                    place.low, place.cell,
                    lambda step: self.got_far(stage, step, piece).wait_recv(),
                )

        def leave(piece):
            each(place.low, place.cell, lambda step: self.back_far(stage, step, piece).start())

            @pl.when(place.inner)
            def _():
                self.ret_far[stage, rows_of(place.spot), self.wires(piece)] = self.ysend[
                    first * LANE_ROWS:(first + 1) * LANE_ROWS, self.wires(piece)
                ]

        self.serve(first, place.cell, arrive, leave)

    def mix(self, meta, ret, wait, store):
        turned = jnp.transpose(meta[...])[:self.tokens, :]
        whole = turned.astype(jnp.int32)
        mains, tails = self.keys(*[whole[:, row:row + 1] for row in range(4)])
        slot_lanes = iota((self.tokens, self.place.near * LANE_ROWS), 1)

        def mixing(first, second):
            values = jnp.where(slot_lanes == first, turned[:, 4:5], 0.0) + jnp.where(
                slot_lanes == second, turned[:, 5:6], 0.0
            )
            return halves(values)

        main_mix = [mixing(first, second) for first, second in mains]
        tail_mix = [
            mixing(tails[0] + part, tails[1] + part) for part in range(self.parts)
        ]
        for number in range(PIECES):
            wait(number)
            at, to = number * self.wire, number * self.step
            for part in range(self.parts):
                low, high = part * self.piece, (part + 1) * self.piece
                coarse, fine = tail_mix[part]
                values = ret[:, at + self.base:at + self.wire]
                total = mm(coarse, values) + mm(fine, values)
                for group, (coarse, fine) in enumerate(main_mix):
                    start = at + group * self.step
                    values = ret[:, start + low:start + high]
                    total = total + (mm(coarse, values) + mm(fine, values))
                store(number, to + low, to + high, total)

    def mix_own(self):
        place = self.place

        def wait(piece):
            with jax.named_scope("wait_back"):
                each(1, place.near, lambda distance: self.back_here(distance, piece).wait_recv())

        def store(number, low, high, value):
            self.total[:, low:high] = self.total[:, low:high] + value

        self.mix(self.meta, self.ret_own, wait, store)

    def mix_far(self, stage):
        @pl.when(self.place.inner)
        def _():
            def wait(piece):
                with jax.named_scope("wait_ret"):
                    self.others(lambda turn: self.returned_far(stage, turn, piece).wait_recv())

            def store(number, low, high, value):
                self.far_out[stage, :, low:high] = value.astype(BF16)
                if high == (number + 1) * self.step:
                    self.result_to(stage, number).start()

            self.mix(self.far_meta.at[stage], self.ret_far.at[stage], wait, store)

    def out_copy(self, piece):
        columns = self.columns(piece)
        return pltpu.make_async_copy(
            self.out.at[:, columns], self.out_ref.at[:, columns], self.out_sem.at[piece]
        )

    def close(self):
        place = self.place
        for piece in range(PIECES):
            with jax.named_scope("wait_result"):
                self.result_to(0, piece).wait_recv()
            columns = self.columns(piece)
            self.out[:, columns] = (
                self.total[:, columns] + self.far_in[:, columns].astype(F32)
            ).astype(BF16)
            self.out_copy(piece).start()
        self.meta_copy().wait_send()
        for piece in range(PIECES):
            self.block_to(0, piece).wait_send()
            each(1, place.near, lambda distance: self.go_own(distance, piece).wait_send())
            each(1, place.near, lambda distance: self.back_own(distance, piece).wait_send())
            for stage in range(place.depth):
                each(
                    place.low, place.cell,
                    lambda step: self.back_far(stage, step, piece).wait_send(),
                )

        @pl.when(place.inner)
        def _():
            for piece in range(PIECES):
                for stage in range(place.depth):
                    self.others(lambda turn: self.go_far(stage, turn, piece).wait_send())
                    self.result_to(stage, piece).wait_send()

        for piece in range(PIECES):
            self.out_copy(piece).wait()


STATE_ROWS = 8


def nt(left, right, precision=None):
    return lax.dot_general(
        left, right, (((1,), (1,)), ((), ())), precision=precision, preferred_element_type=F32
    )


def halves(value):
    high = value.astype(BF16)
    return high, (value - high.astype(F32)).astype(BF16)


def log_one_plus(small):
    series = small * (1.0 - small * (0.5 - small * (1.0 / 3.0 - small * 0.25)))
    return jnp.where(small < 0.01, series, jnp.log(1.0 + small))


def mixer_parts(place_at, ep_count, tp_count, refs):
    (q_hbm, k_hbm, v_hbm, in_ref, forget_ref, bias_ref, extra_ref, gate_hbm, gain_ref, wo_hbm,
     out_hbm, q_ref, k_ref, v_ref, gate_ref, out_ref, in_sem, out_sem, wo, locals_ref, state_send, state_recv, total_send, total_recv, total_ref,
     total_max, incoming, incoming_max, u_ref, squares_ref,
     u_recv, squares_recv, wo_sem, st_send, st_recv, tot_send, tot_recv, us_send, us_recv, sq_send, sq_recv) = refs
    exact = lax.Precision.HIGHEST
    heads, length = in_ref.shape
    blocks = length // BLK
    key_dim = q_ref.shape[1] // heads
    value_dim = v_ref.shape[1] // heads
    own_width = heads * value_dim
    scale = key_dim ** (-0.5)
    message = key_dim + STATE_ROWS
    share = length // tp_count
    share_blocks = share // BLK
    ep_at, tp_at = place_at.ep_at, place_at.tp_at
    load = pltpu.make_async_copy(wo_hbm, wo, wo_sem)

    def block_rows(ref, transform=lambda value, head: value):
        whole = ref[...]
        return jnp.concatenate(
            [
                transform(whole[head:head + 1, at * BLK:(at + 1) * BLK], head)
                for head in range(heads)
                for at in range(blocks)
            ],
            axis=0,
        )

    def key_block(head, at):
        return k_ref[at * BLK:(at + 1) * BLK, head * key_dim:(head + 1) * key_dim]

    def wide_values(head, at):
        values = v_ref[at * BLK:(at + 1) * BLK, head * value_dim:(head + 1) * value_dim]
        return jnp.concatenate([values, jnp.ones((BLK, value_dim), BF16)], axis=1)

    inputs = [
        pltpu.make_async_copy(source, target, in_sem.at[number])
        for number, (source, target) in enumerate(
            [(k_hbm, k_ref), (v_hbm, v_ref), (q_hbm, q_ref), (gate_hbm, gate_ref)]
        )
    ]

    def fetch():
        for copy in inputs:
            copy.start()

    def out_copy(at):
        rows = slice(at * BLK, (at + 1) * BLK)
        return pltpu.make_async_copy(
            out_ref.at[rows, :], out_hbm.at[rows, :], out_sem.at[at]
        )

    found = {}

    def grow(state, number):
        memory, top = state
        total = found["total"][number:number + 1, :]
        block_top = found["block_top"][number:number + 1, :]
        new_top = jnp.maximum(top + total, block_top)
        memory = jnp.exp(top + total - new_top) * memory + jnp.exp(
            block_top - new_top
        ) * locals_ref[number]
        return memory, new_top

    def diagonal():
        shape = (key_dim, value_dim)
        return iota(shape, 0) == iota(shape, 1)

    def early():
        load.start()
        for copy in inputs:
            copy.wait()
        logits = block_rows(forget_ref, lambda value, head: value + bias_ref[:, head:head + 1])
        kept = jnp.minimum(logits, 0.0) - log_one_plus(jnp.exp(-jnp.abs(logits)))
        kept = kept + block_rows(extra_ref)
        gates = block_rows(in_ref)
        upper = (iota((BLK, BLK), 0) <= iota((BLK, BLK), 1)).astype(F32)
        cumulative = jnp.dot(kept, upper, precision=exact, preferred_element_type=F32)
        total = cumulative[:, BLK - 1:BLK]
        gap = total - cumulative + gates
        block_top = jnp.max(gap, axis=1, keepdims=True)
        weight = jnp.exp(gap - block_top)
        found["total"], found["block_top"] = total, block_top
        found["cumulative"], found["shift"] = cumulative, gates - cumulative
        eye = (iota((key_dim, key_dim), 0) == iota((key_dim, key_dim), 1)).astype(F32).astype(BF16)
        for head in range(heads):
            state = (
                jnp.zeros((key_dim, 2 * value_dim), F32), jnp.full((1, 1), -1e30, F32)
            )
            decay = jnp.zeros((1, 1), F32)
            for at in range(blocks):
                number = head * blocks + at
                turned = nt(eye, key_block(head, at)) * weight[number:number + 1, :]
                high, low = halves(turned)
                values = wide_values(head, at)
                locals_ref[number] = mm(high, values) + mm(low, values)
                state = grow(state, number)
                decay = decay + total[number:number + 1, :]
            memory, top = state
            low_row = head * message
            state_send[low_row:low_row + key_dim, :] = memory[:, :value_dim]
            norm = jnp.sum(
                jnp.where(diagonal(), memory[:, value_dim:], 0.0), axis=0, keepdims=True
            )
            row = iota((STATE_ROWS, value_dim), 0)
            state_send[low_row + key_dim:low_row + message, :] = jnp.where(
                row == 0, norm, jnp.where(row == 1, top, decay)
            )

    span = place_at.depth * place_at.side
    own_at = lax.rem(ep_at, span)
    lower_half = place_at.half == 0

    def state_copy(distance, sign):
        at = lax.rem(own_at + sign * distance + span, span)
        return remote(
            state_send, state_recv.at[distance], st_send.at[distance], st_recv.at[distance],
            (place_at.half * span + at, tp_at),
        )

    low_inner = lower_half & place_at.inner
    first_inner = (place_at.depth - 1) * place_at.side

    def total_copy(stage):
        return remote(
            total_send, total_recv, tot_send.at[stage], tot_recv, place_at.beyond(stage)
        )

    def sends_to(distance):
        at = lax.rem(own_at + distance, span)
        return (own_at + distance < span) | (lower_half & (at >= first_inner))

    def takes_from(distance):
        return (own_at >= distance) | low_inner

    def u_copies(target, sender):
        place = pl.ds(pl.multiple_of(sender * own_width, own_width), own_width)
        return [
            remote(
                u_ref.at[target * share:(target + 1) * share, :], u_recv.at[:, place],
                us_send.at[target], us_recv.at[sender], (ep_at, target),
            ),
            remote(
                squares_ref.at[target], squares_recv.at[sender],
                sq_send.at[target], sq_recv.at[sender], (ep_at, target),
            ),
        ]

    def send_states():
        for distance in range(1, span):
            @pl.when(sends_to(distance))
            def _():
                state_copy(distance, 1).start()

    def absorb(memory_ref, max_ref, message_ref):
        for head in range(heads):
            low_row = head * message
            memory = message_ref[low_row:low_row + key_dim, :]
            extra = message_ref[low_row + key_dim:low_row + message, :]
            norm = jnp.sum(jnp.where(diagonal(), extra[0:1, :], 0.0), axis=1, keepdims=True)
            top, decay = extra[1:2, :], extra[2:3, :]
            old_top = max_ref[head, 0:1, :]
            new_top = jnp.maximum(old_top + decay, top)
            left = jnp.exp(old_top + decay - new_top)
            right = jnp.exp(top - new_top)
            memory_ref[head, :, :value_dim] = (
                left * memory_ref[head, :, :value_dim] + right * memory
            )
            memory_ref[head, :, value_dim:] = (
                left * memory_ref[head, :, value_dim:] + right * norm
            )
            max_ref[head] = jnp.broadcast_to(new_top, max_ref.shape[1:])

    def take_states():
        for distance in range(1, span):
            @pl.when(takes_from(distance))
            def _():
                state_copy(distance, 1).wait_recv()

        @pl.when(lower_half)
        def _():
            total_ref[...] = jnp.zeros_like(total_ref)
            total_max[...] = jnp.full_like(total_max, -1e30)
            for distance in range(span - 1, 0, -1):
                @pl.when(own_at >= distance)
                def _():
                    absorb(total_ref, total_max, state_recv.at[distance])
            incoming[...] = total_ref[...]
            incoming_max[...] = total_max[...]

        @pl.when(low_inner)
        def _():
            absorb(total_ref, total_max, state_send)
            for distance in range(span - 1, 0, -1):
                @pl.when(own_at < distance)
                def _():
                    absorb(total_ref, total_max, state_recv.at[distance])
            for head in range(heads):
                low_row = head * message
                total_send[low_row:low_row + key_dim, :] = total_ref[head, :, :value_dim]
                norm = jnp.sum(
                    jnp.where(diagonal(), total_ref[head, :, value_dim:], 0.0),
                    axis=0, keepdims=True,
                )
                row = iota((STATE_ROWS, value_dim), 0)
                total_send[low_row + key_dim:low_row + message, :] = jnp.where(
                    row == 0, norm, jnp.where(row == 1, total_max[head], 0.0)
                )
            for stage in range(place_at.depth):
                total_copy(stage).start()

    def take_total():
        @pl.when(jnp.logical_not(lower_half))
        def _():
            incoming[...] = jnp.zeros_like(incoming)
            incoming_max[...] = jnp.full_like(incoming_max, -1e30)
            total_copy(0).wait_recv()
            absorb(incoming, incoming_max, total_recv)
            for distance in range(span - 1, 0, -1):
                @pl.when(own_at >= distance)
                def _():
                    absorb(incoming, incoming_max, state_recv.at[distance])

    def walk(low_block, high_block):
        if low_block == 0:
            found["states"] = [
                (incoming[head], incoming_max[head, 0:1, 0:1]) for head in range(heads)
            ]
            found["columns"] = jnp.transpose(found["cumulative"])
        states, columns = found["states"], found["columns"]
        lower = iota((BLK, BLK), 0) >= iota((BLK, BLK), 1)
        ones = jnp.ones((STATE_ROWS, value_dim), F32)
        for at in range(low_block, high_block):
            squares = jnp.zeros((STATE_ROWS, BLK), F32)
            for head in range(heads):
                number = head * blocks + at
                memory, top = states[head]
                query = q_ref[at * BLK:(at + 1) * BLK, head * key_dim:(head + 1) * key_dim]
                column = columns[:, number:number + 1]
                gap = jnp.where(
                    lower, column + found["shift"][number:number + 1, :], -jnp.inf
                )
                carried = column + top
                stabilizer = jnp.maximum(carried, jnp.max(gap, axis=1, keepdims=True))
                scores = nt(query, key_block(head, at)) * scale * jnp.exp(gap - stabilizer)
                high, low = halves(scores)
                values = wide_values(head, at)
                sums = mm(high, values) + mm(low, values)
                high, low = halves(memory)
                sums = sums + (jnp.exp(carried - stabilizer) * scale) * (
                    mm(query, high) + mm(query, low)
                )
                hidden = sums[:, :value_dim] / jnp.maximum(
                    jnp.abs(sums[:, value_dim:]), jnp.exp(-stabilizer)
                )
                squares = squares + nt(ones, hidden * hidden, exact)
                place = slice(head * value_dim, (head + 1) * value_dim)
                gate = gate_ref[at * BLK:(at + 1) * BLK, place].astype(F32)
                u_ref[at * BLK:(at + 1) * BLK, place] = (
                    hidden * gain_ref[:, place] * jax.nn.sigmoid(gate)
                ).astype(BF16)
                states[head] = grow(states[head], number)
            squares_ref[at // share_blocks, at % share_blocks] = squares
            if at % share_blocks == share_blocks - 1:
                @pl.when(jnp.logical_not(place_at.inner))
                def _():
                    send_share(at // share_blocks)

    def send_share(target):
        @pl.when(tp_at != target)
        def _():
            for copy in u_copies(target, tp_at):
                copy.start()

        @pl.when(tp_at == target)
        def _():
            place = pl.ds(pl.multiple_of(tp_at * own_width, own_width), own_width)
            u_recv[:, place] = u_ref[target * share:(target + 1) * share, :]
            squares_recv[tp_at] = squares_ref[target]

    def send_u():
        @pl.when(place_at.inner)
        def _():
            for target in range(tp_count):
                send_share(target)

    def late():
        for sender in range(tp_count):
            @pl.when(tp_at != sender)
            def _():
                for copy in u_copies(0, sender):
                    copy.wait_recv()
        squares = squares_recv[0]
        for sender in range(1, tp_count):
            squares = squares + squares_recv[sender]
        inverse_row = lax.rsqrt(squares / (heads * tp_count * value_dim) + 1e-6)
        eye = (iota((BLK, BLK), 0) == iota((BLK, BLK), 1)).astype(F32)
        load.wait()
        width = wo.shape[1]
        for at in range(share_blocks):
            inverse = nt(eye, inverse_row[at], exact)[:, 0:1]

            @pl.loop(0, width // 512)
            def _(turn):
                place = pl.ds(pl.multiple_of(turn * 512, 512), 512)
                product = mm(u_recv[at * BLK:(at + 1) * BLK, :], wo[:, place])
                out_ref[at * BLK:(at + 1) * BLK, place] = (product * inverse).astype(BF16)

            out_copy(at).start()


    def close():
        for at in range(share_blocks):
            out_copy(at).wait()
        for distance in range(1, span):
            @pl.when(sends_to(distance))
            def _():
                state_copy(distance, 1).wait_send()

        @pl.when(low_inner)
        def _():
            for stage in range(place_at.depth):
                total_copy(stage).wait_send()

        for target in range(tp_count):
            @pl.when(tp_at != target)
            def _():
                for copy in u_copies(target, tp_at):
                    copy.wait_send()

    return fetch, early, send_u, send_states, take_states, take_total, walk, late, close


def on_device(
    queries,
    head_key_rows,
    head_value_rows,
    log_input_gate,
    forget_logits,
    head_forget_bias,
    extra_log_forget,
    output_gate_logits,
    head_norm_gain,
    mixer_output_weight,
    second_batch_input,
    expert_norm_gain,
    routed_expert_index,
    routed_copy_weight,
    routed_gate_weight,
    routed_up_weight,
    routed_down_weight,
    shared_gate_weight,
    shared_up_weight,
    shared_down_weight,
):
    tokens, width = second_batch_input.shape
    ep_count = lax.axis_size("ep")
    tp_count = lax.axis_size("tp")
    count = ep_count * tp_count
    top_count = routed_expert_index.shape[1]
    capacity = max(2, 3 * tokens * top_count // (2 * count))
    groups = capacity // LANE_ROWS
    step = width // PIECES
    wire = PIECES * (groups * step + step * (capacity - groups * LANE_ROWS) // LANE_ROWS)
    side = max(1, tp_count // CORES)
    near = count // 2
    span = ep_count // 2
    depth = ep_count // side // 2
    rows = near * capacity
    padded = -(-tokens // 128) * 128
    hidden_width = routed_gate_weight.shape[2]
    length = queries.shape[0]
    heads = head_forget_bias.shape[0]
    key_dim = queries.shape[1] // heads
    value_dim = head_value_rows.shape[1] // heads
    blocks = length // BLK
    share = length // tp_count
    dma = pltpu.SemaphoreType.DMA
    vmem = pl.BlockSpec(memory_space=pltpu.VMEM)
    hbm = pl.BlockSpec(memory_space=pl.ANY)

    block = pltpu.VMEM((tokens, width), BF16)
    meta = pltpu.VMEM((STATE_ROWS, padded), F32)
    half_slots = pltpu.VMEM((near * LANE_ROWS, wire), BF16)
    far_slots = pltpu.VMEM((depth, near * LANE_ROWS, wire), BF16)
    far_block = pltpu.VMEM((depth, tokens, width), BF16)
    slots = pltpu.VMEM((2 * near * LANE_ROWS, wire), BF16)
    moe_scratch = (
        [block, meta, far_block, pltpu.VMEM((depth, STATE_ROWS, padded), F32)]
        + [half_slots, far_slots, slots, slots, half_slots, far_slots]
        + [far_block, block]
        + [
            pltpu.VMEM(array.shape[-2:], BF16)
            for array in (
                routed_gate_weight, routed_up_weight, routed_down_weight,
                shared_gate_weight, shared_up_weight, shared_down_weight,
            )
        ]
        + [
            pltpu.VMEM((rows, width), BF16),
            pltpu.VMEM((rows, hidden_width), BF16),
            pltpu.VMEM((rows, width), BF16),
            pltpu.VMEM((rows, hidden_width), F32),
            pltpu.VMEM((rows, hidden_width), F32),
            pltpu.VMEM((tokens, width), F32),
            block,
            dma((6,)), dma((PIECES, near)), dma((PIECES, count)), dma((PIECES, depth * near)),
            dma((PIECES, count)), dma((PIECES, near)), dma((PIECES, depth * near)),
            dma((PIECES,)), dma((depth, PIECES)), dma((depth, PIECES)), dma((PIECES,)),
            dma, dma((depth,)), dma((PIECES,)),
        ]
    )
    message = heads * (key_dim + STATE_ROWS)
    mixer_scratch = [
        *[
            pltpu.VMEM(array.shape, BF16)
            for array in (queries, head_key_rows, head_value_rows, output_gate_logits)
        ],
        pltpu.VMEM((share, width), BF16), dma((4,)), dma((share // BLK,)),
        pltpu.VMEM(mixer_output_weight.shape, BF16),
        pltpu.VMEM((heads * blocks, key_dim, 2 * value_dim), F32),
        pltpu.VMEM((message, value_dim), F32),
        pltpu.VMEM((span, message, value_dim), F32),
        pltpu.VMEM((message, value_dim), F32),
        pltpu.VMEM((message, value_dim), F32),
        pltpu.VMEM((heads, key_dim, 2 * value_dim), F32),
        pltpu.VMEM((heads, STATE_ROWS, value_dim), F32),
        pltpu.VMEM((heads, key_dim, 2 * value_dim), F32),
        pltpu.VMEM((heads, STATE_ROWS, value_dim), F32),
        pltpu.VMEM((length, heads * value_dim), BF16),
        pltpu.VMEM((tp_count, share // BLK, STATE_ROWS, BLK), F32),
        pltpu.VMEM((share, tp_count * heads * value_dim), BF16),
        pltpu.VMEM((tp_count, share // BLK, STATE_ROWS, BLK), F32),
        dma, dma((span,)), dma((span,)), dma((depth,)), dma,
        dma((tp_count,)), dma((tp_count,)), dma((tp_count,)), dma((tp_count,)),
    ]

    def kernel(*refs):
        mixer_in, moe_in = refs[:10], refs[10:20]
        mixer_out, moe_out = refs[20], refs[21]
        scratch = refs[22:]
        cut = len(moe_scratch)
        place = Place(ep_count, tp_count)
        fetch, early, send_u, send_states, take_states, take_total, walk, late, close = mixer_parts(
            place, ep_count, tp_count, (*mixer_in, mixer_out, *scratch[cut:])
        )
        experts = Experts(place, capacity, (*moe_in, moe_out, *scratch[:cut]))
        depth = place.depth
        fetch()
        experts.open()
        experts.meet()
        experts.start()
        early()
        send_states()
        experts.common()
        for piece in range(PIECES):
            experts.relay(0, piece)
        experts.serve_own()
        experts.return_plane()
        for stage in range(depth):
            if stage + 1 < depth:
                experts.relay(stage + 1, 0)
            experts.serve_far(stage)
            if stage + 1 < depth:
                for piece in range(1, PIECES):
                    experts.relay(stage + 1, piece)
            else:
                experts.return_planes(jnp.logical_not(place.inner))
            if stage == 0:
                experts.return_planes(place.inner)
                take_states()
                take_total()
            walk(blocks * stage // depth, blocks * (stage + 1) // depth)
            experts.mix_far(stage)
        send_u()
        experts.mix_own()
        late()
        experts.close()
        close()

    return pl.pallas_call(
        kernel,
        out_shape=(
            jax.ShapeDtypeStruct((share, width), BF16),
            jax.ShapeDtypeStruct((tokens, width), BF16),
        ),
        in_specs=[hbm] * 3 + [vmem] * 4 + [hbm, vmem, hbm] + [vmem] * 4 + [hbm] * 6,
        out_specs=(hbm, hbm),
        scratch_shapes=moe_scratch + mixer_scratch,
        compiler_params=pltpu.CompilerParams(
            collective_id=0, has_side_effects=True, vmem_limit_bytes=62 * 1024 * 1024
        ),
        name="both",
    )(
        queries, head_key_rows, head_value_rows, log_input_gate.T, forget_logits.T,
        head_forget_bias[None, :], extra_log_forget.T, output_gate_logits,
        head_norm_gain[None, :], mixer_output_weight,
        second_batch_input, expert_norm_gain[None, :], routed_expert_index.T,
        routed_copy_weight.T, routed_gate_weight, routed_up_weight,
        routed_down_weight, shared_gate_weight, shared_up_weight, shared_down_weight,
    )


def solution(mesh):
    in_specs = (
        P("ep", "tp"),
        P("ep", "tp"),
        P("ep", "tp"),
        P("ep", "tp"),
        P("ep", "tp"),
        P("tp"),
        P("ep", "tp"),
        P("ep", "tp"),
        P("tp"),
        P(),
        P(("ep", "tp"), None),
        P(),
        P(("ep", "tp"), None),
        P(("ep", "tp"), None),
        P(("ep", "tp"), None, None),
        P(("ep", "tp"), None, None),
        P(("ep", "tp"), None, None),
        P(),
        P(),
        P(),
    )
    out_specs = (P(("ep", "tp"), None), P(("ep", "tp"), None))
    return jax.shard_map(
        on_device, mesh=mesh, in_specs=in_specs, out_specs=out_specs, check_vma=False
    )
```

```python
import jax
import jax.numpy as jnp
from jax import lax
from jax.experimental import pallas as pl
from jax.experimental.pallas import tpu as pltpu
from jax.sharding import PartitionSpec as P

BLK = 128


F32 = jnp.float32
BF16 = jnp.bfloat16
LANE_ROWS = 16
CORES = 2
PIECES = 2


def mm(left, right):
    return jnp.dot(left, right, preferred_element_type=F32)


def iota(shape, axis):
    return lax.broadcasted_iota(jnp.int32, shape, axis)


class Place:
    def __init__(self, ep_count, tp_count):
        self.side = max(1, tp_count // CORES)
        self.tp_count = tp_count
        self.planes = ep_count // self.side
        self.depth = self.planes // 2
        self.cell = self.side * tp_count
        self.near = self.depth * self.cell
        self.ep_at = lax.axis_index("ep")
        self.tp_at = lax.axis_index("tp")
        plane = self.ep_at // self.side
        self.row = lax.rem(self.ep_at, self.side)
        self.half = plane // self.depth
        self.level = plane - self.half * self.depth
        self.stage = self.half * self.level + (1 - self.half) * (self.depth - 1 - self.level)
        self.spot = self.level * self.cell + self.row * tp_count + self.tp_at
        self.inner = self.stage == 0
        self.low = jnp.where(self.inner, 1, 0)
        self.proxy = self.beyond(0)

    def at(self, level, row, tp):
        device = ((self.half * self.depth + level) * self.side + row, tp)
        return device, level * self.cell + row * self.tp_count + tp

    def across(self, step, sign):
        row_step, tp_step = step // self.tp_count, lax.rem(step, self.tp_count)
        row = lax.rem(self.row + sign * row_step + self.side, self.side)
        tp = lax.rem(self.tp_at + sign * tp_step + self.tp_count, self.tp_count)
        return row, tp

    def away(self, distance, sign):
        level_step = distance // self.cell
        level = lax.rem(self.level + sign * level_step + self.depth, self.depth)
        return self.at(level, *self.across(lax.rem(distance, self.cell), sign))

    def beyond(self, stage):
        plane = (1 - self.half) * (self.depth + stage) + self.half * (self.depth - 1 - stage)
        return plane * self.side + self.row, self.tp_at


def each(low, high, work):
    def turn(step, carry):
        work(step)
        return carry

    lax.fori_loop(low, high, turn, 0)


def rows_of(index):
    return pl.ds(pl.multiple_of(index * LANE_ROWS, LANE_ROWS), LANE_ROWS)


def remote(source, target, send_sem, recv_sem, device):
    return pltpu.make_async_remote_copy(
        src_ref=source, dst_ref=target, send_sem=send_sem, recv_sem=recv_sem,
        device_id=device, device_id_type=pl.DeviceIdType.MESH,
    )


def as_weight(mask):
    return mask.astype(F32).astype(BF16)


class Experts:
    def __init__(self, place, capacity, refs):
        (self.x_ref, self.gain_ref, self.idx_ref, self.weight_ref, wg_hbm, wu_hbm, wd_hbm, sg_hbm,
         su_hbm, sd_hbm, self.out_ref, self.normed, self.meta, self.far_block, self.far_meta,
         self.send_own, self.send_far, self.recv, self.ysend, self.ret_own, self.ret_far,
         self.far_out, self.far_in, self.wg, self.wu, self.wd, self.sg, self.su, self.sd, self.xc,
         self.hc, self.yc, self.gates, self.ups, self.total, self.out, load_sem, self.go_send, self.go_recv, self.far_send,
         self.far_got, self.far_back, self.back_send, self.back_recv, self.far_recv, self.over_send, self.over_recv,
         self.result_send, self.result_recv, self.meta_send, self.meta_recv, self.out_sem) = refs
        self.place = place
        self.tokens, self.width = self.x_ref.shape
        self.step = self.width // PIECES
        self.groups = capacity // LANE_ROWS
        self.tail = capacity - self.groups * LANE_ROWS
        self.parts = LANE_ROWS // self.tail
        self.piece = self.step // self.parts
        self.base = self.groups * self.step
        self.wire = self.base + self.piece
        self.loads = [
            pltpu.make_async_copy(source, target, load_sem.at[number])
            for number, (source, target) in enumerate(
                [(sg_hbm, self.sg), (su_hbm, self.su), (sd_hbm, self.sd),
                 (wg_hbm.at[0], self.wg), (wu_hbm.at[0], self.wu), (wd_hbm.at[0], self.wd)]
            )
        ]

    def open(self):
        place, tokens = self.place, self.tokens
        for load in self.loads:
            load.start()
        barrier = pltpu.get_barrier_semaphore()

        def greet(device):
            pl.semaphore_signal(
                barrier, inc=1, device_id=device, device_id_type=pl.DeviceIdType.MESH
            )

        each(1, place.near, lambda distance: greet(place.away(distance, 1)[0]))
        greet(place.proxy)

        @pl.when(place.inner)
        def _():
            for stage in range(1, place.depth):
                greet(place.beyond(stage))

        floats = self.x_ref[...].astype(F32)
        inverse = lax.rsqrt(jnp.mean(floats * floats, axis=1, keepdims=True) + 1e-6)
        self.normed[...] = (floats * inverse * self.gain_ref[...]).astype(BF16)

        expert_rows = iota((2 * place.near, tokens), 0)
        first, second = self.idx_ref[0:1, :], self.idx_ref[1:2, :]
        hit_first = expert_rows == first
        hit_second = expert_rows == second
        named = as_weight(hit_first | hit_second)
        before = as_weight(iota((tokens, tokens), 0) < iota((tokens, tokens), 1))
        earlier = mm(named, before)
        self.meta[...] = jnp.zeros_like(self.meta)
        self.meta[0:1, :tokens] = first.astype(F32)
        self.meta[1:2, :tokens] = second.astype(F32)
        self.meta[2:3, :tokens] = jnp.sum(jnp.where(hit_first, earlier, 0.0), axis=0, keepdims=True)
        self.meta[3:4, :tokens] = jnp.sum(
            jnp.where(hit_second, earlier, 0.0), axis=0, keepdims=True
        )
        self.meta[4:6, :tokens] = self.weight_ref[...]
    def meet(self):
        place = self.place
        pl.semaphore_wait(
            pltpu.get_barrier_semaphore(), place.near - 1 + jnp.where(place.inner, place.depth, 1)
        )

    def keys(self, first, second, place_first, place_second):
        near, low = self.place.near, self.place.half * self.place.near

        def main(expert, place, group):
            local, near_expert = place - group * LANE_ROWS, expert - low
            inside = (near_expert >= 0) & (near_expert < near)
            inside = inside & (local >= 0) & (local < LANE_ROWS)
            return jnp.where(inside, near_expert * LANE_ROWS + local, -LANE_ROWS)

        def tail(expert, place):
            local, near_expert = place - self.groups * LANE_ROWS, expert - low
            inside = (near_expert >= 0) & (near_expert < near) & (local >= 0)
            return jnp.where(inside, near_expert * LANE_ROWS + local * self.parts, -LANE_ROWS)

        mains = [
            (main(first, place_first, group), main(second, place_second, group))
            for group in range(self.groups)
        ]
        return mains, (tail(first, place_first), tail(second, place_second))

    def slots(self, piece, block, meta, send):
        whole = meta[:, :self.tokens].astype(jnp.int32)
        mains, tails = self.keys(*[whole[row:row + 1, :] for row in range(4)])
        slot_rows = iota((self.place.near * LANE_ROWS, self.tokens), 0)
        low, to = piece * self.step, piece * self.wire
        step = self.step // 2
        for group, (first, second) in enumerate(mains):
            pick = as_weight((slot_rows == first) | (slot_rows == second))
            for at in range(0, self.step, step):
                start = to + group * self.step + at
                send[:, start:start + step] = mm(
                    pick, block[:, low + at:low + at + step]
                ).astype(BF16)
        total = jnp.zeros((self.place.near * LANE_ROWS, self.piece), F32)
        for part in range(self.parts):
            pick = as_weight((slot_rows == tails[0] + part) | (slot_rows == tails[1] + part))
            at = low + part * self.piece
            total = total + mm(pick, block[:, at:at + self.piece])
        send[:, to + self.base:to + self.wire] = total.astype(BF16)

    def columns(self, piece):
        return slice(piece * self.step, (piece + 1) * self.step)

    def wires(self, piece):
        return slice(piece * self.wire, (piece + 1) * self.wire)

    def meta_copy(self):
        return remote(
            self.meta, self.far_meta.at[self.place.stage], self.meta_send,
            self.meta_recv.at[self.place.stage], self.place.proxy,
        )

    def meta_from(self, stage):
        return remote(
            self.meta, self.far_meta.at[stage], self.meta_send, self.meta_recv.at[stage],
            self.place.proxy,
        )

    def block_to(self, stage, piece):
        columns = self.columns(piece)
        return remote(
            self.normed.at[:, columns], self.far_block.at[stage, :, columns],
            self.over_send, self.over_recv.at[stage, piece], self.place.proxy,
        )

    def result_to(self, stage, piece):
        columns = self.columns(piece)
        return remote(
            self.far_out.at[stage, :, columns], self.far_in.at[:, columns],
            self.result_send, self.result_recv.at[piece],
            self.place.beyond(stage),
        )

    def go_own(self, distance, piece):
        device, spot = self.place.away(distance, 1)
        wires = self.wires(piece)
        return remote(
            self.send_own.at[rows_of(spot), wires], self.recv.at[rows_of(distance), wires],
            self.go_send, self.go_recv.at[piece], device,
        )

    def back_own(self, distance, piece):
        device, _ = self.place.away(distance, -1)
        wires = self.wires(piece)
        return remote(
            self.ysend.at[rows_of(distance), wires],
            self.ret_own.at[rows_of(self.place.spot), wires],
            self.back_send, self.back_recv.at[piece], device,
        )

    def all_of(self, source, target, send_sem, recv_sem):
        return remote(source, target, send_sem, recv_sem, self.place.proxy)

    def go_far(self, stage, turn, piece):
        place = self.place
        level, step = turn // place.cell, lax.rem(turn, place.cell)
        device, spot = place.at(level, *place.across(step, 1))
        slot = place.near + stage * place.cell + step
        wires = self.wires(piece)
        return remote(
            self.send_far.at[stage, rows_of(spot), wires], self.recv.at[rows_of(slot), wires],
            self.far_send, self.far_got.at[stage, piece], device,
        )

    def back_far(self, stage, step, piece):
        place = self.place
        level = (1 - place.half) * (place.depth - 1)
        device, _ = place.at(level, *place.across(step, -1))
        slot = place.near + stage * place.cell + step
        wires = self.wires(piece)
        return remote(
            self.ysend.at[rows_of(slot), wires],
            self.ret_far.at[stage, rows_of(place.spot), wires],
            self.far_back, self.far_recv.at[stage, piece], device,
        )

    def others(self, work):
        own = self.place.level * self.place.cell
        each(0, own, work)
        each(own + 1, self.place.near, work)

    def start(self):
        place = self.place

        @pl.when(place.inner)
        def _():
            self.meta_copy().start()
            for piece in range(PIECES):
                self.block_to(0, piece).start()

        for piece in range(PIECES):
            self.slots(piece, self.normed, self.meta, self.send_own)
            each(1, place.near, lambda distance: self.go_own(distance, piece).start())
        self.recv[0:LANE_ROWS, :] = self.send_own[rows_of(place.spot), :]

    def start_outer(self):
        place = self.place

        @pl.when(jnp.logical_not(place.inner))
        def _():
            self.meta_copy().start()
            for piece in range(PIECES):
                self.block_to(place.stage, piece).start()

    def relay(self, stage, piece):
        place = self.place

        @pl.when(place.inner)
        def _():
            if piece == 0:
                self.meta_from(stage).wait_recv()
            self.block_to(stage, piece).wait_recv()
            self.slots(piece, self.far_block.at[stage], self.far_meta.at[stage], self.send_far.at[stage])
            self.others(lambda turn: self.go_far(stage, turn, piece).start())
            slot = (place.near + stage * place.cell) * LANE_ROWS
            self.recv[slot:slot + LANE_ROWS, self.wires(piece)] = self.send_far[
                stage, rows_of(place.spot), self.wires(piece)
            ]

    def common(self):
        for load in self.loads[:3]:
            load.wait()
        gate = mm(self.normed[...], self.sg[...])
        hidden = (gate * jax.nn.sigmoid(gate) * mm(self.normed[...], self.su[...])).astype(BF16)
        step = self.width // 4
        for at in range(0, self.width, step):
            self.total[:, at:at + step] = mm(hidden, self.sd[:, at:at + step])
        for load in self.loads[3:]:
            load.wait()

    def serve(self, first, sources, arrive, leave):
        main_rows, tail_rows = sources * LANE_ROWS, sources * self.tail
        low, piece = first * LANE_ROWS, self.piece
        start = self.groups * main_rows
        rows = start + tail_rows
        recv, ysend, xc, hc, yc = self.recv, self.ysend, self.xc, self.hc, self.yc

        def select(part, transposed):
            shape = (main_rows, tail_rows) if transposed else (tail_rows, main_rows)
            axis = 1 if transposed else 0
            return as_weight(iota(shape, 1 - axis) == iota(shape, axis) * self.parts + part)

        for number in range(PIECES):
            arrive(number)
            at, to = number * self.wire, number * self.step
            for group in range(self.groups):
                xc[group * main_rows:(group + 1) * main_rows, to:to + self.step] = recv[
                    low:low + main_rows, at + group * self.step:at + (group + 1) * self.step
                ]
            for part in range(self.parts):
                xc[start:rows, to + part * piece:to + (part + 1) * piece] = mm(
                    select(part, False),
                    recv[low:low + main_rows, at + self.base:at + self.wire],
                ).astype(BF16)
            last = number == PIECES - 1

            @pl.loop(0, hc.shape[1] // 256)
            def _(turn):
                columns = pl.ds(pl.multiple_of(turn * 256, 256), 256)
                gate = mm(xc[:rows, to:to + self.step], self.wg[to:to + self.step, columns])
                up = mm(xc[:rows, to:to + self.step], self.wu[to:to + self.step, columns])
                if number:
                    gate = gate + self.gates[:rows, columns]
                    up = up + self.ups[:rows, columns]
                if last:
                    hc[:rows, columns] = (gate * jax.nn.sigmoid(gate) * up).astype(BF16)
                else:
                    self.gates[:rows, columns] = gate
                    self.ups[:rows, columns] = up

        for number in range(PIECES):
            at, to = number * self.wire, number * self.step

            @pl.loop(0, self.step // 256)
            def _(turn):
                columns = pl.ds(pl.multiple_of(to + turn * 256, 256), 256)
                yc[:rows, columns] = mm(hc[:rows, :], self.wd[:, columns]).astype(BF16)

            for group in range(self.groups):
                ysend[
                    low:low + main_rows, at + group * self.step:at + (group + 1) * self.step
                ] = yc[group * main_rows:(group + 1) * main_rows, to:to + self.step]
            total = jnp.zeros((main_rows, piece), F32)
            for part in range(self.parts):
                total = total + mm(
                    select(part, True),
                    yc[start:rows, to + part * piece:to + (part + 1) * piece],
                )
            ysend[low:low + main_rows, at + self.base:at + self.wire] = total.astype(BF16)
            leave(number)

    def serve_own(self):
        place = self.place

        def arrive(piece):
            with jax.named_scope("wait_own"):
                region = self.recv.at[LANE_ROWS:place.near * LANE_ROWS, self.wires(piece)]
                self.all_of(region, region, self.go_send, self.go_recv.at[piece]).wait_recv()

        def leave(piece):
            if piece == 0:
                self.start_outer()

        self.serve(0, place.near, arrive, leave)

    def return_own(self, low, high):
        for piece in range(PIECES):
            each(low, high, lambda distance: self.back_own(distance, piece).start())

    def return_plane(self):
        place = self.place
        self.return_own(1, place.cell)
        self.ret_own[rows_of(place.spot), :] = self.ysend[0:LANE_ROWS, :]

    def return_planes(self, chosen):
        @pl.when(chosen)
        def _():
            self.return_own(self.place.cell, self.place.near)

    def serve_far(self, stage):
        place = self.place
        first = place.near + stage * place.cell

        def arrive(piece):
            with jax.named_scope("wait_far"):
                for inner, count in ((True, place.cell - 1), (False, place.cell)):
                    @pl.when(place.inner == inner)
                    def _():
                        end = (first + place.cell) * LANE_ROWS
                        region = self.recv.at[end - count * LANE_ROWS:end, self.wires(piece)]
                        self.all_of(
                            region, region, self.far_send, self.far_got.at[stage, piece]
                        ).wait_recv()

        def leave(piece):
            each(place.low, place.cell, lambda step: self.back_far(stage, step, piece).start())

            @pl.when(place.inner)
            def _():
                self.ret_far[stage, rows_of(place.spot), self.wires(piece)] = self.ysend[
                    first * LANE_ROWS:(first + 1) * LANE_ROWS, self.wires(piece)
                ]

        self.serve(first, place.cell, arrive, leave)

    def mix(self, meta, ret, wait, store):
        turned = jnp.transpose(meta[...])[:self.tokens, :]
        whole = turned.astype(jnp.int32)
        mains, tails = self.keys(*[whole[:, row:row + 1] for row in range(4)])
        slot_lanes = iota((self.tokens, self.place.near * LANE_ROWS), 1)

        def mixing(first, second):
            values = jnp.where(slot_lanes == first, turned[:, 4:5], 0.0) + jnp.where(
                slot_lanes == second, turned[:, 5:6], 0.0
            )
            return halves(values)

        main_mix = [mixing(first, second) for first, second in mains]
        tail_mix = [
            mixing(tails[0] + part, tails[1] + part) for part in range(self.parts)
        ]
        for number in range(PIECES):
            wait(number)
            at, to = number * self.wire, number * self.step
            for part in range(self.parts):
                low, high = part * self.piece, (part + 1) * self.piece
                coarse, fine = tail_mix[part]
                values = ret[:, at + self.base:at + self.wire]
                total = mm(coarse, values) + mm(fine, values)
                for group, (coarse, fine) in enumerate(main_mix):
                    start = at + group * self.step
                    values = ret[:, start + low:start + high]
                    total = total + (mm(coarse, values) + mm(fine, values))
                store(number, to + low, to + high, total)

    def mix_own(self):
        place = self.place

        def wait(piece):
            with jax.named_scope("wait_back"):
                region = self.ret_own.at[LANE_ROWS:place.near * LANE_ROWS, self.wires(piece)]
                self.all_of(region, region, self.back_send, self.back_recv.at[piece]).wait_recv()

        def store(number, low, high, value):
            self.total[:, low:high] = self.total[:, low:high] + value

        self.mix(self.meta, self.ret_own, wait, store)

    def mix_far(self, stage):
        @pl.when(self.place.inner)
        def _():
            def wait(piece):
                with jax.named_scope("wait_ret"):
                    region = self.ret_far.at[
                        stage, LANE_ROWS:self.place.near * LANE_ROWS, self.wires(piece)
                    ]
                    self.all_of(
                        region, region, self.far_back, self.far_recv.at[stage, piece]
                    ).wait_recv()

            def store(number, low, high, value):
                self.far_out[stage, :, low:high] = value.astype(BF16)
                if high == (number + 1) * self.step:
                    self.result_to(stage, number).start()

            self.mix(self.far_meta.at[stage], self.ret_far.at[stage], wait, store)

    def out_copy(self, piece):
        columns = self.columns(piece)
        return pltpu.make_async_copy(
            self.out.at[:, columns], self.out_ref.at[:, columns], self.out_sem.at[piece]
        )

    def close(self):
        place = self.place
        for piece in range(PIECES):
            with jax.named_scope("wait_result"):
                self.result_to(0, piece).wait_recv()
            columns = self.columns(piece)
            self.out[:, columns] = (
                self.total[:, columns] + self.far_in[:, columns].astype(F32)
            ).astype(BF16)
            self.out_copy(piece).start()
        def sent(region, sem, other):
            self.all_of(region, region, sem, other).wait_send()

        others = (place.near - 1) * LANE_ROWS
        self.meta_copy().wait_send()
        sent(self.normed, self.over_send, self.over_recv.at[0, 0])
        sent(self.send_own.at[:others, :], self.go_send, self.go_recv.at[0])
        sent(self.ysend.at[:others, :], self.back_send, self.back_recv.at[0])
        for inner, count in ((True, place.cell - 1), (False, place.cell)):
            @pl.when(place.inner == inner)
            def _():
                rows = place.depth * count * LANE_ROWS
                sent(self.ysend.at[:rows, :], self.far_back, self.far_recv.at[0, 0])

        @pl.when(place.inner)
        def _():
            sent(self.send_far.at[:, :others, :], self.far_send, self.far_got.at[0, 0])
            sent(self.far_out, self.result_send, self.result_recv.at[0])

        for piece in range(PIECES):
            self.out_copy(piece).wait()


STATE_ROWS = 8


def nt(left, right, precision=None):
    return lax.dot_general(
        left, right, (((1,), (1,)), ((), ())), precision=precision, preferred_element_type=F32
    )


def halves(value):
    high = value.astype(BF16)
    return high, (value - high.astype(F32)).astype(BF16)


def log_one_plus(small):
    series = small * (1.0 - small * (0.5 - small * (1.0 / 3.0 - small * 0.25)))
    return jnp.where(small < 0.01, series, jnp.log(1.0 + small))


def mixer_parts(place_at, ep_count, tp_count, refs):
    (q_hbm, k_hbm, v_hbm, in_ref, forget_ref, bias_ref, extra_ref, gate_hbm, gain_ref, wo_hbm,
     out_hbm, q_ref, k_ref, v_ref, gate_ref, out_ref, in_sem, out_sem, wo, locals_ref, state_send, state_recv, total_send, total_recv, total_ref,
     total_max, incoming, incoming_max, u_ref, squares_ref,
     u_recv, squares_recv, wo_sem, st_send, st_recv, tot_send, tot_recv, us_send, us_recv, sq_send, sq_recv) = refs
    exact = lax.Precision.HIGHEST
    heads, length = in_ref.shape
    blocks = length // BLK
    key_dim = q_ref.shape[1] // heads
    value_dim = v_ref.shape[1] // heads
    own_width = heads * value_dim
    scale = key_dim ** (-0.5)
    message = key_dim + STATE_ROWS
    share = length // tp_count
    share_blocks = share // BLK
    ep_at, tp_at = place_at.ep_at, place_at.tp_at
    load = pltpu.make_async_copy(wo_hbm, wo, wo_sem)

    def block_rows(ref, transform=lambda value, head: value):
        whole = ref[...]
        return jnp.concatenate(
            [
                transform(whole[head:head + 1, at * BLK:(at + 1) * BLK], head)
                for head in range(heads)
                for at in range(blocks)
            ],
            axis=0,
        )

    def key_block(head, at):
        return k_ref[at * BLK:(at + 1) * BLK, head * key_dim:(head + 1) * key_dim]

    def wide_values(head, at):
        values = v_ref[at * BLK:(at + 1) * BLK, head * value_dim:(head + 1) * value_dim]
        return jnp.concatenate([values, jnp.ones((BLK, value_dim), BF16)], axis=1)

    inputs = [
        pltpu.make_async_copy(source, target, in_sem.at[number])
        for number, (source, target) in enumerate(
            [(k_hbm, k_ref), (v_hbm, v_ref), (q_hbm, q_ref), (gate_hbm, gate_ref)]
        )
    ]

    def fetch():
        for copy in inputs:
            copy.start()

    def out_copy(at):
        rows = slice(at * BLK, (at + 1) * BLK)
        return pltpu.make_async_copy(
            out_ref.at[rows, :], out_hbm.at[rows, :], out_sem.at[at]
        )

    found = {}

    def grow(state, number):
        memory, top = state
        total = found["total"][number:number + 1, :]
        block_top = found["block_top"][number:number + 1, :]
        new_top = jnp.maximum(top + total, block_top)
        memory = jnp.exp(top + total - new_top) * memory + jnp.exp(
            block_top - new_top
        ) * locals_ref[number]
        return memory, new_top

    def diagonal():
        shape = (key_dim, value_dim)
        return iota(shape, 0) == iota(shape, 1)

    def early():
        load.start()
        for copy in inputs:
            copy.wait()
        logits = block_rows(forget_ref, lambda value, head: value + bias_ref[:, head:head + 1])
        kept = jnp.minimum(logits, 0.0) - log_one_plus(jnp.exp(-jnp.abs(logits)))
        kept = kept + block_rows(extra_ref)
        gates = block_rows(in_ref)
        upper = (iota((BLK, BLK), 0) <= iota((BLK, BLK), 1)).astype(F32)
        cumulative = jnp.dot(kept, upper, precision=exact, preferred_element_type=F32)
        total = cumulative[:, BLK - 1:BLK]
        gap = total - cumulative + gates
        block_top = jnp.max(gap, axis=1, keepdims=True)
        weight = jnp.exp(gap - block_top)
        found["total"], found["block_top"] = total, block_top
        found["cumulative"], found["shift"] = cumulative, gates - cumulative
        eye = (iota((key_dim, key_dim), 0) == iota((key_dim, key_dim), 1)).astype(F32).astype(BF16)
        for head in range(heads):
            state = (
                jnp.zeros((key_dim, 2 * value_dim), F32), jnp.full((1, 1), -1e30, F32)
            )
            decay = jnp.zeros((1, 1), F32)
            for at in range(blocks):
                number = head * blocks + at
                turned = nt(eye, key_block(head, at)) * weight[number:number + 1, :]
                high, low = halves(turned)
                values = wide_values(head, at)
                locals_ref[number] = mm(high, values) + mm(low, values)
                state = grow(state, number)
                decay = decay + total[number:number + 1, :]
            memory, top = state
            low_row = head * message
            state_send[low_row:low_row + key_dim, :] = memory[:, :value_dim]
            norm = jnp.sum(
                jnp.where(diagonal(), memory[:, value_dim:], 0.0), axis=0, keepdims=True
            )
            row = iota((STATE_ROWS, value_dim), 0)
            state_send[low_row + key_dim:low_row + message, :] = jnp.where(
                row == 0, norm, jnp.where(row == 1, top, decay)
            )

    span = place_at.depth * place_at.side
    own_at = lax.rem(ep_at, span)
    lower_half = place_at.half == 0

    def state_copy(distance, sign):
        at = lax.rem(own_at + sign * distance + span, span)
        return remote(
            state_send, state_recv.at[distance], st_send.at[distance], st_recv.at[distance],
            (place_at.half * span + at, tp_at),
        )

    low_inner = lower_half & place_at.inner
    first_inner = (place_at.depth - 1) * place_at.side

    def total_copy(stage):
        return remote(
            total_send, total_recv, tot_send.at[stage], tot_recv, place_at.beyond(stage)
        )

    def sends_to(distance):
        at = lax.rem(own_at + distance, span)
        return (own_at + distance < span) | (lower_half & (at >= first_inner))

    def takes_from(distance):
        return (own_at >= distance) | low_inner

    def u_copies(target, sender):
        place = pl.ds(pl.multiple_of(sender * own_width, own_width), own_width)
        return [
            remote(
                u_ref.at[target * share:(target + 1) * share, :], u_recv.at[:, place],
                us_send, us_recv, (ep_at, target),
            ),
            remote(
                squares_ref.at[target], squares_recv.at[sender],
                sq_send, sq_recv, (ep_at, target),
            ),
        ]

    def send_states():
        for distance in range(1, span):
            @pl.when(sends_to(distance))
            def _():
                state_copy(distance, 1).start()

    def absorb(memory_ref, max_ref, message_ref):
        for head in range(heads):
            low_row = head * message
            memory = message_ref[low_row:low_row + key_dim, :]
            extra = message_ref[low_row + key_dim:low_row + message, :]
            norm = jnp.sum(jnp.where(diagonal(), extra[0:1, :], 0.0), axis=1, keepdims=True)
            top, decay = extra[1:2, :], extra[2:3, :]
            old_top = max_ref[head, 0:1, :]
            new_top = jnp.maximum(old_top + decay, top)
            left = jnp.exp(old_top + decay - new_top)
            right = jnp.exp(top - new_top)
            memory_ref[head, :, :value_dim] = (
                left * memory_ref[head, :, :value_dim] + right * memory
            )
            memory_ref[head, :, value_dim:] = (
                left * memory_ref[head, :, value_dim:] + right * norm
            )
            max_ref[head] = jnp.broadcast_to(new_top, max_ref.shape[1:])

    def take_states():
        for distance in range(1, span):
            @pl.when(takes_from(distance))
            def _():
                state_copy(distance, 1).wait_recv()

        @pl.when(lower_half)
        def _():
            total_ref[...] = jnp.zeros_like(total_ref)
            total_max[...] = jnp.full_like(total_max, -1e30)
            for distance in range(span - 1, 0, -1):
                @pl.when(own_at >= distance)
                def _():
                    absorb(total_ref, total_max, state_recv.at[distance])
            incoming[...] = total_ref[...]
            incoming_max[...] = total_max[...]

        @pl.when(low_inner)
        def _():
            absorb(total_ref, total_max, state_send)
            for distance in range(span - 1, 0, -1):
                @pl.when(own_at < distance)
                def _():
                    absorb(total_ref, total_max, state_recv.at[distance])
            for head in range(heads):
                low_row = head * message
                total_send[low_row:low_row + key_dim, :] = total_ref[head, :, :value_dim]
                norm = jnp.sum(
                    jnp.where(diagonal(), total_ref[head, :, value_dim:], 0.0),
                    axis=0, keepdims=True,
                )
                row = iota((STATE_ROWS, value_dim), 0)
                total_send[low_row + key_dim:low_row + message, :] = jnp.where(
                    row == 0, norm, jnp.where(row == 1, total_max[head], 0.0)
                )
            for stage in range(place_at.depth):
                total_copy(stage).start()

    def take_total():
        @pl.when(jnp.logical_not(lower_half))
        def _():
            incoming[...] = jnp.zeros_like(incoming)
            incoming_max[...] = jnp.full_like(incoming_max, -1e30)
            total_copy(0).wait_recv()
            absorb(incoming, incoming_max, total_recv)
            for distance in range(span - 1, 0, -1):
                @pl.when(own_at >= distance)
                def _():
                    absorb(incoming, incoming_max, state_recv.at[distance])

    def walk(low_block, high_block):
        if low_block == 0:
            found["states"] = [
                (incoming[head], incoming_max[head, 0:1, 0:1]) for head in range(heads)
            ]
            found["columns"] = jnp.transpose(found["cumulative"])
        states, columns = found["states"], found["columns"]
        lower = iota((BLK, BLK), 0) >= iota((BLK, BLK), 1)
        ones = jnp.ones((STATE_ROWS, value_dim), F32)
        for at in range(low_block, high_block):
            squares = jnp.zeros((STATE_ROWS, BLK), F32)
            for head in range(heads):
                number = head * blocks + at
                memory, top = states[head]
                query = q_ref[at * BLK:(at + 1) * BLK, head * key_dim:(head + 1) * key_dim]
                column = columns[:, number:number + 1]
                gap = jnp.where(
                    lower, column + found["shift"][number:number + 1, :], -jnp.inf
                )
                carried = column + top
                stabilizer = jnp.maximum(carried, jnp.max(gap, axis=1, keepdims=True))
                scores = nt(query, key_block(head, at)) * scale * jnp.exp(gap - stabilizer)
                high, low = halves(scores)
                values = wide_values(head, at)
                sums = mm(high, values) + mm(low, values)
                high, low = halves(memory)
                sums = sums + (jnp.exp(carried - stabilizer) * scale) * (
                    mm(query, high) + mm(query, low)
                )
                hidden = sums[:, :value_dim] / jnp.maximum(
                    jnp.abs(sums[:, value_dim:]), jnp.exp(-stabilizer)
                )
                squares = squares + nt(ones, hidden * hidden, exact)
                place = slice(head * value_dim, (head + 1) * value_dim)
                gate = gate_ref[at * BLK:(at + 1) * BLK, place].astype(F32)
                u_ref[at * BLK:(at + 1) * BLK, place] = (
                    hidden * gain_ref[:, place] * jax.nn.sigmoid(gate)
                ).astype(BF16)
                states[head] = grow(states[head], number)
            squares_ref[at // share_blocks, at % share_blocks] = squares
            if at % share_blocks == share_blocks - 1:
                @pl.when(jnp.logical_not(place_at.inner))
                def _():
                    send_share(at // share_blocks)

    def send_share(target):
        @pl.when(tp_at != target)
        def _():
            for copy in u_copies(target, tp_at):
                copy.start()

        @pl.when(tp_at == target)
        def _():
            place = pl.ds(pl.multiple_of(tp_at * own_width, own_width), own_width)
            u_recv[:, place] = u_ref[target * share:(target + 1) * share, :]
            squares_recv[tp_at] = squares_ref[target]

    def send_u():
        @pl.when(place_at.inner)
        def _():
            for target in range(tp_count):
                send_share(target)

    def late():
        others = tp_count - 1
        region = u_recv.at[:, :others * own_width]
        remote(region, region, us_send, us_recv, place_at.proxy).wait_recv()
        region = squares_recv.at[:others]
        remote(region, region, sq_send, sq_recv, place_at.proxy).wait_recv()
        squares = squares_recv[0]
        for sender in range(1, tp_count):
            squares = squares + squares_recv[sender]
        inverse_row = lax.rsqrt(squares / (heads * tp_count * value_dim) + 1e-6)
        eye = (iota((BLK, BLK), 0) == iota((BLK, BLK), 1)).astype(F32)
        load.wait()
        width = wo.shape[1]
        for at in range(share_blocks):
            inverse = nt(eye, inverse_row[at], exact)[:, 0:1]

            @pl.loop(0, width // 512)
            def _(turn):
                place = pl.ds(pl.multiple_of(turn * 512, 512), 512)
                product = mm(u_recv[at * BLK:(at + 1) * BLK, :], wo[:, place])
                out_ref[at * BLK:(at + 1) * BLK, place] = (product * inverse).astype(BF16)

            out_copy(at).start()


    def close():
        for at in range(share_blocks):
            out_copy(at).wait()
        for distance in range(1, span):
            @pl.when(sends_to(distance))
            def _():
                state_copy(distance, 1).wait_send()

        @pl.when(low_inner)
        def _():
            for stage in range(place_at.depth):
                total_copy(stage).wait_send()

        region = u_ref.at[:(tp_count - 1) * share, :]
        remote(region, region, us_send, us_recv, place_at.proxy).wait_send()
        region = squares_ref.at[:tp_count - 1]
        remote(region, region, sq_send, sq_recv, place_at.proxy).wait_send()

    return fetch, early, send_u, send_states, take_states, take_total, walk, late, close


def settle(results):
    count = len(results)
    parts = 4

    def kernel(*refs):
        sources, targets, held = refs[:count], refs[count:2 * count], refs[2 * count:3 * count]
        in_sem, out_sem = refs[3 * count:]
        ins, outs = [], []
        for number in range(count):
            rows = held[number].shape[0] // parts
            for part in range(parts):
                place, at = slice(part * rows, (part + 1) * rows), number * parts + part
                here = held[number].at[place, :]
                ins.append(
                    pltpu.make_async_copy(sources[number].at[place, :], here, in_sem.at[at])
                )
                outs.append(
                    pltpu.make_async_copy(here, targets[number].at[place, :], out_sem.at[at])
                )
        for copy in ins:
            copy.start()
        for come, leave in zip(ins, outs):
            come.wait()
            leave.start()
        for copy in outs:
            copy.wait()

    hbm = pl.BlockSpec(memory_space=pl.ANY)
    sems = pltpu.SemaphoreType.DMA((count * parts,))
    return pl.pallas_call(
        kernel,
        out_shape=tuple(jax.ShapeDtypeStruct(array.shape, array.dtype) for array in results),
        in_specs=[hbm] * count,
        out_specs=(hbm,) * count,
        scratch_shapes=[pltpu.VMEM(array.shape, array.dtype) for array in results] + [sems, sems],
        name="settle",
    )(*results)


def on_device(
    queries,
    head_key_rows,
    head_value_rows,
    log_input_gate,
    forget_logits,
    head_forget_bias,
    extra_log_forget,
    output_gate_logits,
    head_norm_gain,
    mixer_output_weight,
    second_batch_input,
    expert_norm_gain,
    routed_expert_index,
    routed_copy_weight,
    routed_gate_weight,
    routed_up_weight,
    routed_down_weight,
    shared_gate_weight,
    shared_up_weight,
    shared_down_weight,
):
    tokens, width = second_batch_input.shape
    ep_count = lax.axis_size("ep")
    tp_count = lax.axis_size("tp")
    count = ep_count * tp_count
    top_count = routed_expert_index.shape[1]
    capacity = max(2, 3 * tokens * top_count // (2 * count))
    groups = capacity // LANE_ROWS
    step = width // PIECES
    wire = PIECES * (groups * step + step * (capacity - groups * LANE_ROWS) // LANE_ROWS)
    side = max(1, tp_count // CORES)
    near = count // 2
    span = ep_count // 2
    depth = ep_count // side // 2
    rows = near * capacity
    padded = -(-tokens // 128) * 128
    hidden_width = routed_gate_weight.shape[2]
    length = queries.shape[0]
    heads = head_forget_bias.shape[0]
    key_dim = queries.shape[1] // heads
    value_dim = head_value_rows.shape[1] // heads
    blocks = length // BLK
    share = length // tp_count
    dma = pltpu.SemaphoreType.DMA
    vmem = pl.BlockSpec(memory_space=pltpu.VMEM)
    hbm = pl.BlockSpec(memory_space=pl.ANY)

    block = pltpu.VMEM((tokens, width), BF16)
    meta = pltpu.VMEM((STATE_ROWS, padded), F32)
    half_slots = pltpu.VMEM((near * LANE_ROWS, wire), BF16)
    far_slots = pltpu.VMEM((depth, near * LANE_ROWS, wire), BF16)
    far_block = pltpu.VMEM((depth, tokens, width), BF16)
    slots = pltpu.VMEM((2 * near * LANE_ROWS, wire), BF16)
    moe_scratch = (
        [block, meta, far_block, pltpu.VMEM((depth, STATE_ROWS, padded), F32)]
        + [half_slots, far_slots, slots, slots, half_slots, far_slots]
        + [far_block, block]
        + [
            pltpu.VMEM(array.shape[-2:], BF16)
            for array in (
                routed_gate_weight, routed_up_weight, routed_down_weight,
                shared_gate_weight, shared_up_weight, shared_down_weight,
            )
        ]
        + [
            pltpu.VMEM((rows, width), BF16),
            pltpu.VMEM((rows, hidden_width), BF16),
            pltpu.VMEM((rows, width), BF16),
            pltpu.VMEM((rows, hidden_width), F32),
            pltpu.VMEM((rows, hidden_width), F32),
            pltpu.VMEM((tokens, width), F32),
            block,
            dma((6,)), dma, dma((PIECES,)), dma, dma((depth, PIECES)), dma, dma,
            dma((PIECES,)), dma((depth, PIECES)), dma, dma((depth, PIECES)), dma,
            dma((PIECES,)), dma, dma((depth,)), dma((PIECES,)),
        ]
    )
    message = heads * (key_dim + STATE_ROWS)
    mixer_scratch = [
        *[
            pltpu.VMEM(array.shape, BF16)
            for array in (queries, head_key_rows, head_value_rows, output_gate_logits)
        ],
        pltpu.VMEM((share, width), BF16), dma((4,)), dma((share // BLK,)),
        pltpu.VMEM(mixer_output_weight.shape, BF16),
        pltpu.VMEM((heads * blocks, key_dim, 2 * value_dim), F32),
        pltpu.VMEM((message, value_dim), F32),
        pltpu.VMEM((span, message, value_dim), F32),
        pltpu.VMEM((message, value_dim), F32),
        pltpu.VMEM((message, value_dim), F32),
        pltpu.VMEM((heads, key_dim, 2 * value_dim), F32),
        pltpu.VMEM((heads, STATE_ROWS, value_dim), F32),
        pltpu.VMEM((heads, key_dim, 2 * value_dim), F32),
        pltpu.VMEM((heads, STATE_ROWS, value_dim), F32),
        pltpu.VMEM((length, heads * value_dim), BF16),
        pltpu.VMEM((tp_count, share // BLK, STATE_ROWS, BLK), F32),
        pltpu.VMEM((share, tp_count * heads * value_dim), BF16),
        pltpu.VMEM((tp_count, share // BLK, STATE_ROWS, BLK), F32),
        dma, dma((span,)), dma((span,)), dma((depth,)), dma,
        dma, dma, dma, dma,
    ]

    def kernel(*refs):
        mixer_in, moe_in = refs[:10], refs[10:20]
        mixer_out, moe_out = refs[20], refs[21]
        scratch = refs[22:]
        cut = len(moe_scratch)
        place = Place(ep_count, tp_count)
        fetch, early, send_u, send_states, take_states, take_total, walk, late, close = mixer_parts(
            place, ep_count, tp_count, (*mixer_in, mixer_out, *scratch[cut:])
        )
        experts = Experts(place, capacity, (*moe_in, moe_out, *scratch[:cut]))
        depth = place.depth
        fetch()
        experts.open()
        experts.meet()
        experts.start()
        early()
        send_states()
        experts.common()
        for piece in range(PIECES):
            experts.relay(0, piece)
        experts.serve_own()
        experts.return_plane()
        for stage in range(depth):
            if stage + 1 < depth:
                experts.relay(stage + 1, 0)
            experts.serve_far(stage)
            if stage + 1 < depth:
                for piece in range(1, PIECES):
                    experts.relay(stage + 1, piece)
            else:
                experts.return_planes(jnp.logical_not(place.inner))
            if stage == 0:
                experts.return_planes(place.inner)
                take_states()
                take_total()
            walk(blocks * stage // depth, blocks * (stage + 1) // depth)
            experts.mix_far(stage)
        send_u()
        experts.mix_own()
        late()
        experts.close()
        close()

    results = pl.pallas_call(
        kernel,
        out_shape=(
            jax.ShapeDtypeStruct((share, width), BF16),
            jax.ShapeDtypeStruct((tokens, width), BF16),
        ),
        in_specs=[hbm] * 3 + [vmem] * 4 + [hbm, vmem, hbm] + [vmem] * 4 + [hbm] * 6,
        out_specs=(hbm, hbm),
        scratch_shapes=moe_scratch + mixer_scratch,
        compiler_params=pltpu.CompilerParams(
            collective_id=0, has_side_effects=True, vmem_limit_bytes=62 * 1024 * 1024
        ),
        name="both",
    )(
        queries, head_key_rows, head_value_rows, log_input_gate.T, forget_logits.T,
        head_forget_bias[None, :], extra_log_forget.T, output_gate_logits,
        head_norm_gain[None, :], mixer_output_weight,
        second_batch_input, expert_norm_gain[None, :], routed_expert_index.T,
        routed_copy_weight.T, routed_gate_weight, routed_up_weight,
        routed_down_weight, shared_gate_weight, shared_up_weight, shared_down_weight,
    )
    return settle(results)


def solution(mesh):
    in_specs = (
        P("ep", "tp"),
        P("ep", "tp"),
        P("ep", "tp"),
        P("ep", "tp"),
        P("ep", "tp"),
        P("tp"),
        P("ep", "tp"),
        P("ep", "tp"),
        P("tp"),
        P(),
        P(("ep", "tp"), None),
        P(),
        P(("ep", "tp"), None),
        P(("ep", "tp"), None),
        P(("ep", "tp"), None, None),
        P(("ep", "tp"), None, None),
        P(("ep", "tp"), None, None),
        P(),
        P(),
        P(),
    )
    out_specs = (P(("ep", "tp"), None), P(("ep", "tp"), None))
    return jax.shard_map(
        on_device, mesh=mesh, in_specs=in_specs, out_specs=out_specs, check_vma=False
    )
```

```python
import jax
import jax.numpy as jnp
from jax import lax
from jax.experimental import pallas as pl
from jax.experimental.pallas import tpu as pltpu
from jax.sharding import PartitionSpec as P

BLK = 128


F32 = jnp.float32
BF16 = jnp.bfloat16
LANE_ROWS = 16
CORES = 2
PIECES = 2
RESULTS = 4


def mm(left, right):
    return jnp.dot(left, right, preferred_element_type=F32)


def iota(shape, axis):
    return lax.broadcasted_iota(jnp.int32, shape, axis)


class Place:
    def __init__(self, ep_count, tp_count):
        self.side = max(1, tp_count // CORES)
        self.tp_count = tp_count
        self.planes = ep_count // self.side
        self.depth = self.planes // 2
        self.cell = self.side * tp_count
        self.near = self.depth * self.cell
        self.ep_at = lax.axis_index("ep")
        self.tp_at = lax.axis_index("tp")
        plane = self.ep_at // self.side
        self.row = lax.rem(self.ep_at, self.side)
        self.half = plane // self.depth
        self.level = plane - self.half * self.depth
        self.stage = self.half * self.level + (1 - self.half) * (self.depth - 1 - self.level)
        self.spot = self.level * self.cell + self.row * tp_count + self.tp_at
        self.inner = self.stage == 0
        self.low = jnp.where(self.inner, 1, 0)
        self.proxy = self.beyond(0)

    def at(self, level, row, tp):
        device = ((self.half * self.depth + level) * self.side + row, tp)
        return device, level * self.cell + row * self.tp_count + tp

    def across(self, step, sign):
        row_step, tp_step = step // self.tp_count, lax.rem(step, self.tp_count)
        row = lax.rem(self.row + sign * row_step + self.side, self.side)
        tp = lax.rem(self.tp_at + sign * tp_step + self.tp_count, self.tp_count)
        return row, tp

    def away(self, distance, sign):
        level_step = distance // self.cell
        level = lax.rem(self.level + sign * level_step + self.depth, self.depth)
        return self.at(level, *self.across(lax.rem(distance, self.cell), sign))

    def beyond(self, stage):
        plane = (1 - self.half) * (self.depth + stage) + self.half * (self.depth - 1 - stage)
        return plane * self.side + self.row, self.tp_at


def each(low, high, work):
    def turn(step, carry):
        work(step)
        return carry

    lax.fori_loop(low, high, turn, 0)


def rows_of(index):
    return pl.ds(pl.multiple_of(index * LANE_ROWS, LANE_ROWS), LANE_ROWS)


def remote(source, target, send_sem, recv_sem, device):
    return pltpu.make_async_remote_copy(
        src_ref=source, dst_ref=target, send_sem=send_sem, recv_sem=recv_sem,
        device_id=device, device_id_type=pl.DeviceIdType.MESH,
    )


def as_weight(mask):
    return mask.astype(F32).astype(BF16)


class Experts:
    def __init__(self, place, capacity, refs):
        (x_hbm, self.gain_ref, self.idx_ref, self.weight_ref, wg_hbm, wu_hbm, wd_hbm, sg_hbm,
         su_hbm, sd_hbm, self.out_ref, self.normed, self.meta, self.far_block, self.far_meta,
         self.send_own, self.send_far, self.recv, self.ysend, self.ret_own, self.ret_far,
         self.far_out, self.far_in, self.wg, self.wu, self.wd, self.sg, self.su, self.sd, self.xc,
         self.hc, self.yc, self.gates, self.ups, self.total, self.out, self.mixes, self.x_ref, x_sem, load_sem, self.go_send, self.go_recv, self.far_send,
         self.far_got, self.far_back, self.back_send, self.back_recv, self.far_recv, self.over_send, self.over_recv,
         self.result_send, self.result_recv, self.meta_send, self.meta_recv, self.out_sem) = refs
        self.place = place
        self.x_load = pltpu.make_async_copy(x_hbm, self.x_ref, x_sem)
        self.tokens, self.width = self.x_ref.shape
        self.step = self.width // PIECES
        self.groups = capacity // LANE_ROWS
        self.tail = capacity - self.groups * LANE_ROWS
        self.parts = LANE_ROWS // self.tail
        self.piece = self.step // self.parts
        self.base = self.groups * self.step
        self.wire = self.base + self.piece
        self.loads = [
            pltpu.make_async_copy(source, target, load_sem.at[number])
            for number, (source, target) in enumerate(
                [(sg_hbm, self.sg), (su_hbm, self.su), (sd_hbm, self.sd),
                 (wg_hbm.at[0], self.wg), (wu_hbm.at[0], self.wu), (wd_hbm.at[0], self.wd)]
            )
        ]

    def open(self):
        place, tokens = self.place, self.tokens
        self.x_load.start()
        barrier = pltpu.get_barrier_semaphore()

        def greet(device):
            pl.semaphore_signal(
                barrier, inc=1, device_id=device, device_id_type=pl.DeviceIdType.MESH
            )

        each(1, place.near, lambda distance: greet(place.away(distance, 1)[0]))
        greet(place.proxy)

        @pl.when(place.inner)
        def _():
            for stage in range(1, place.depth):
                greet(place.beyond(stage))

        for load in self.loads:
            load.start()
        self.x_load.wait()
        floats = self.x_ref[...].astype(F32)
        inverse = lax.rsqrt(jnp.mean(floats * floats, axis=1, keepdims=True) + 1e-6)
        self.normed[...] = (floats * inverse * self.gain_ref[...]).astype(BF16)

        expert_rows = iota((2 * place.near, tokens), 0)
        first, second = self.idx_ref[0:1, :], self.idx_ref[1:2, :]
        hit_first = expert_rows == first
        hit_second = expert_rows == second
        named = as_weight(hit_first | hit_second)
        before = as_weight(iota((tokens, tokens), 0) < iota((tokens, tokens), 1))
        earlier = mm(named, before)
        self.meta[...] = jnp.zeros_like(self.meta)
        self.meta[0:1, :tokens] = first.astype(F32)
        self.meta[1:2, :tokens] = second.astype(F32)
        self.meta[2:3, :tokens] = jnp.sum(jnp.where(hit_first, earlier, 0.0), axis=0, keepdims=True)
        self.meta[3:4, :tokens] = jnp.sum(
            jnp.where(hit_second, earlier, 0.0), axis=0, keepdims=True
        )
        self.meta[4:6, :tokens] = self.weight_ref[...]
    def meet(self):
        place = self.place
        pl.semaphore_wait(
            pltpu.get_barrier_semaphore(), place.near - 1 + jnp.where(place.inner, place.depth, 1)
        )

    def keys(self, first, second, place_first, place_second):
        near, low = self.place.near, self.place.half * self.place.near

        def main(expert, place, group):
            local, near_expert = place - group * LANE_ROWS, expert - low
            inside = (near_expert >= 0) & (near_expert < near)
            inside = inside & (local >= 0) & (local < LANE_ROWS)
            return jnp.where(inside, near_expert * LANE_ROWS + local, -LANE_ROWS)

        def tail(expert, place):
            local, near_expert = place - self.groups * LANE_ROWS, expert - low
            inside = (near_expert >= 0) & (near_expert < near) & (local >= 0)
            return jnp.where(inside, near_expert * LANE_ROWS + local * self.parts, -LANE_ROWS)

        mains = [
            (main(first, place_first, group), main(second, place_second, group))
            for group in range(self.groups)
        ]
        return mains, (tail(first, place_first), tail(second, place_second))

    def slots(self, piece, block, meta, send):
        whole = meta[:, :self.tokens].astype(jnp.int32)
        mains, tails = self.keys(*[whole[row:row + 1, :] for row in range(4)])
        slot_rows = iota((self.place.near * LANE_ROWS, self.tokens), 0)
        low, to = piece * self.step, piece * self.wire
        step = self.step // 2
        for group, (first, second) in enumerate(mains):
            pick = as_weight((slot_rows == first) | (slot_rows == second))
            for at in range(0, self.step, step):
                start = to + group * self.step + at
                send[:, start:start + step] = mm(
                    pick, block[:, low + at:low + at + step]
                ).astype(BF16)
        total = jnp.zeros((self.place.near * LANE_ROWS, self.piece), F32)
        for part in range(self.parts):
            pick = as_weight((slot_rows == tails[0] + part) | (slot_rows == tails[1] + part))
            at = low + part * self.piece
            total = total + mm(pick, block[:, at:at + self.piece])
        send[:, to + self.base:to + self.wire] = total.astype(BF16)

    def columns(self, piece):
        return slice(piece * self.step, (piece + 1) * self.step)

    def wires(self, piece):
        return slice(piece * self.wire, (piece + 1) * self.wire)

    def meta_copy(self):
        return remote(
            self.meta, self.far_meta.at[self.place.stage], self.meta_send,
            self.meta_recv.at[self.place.stage], self.place.proxy,
        )

    def meta_from(self, stage):
        return remote(
            self.meta, self.far_meta.at[stage], self.meta_send, self.meta_recv.at[stage],
            self.place.proxy,
        )

    def block_to(self, stage, piece):
        columns = self.columns(piece)
        return remote(
            self.normed.at[:, columns], self.far_block.at[stage, :, columns],
            self.over_send, self.over_recv.at[stage, piece], self.place.proxy,
        )

    def result_columns(self, piece):
        step = self.width // RESULTS
        return slice(piece * step, (piece + 1) * step)

    def result_to(self, stage, piece):
        columns = self.result_columns(piece)
        return remote(
            self.far_out.at[stage, :, columns], self.far_in.at[:, columns],
            self.result_send, self.result_recv.at[piece],
            self.place.beyond(stage),
        )

    def go_own(self, distance, piece):
        device, spot = self.place.away(distance, 1)
        wires = self.wires(piece)
        return remote(
            self.send_own.at[rows_of(spot), wires], self.recv.at[rows_of(distance), wires],
            self.go_send, self.go_recv.at[piece], device,
        )

    def back_own(self, distance, piece):
        device, _ = self.place.away(distance, -1)
        wires = self.wires(piece)
        return remote(
            self.ysend.at[rows_of(distance), wires],
            self.ret_own.at[rows_of(self.place.spot), wires],
            self.back_send, self.back_recv.at[piece], device,
        )

    def all_of(self, source, target, send_sem, recv_sem):
        return remote(source, target, send_sem, recv_sem, self.place.proxy)

    def go_far(self, stage, turn, piece):
        place = self.place
        level, step = turn // place.cell, lax.rem(turn, place.cell)
        device, spot = place.at(level, *place.across(step, 1))
        slot = place.near + stage * place.cell + step
        wires = self.wires(piece)
        return remote(
            self.send_far.at[stage, rows_of(spot), wires], self.recv.at[rows_of(slot), wires],
            self.far_send, self.far_got.at[stage, piece], device,
        )

    def back_far(self, stage, step, piece):
        place = self.place
        level = (1 - place.half) * (place.depth - 1)
        device, _ = place.at(level, *place.across(step, -1))
        slot = place.near + stage * place.cell + step
        wires = self.wires(piece)
        return remote(
            self.ysend.at[rows_of(slot), wires],
            self.ret_far.at[stage, rows_of(place.spot), wires],
            self.far_back, self.far_recv.at[stage, piece], device,
        )

    def others(self, work):
        own = self.place.level * self.place.cell
        each(0, own, work)
        each(own + 1, self.place.near, work)

    def start(self):
        place = self.place

        @pl.when(place.inner)
        def _():
            self.meta_copy().start()
            for piece in range(PIECES):
                self.block_to(0, piece).start()

        for piece in range(PIECES):
            self.slots(piece, self.normed, self.meta, self.send_own)
            each(1, place.near, lambda distance: self.go_own(distance, piece).start())
        self.recv[0:LANE_ROWS, :] = self.send_own[rows_of(place.spot), :]

    def start_outer(self):
        place = self.place

        @pl.when(jnp.logical_not(place.inner))
        def _():
            self.meta_copy().start()
            for piece in range(PIECES):
                self.block_to(place.stage, piece).start()

    def relay(self, stage, piece):
        place = self.place

        @pl.when(place.inner)
        def _():
            if piece == 0:
                self.meta_from(stage).wait_recv()
            self.block_to(stage, piece).wait_recv()
            self.slots(piece, self.far_block.at[stage], self.far_meta.at[stage], self.send_far.at[stage])
            self.others(lambda turn: self.go_far(stage, turn, piece).start())
            slot = (place.near + stage * place.cell) * LANE_ROWS
            self.recv[slot:slot + LANE_ROWS, self.wires(piece)] = self.send_far[
                stage, rows_of(place.spot), self.wires(piece)
            ]

    def common(self):
        for load in self.loads[:3]:
            load.wait()
        gate = mm(self.normed[...], self.sg[...])
        hidden = (gate * jax.nn.sigmoid(gate) * mm(self.normed[...], self.su[...])).astype(BF16)
        step = self.width // 4
        for at in range(0, self.width, step):
            self.total[:, at:at + step] = mm(hidden, self.sd[:, at:at + step])
        for load in self.loads[3:]:
            load.wait()

    def serve(self, first, sources, arrive, leave):
        main_rows, tail_rows = sources * LANE_ROWS, sources * self.tail
        low, piece = first * LANE_ROWS, self.piece
        start = self.groups * main_rows
        rows = start + tail_rows
        recv, ysend, xc, hc, yc = self.recv, self.ysend, self.xc, self.hc, self.yc

        def select(part, transposed):
            shape = (main_rows, tail_rows) if transposed else (tail_rows, main_rows)
            axis = 1 if transposed else 0
            return as_weight(iota(shape, 1 - axis) == iota(shape, axis) * self.parts + part)

        for number in range(PIECES):
            arrive(number)
            at, to = number * self.wire, number * self.step
            for group in range(self.groups):
                xc[group * main_rows:(group + 1) * main_rows, to:to + self.step] = recv[
                    low:low + main_rows, at + group * self.step:at + (group + 1) * self.step
                ]
            for part in range(self.parts):
                xc[start:rows, to + part * piece:to + (part + 1) * piece] = mm(
                    select(part, False),
                    recv[low:low + main_rows, at + self.base:at + self.wire],
                ).astype(BF16)
            last = number == PIECES - 1

            @pl.loop(0, hc.shape[1] // 256)
            def _(turn):
                columns = pl.ds(pl.multiple_of(turn * 256, 256), 256)
                gate = mm(xc[:rows, to:to + self.step], self.wg[to:to + self.step, columns])
                up = mm(xc[:rows, to:to + self.step], self.wu[to:to + self.step, columns])
                if number:
                    gate = gate + self.gates[:rows, columns]
                    up = up + self.ups[:rows, columns]
                if last:
                    hc[:rows, columns] = (gate * jax.nn.sigmoid(gate) * up).astype(BF16)
                else:
                    self.gates[:rows, columns] = gate
                    self.ups[:rows, columns] = up

        for number in range(PIECES):
            at, to = number * self.wire, number * self.step

            @pl.loop(0, self.step // 256)
            def _(turn):
                columns = pl.ds(pl.multiple_of(to + turn * 256, 256), 256)
                yc[:rows, columns] = mm(hc[:rows, :], self.wd[:, columns]).astype(BF16)

            for group in range(self.groups):
                ysend[
                    low:low + main_rows, at + group * self.step:at + (group + 1) * self.step
                ] = yc[group * main_rows:(group + 1) * main_rows, to:to + self.step]
            total = jnp.zeros((main_rows, piece), F32)
            for part in range(self.parts):
                total = total + mm(
                    select(part, True),
                    yc[start:rows, to + part * piece:to + (part + 1) * piece],
                )
            ysend[low:low + main_rows, at + self.base:at + self.wire] = total.astype(BF16)
            leave(number)

    def serve_own(self):
        place = self.place

        def arrive(piece):
            with jax.named_scope("wait_own"):
                region = self.recv.at[LANE_ROWS:place.near * LANE_ROWS, self.wires(piece)]
                self.all_of(region, region, self.go_send, self.go_recv.at[piece]).wait_recv()

        def leave(piece):
            if piece == 0:
                self.start_outer()
            self.return_own(piece, 1, place.cell)
            self.ret_own[rows_of(place.spot), self.wires(piece)] = self.ysend[
                0:LANE_ROWS, self.wires(piece)
            ]

        self.serve(0, place.near, arrive, leave)

    def return_own(self, piece, low, high):
        each(low, high, lambda distance: self.back_own(distance, piece).start())

    def return_planes(self, chosen):
        @pl.when(chosen)
        def _():
            for piece in range(PIECES):
                self.return_own(piece, self.place.cell, self.place.near)

    def serve_far(self, stage):
        place = self.place
        first = place.near + stage * place.cell

        def arrive(piece):
            if piece and stage:
                self.mix_far(stage - 1, piece)
            with jax.named_scope("wait_far"):
                for inner, count in ((True, place.cell - 1), (False, place.cell)):
                    @pl.when(place.inner == inner)
                    def _():
                        end = (first + place.cell) * LANE_ROWS
                        region = self.recv.at[end - count * LANE_ROWS:end, self.wires(piece)]
                        self.all_of(
                            region, region, self.far_send, self.far_got.at[stage, piece]
                        ).wait_recv()

        def leave(piece):
            each(place.low, place.cell, lambda step: self.back_far(stage, step, piece).start())

            @pl.when(place.inner)
            def _():
                self.ret_far[stage, rows_of(place.spot), self.wires(piece)] = self.ysend[
                    first * LANE_ROWS:(first + 1) * LANE_ROWS, self.wires(piece)
                ]

        self.serve(first, place.cell, arrive, leave)

    def weigh(self, meta):
        turned = jnp.transpose(meta[...])[:self.tokens, :]
        whole = turned.astype(jnp.int32)
        mains, tails = self.keys(*[whole[:, row:row + 1] for row in range(4)])
        slot_lanes = iota((self.tokens, self.place.near * LANE_ROWS), 1)
        spots = mains + [(tails[0] + part, tails[1] + part) for part in range(self.parts)]
        for number, (first, second) in enumerate(spots):
            values = jnp.where(slot_lanes == first, turned[:, 4:5], 0.0) + jnp.where(
                slot_lanes == second, turned[:, 5:6], 0.0
            )
            self.mixes[number, 0], self.mixes[number, 1] = halves(values)

    def mix(self, number, ret, store):
        at, to = number * self.wire, number * self.step

        def weighted(spot, values):
            return mm(self.mixes[spot, 0], values) + mm(self.mixes[spot, 1], values)

        for part in range(self.parts):
            low, high = part * self.piece, (part + 1) * self.piece
            total = weighted(self.groups + part, ret[:, at + self.base:at + self.wire])
            for group in range(self.groups):
                start = at + group * self.step
                total = total + weighted(group, ret[:, start + low:start + high])
            store(to + low, to + high, total)

    def mix_own(self):
        place = self.place
        self.weigh(self.meta)

        def store(low, high, value):
            self.total[:, low:high] = self.total[:, low:high] + value

        for piece in range(PIECES):
            with jax.named_scope("wait_back"):
                region = self.ret_own.at[LANE_ROWS:place.near * LANE_ROWS, self.wires(piece)]
                self.all_of(region, region, self.back_send, self.back_recv.at[piece]).wait_recv()
            self.mix(piece, self.ret_own, store)

    def mix_far(self, stage, piece):
        @pl.when(self.place.inner)
        def _():
            if piece == 0:
                self.weigh(self.far_meta.at[stage])

            def store(low, high, value):
                self.far_out[stage, :, low:high] = value.astype(BF16)
                step = self.width // RESULTS
                if high % step == 0:
                    self.result_to(stage, high // step - 1).start()

            with jax.named_scope("wait_ret"):
                region = self.ret_far.at[
                    stage, LANE_ROWS:self.place.near * LANE_ROWS, self.wires(piece)
                ]
                self.all_of(
                    region, region, self.far_back, self.far_recv.at[stage, piece]
                ).wait_recv()
            self.mix(piece, self.ret_far.at[stage], store)

    def out_copy(self, piece):
        columns = self.result_columns(piece)
        return pltpu.make_async_copy(
            self.out.at[:, columns], self.out_ref.at[:, columns], self.out_sem.at[piece]
        )

    def close(self):
        place = self.place
        for piece in range(RESULTS):
            with jax.named_scope("wait_result"):
                self.result_to(0, piece).wait_recv()
            columns = self.result_columns(piece)
            self.out[:, columns] = (
                self.total[:, columns] + self.far_in[:, columns].astype(F32)
            ).astype(BF16)
            self.out_copy(piece).start()
        def sent(region, sem, other):
            self.all_of(region, region, sem, other).wait_send()

        others = (place.near - 1) * LANE_ROWS
        self.meta_copy().wait_send()
        sent(self.normed, self.over_send, self.over_recv.at[0, 0])
        sent(self.send_own.at[:others, :], self.go_send, self.go_recv.at[0])
        sent(self.ysend.at[:others, :], self.back_send, self.back_recv.at[0])
        for inner, count in ((True, place.cell - 1), (False, place.cell)):
            @pl.when(place.inner == inner)
            def _():
                rows = place.depth * count * LANE_ROWS
                sent(self.ysend.at[:rows, :], self.far_back, self.far_recv.at[0, 0])

        @pl.when(place.inner)
        def _():
            sent(self.send_far.at[:, :others, :], self.far_send, self.far_got.at[0, 0])
            sent(self.far_out, self.result_send, self.result_recv.at[0])

        for piece in range(RESULTS):
            self.out_copy(piece).wait()


STATE_ROWS = 8


def nt(left, right, precision=None):
    return lax.dot_general(
        left, right, (((1,), (1,)), ((), ())), precision=precision, preferred_element_type=F32
    )


def halves(value):
    high = value.astype(BF16)
    return high, (value - high.astype(F32)).astype(BF16)


def log_one_plus(small):
    series = small * (1.0 - small * (0.5 - small * (1.0 / 3.0 - small * 0.25)))
    return jnp.where(small < 0.01, series, jnp.log(1.0 + small))


def mixer_parts(place_at, ep_count, tp_count, refs):
    (q_hbm, k_hbm, v_hbm, in_ref, forget_ref, bias_ref, extra_ref, gate_hbm, gain_ref, wo_hbm,
     out_hbm, q_ref, k_ref, v_ref, gate_ref, out_ref, in_sem, out_sem, wo, locals_ref, state_send, state_recv, total_send, total_recv, total_ref,
     total_max, incoming, incoming_max, u_ref, squares_ref,
     u_recv, squares_recv, wo_sem, st_send, st_recv, tot_send, tot_recv, us_send, us_recv, sq_send, sq_recv) = refs
    exact = lax.Precision.HIGHEST
    heads, length = in_ref.shape
    blocks = length // BLK
    key_dim = q_ref.shape[1] // heads
    value_dim = v_ref.shape[1] // heads
    own_width = heads * value_dim
    scale = key_dim ** (-0.5)
    message = key_dim + STATE_ROWS
    share = length // tp_count
    share_blocks = share // BLK
    ep_at, tp_at = place_at.ep_at, place_at.tp_at
    load = pltpu.make_async_copy(wo_hbm, wo, wo_sem)

    def block_rows(ref, transform=lambda value, head: value):
        whole = ref[...]
        return jnp.concatenate(
            [
                transform(whole[head:head + 1, at * BLK:(at + 1) * BLK], head)
                for head in range(heads)
                for at in range(blocks)
            ],
            axis=0,
        )

    def key_block(head, at):
        return k_ref[at * BLK:(at + 1) * BLK, head * key_dim:(head + 1) * key_dim]

    def wide_values(head, at):
        values = v_ref[at * BLK:(at + 1) * BLK, head * value_dim:(head + 1) * value_dim]
        return jnp.concatenate([values, jnp.ones((BLK, value_dim), BF16)], axis=1)

    inputs = [
        pltpu.make_async_copy(source, target, in_sem.at[number])
        for number, (source, target) in enumerate(
            [(k_hbm, k_ref), (v_hbm, v_ref), (q_hbm, q_ref), (gate_hbm, gate_ref)]
        )
    ]

    def fetch():
        for copy in inputs:
            copy.start()

    def out_copy(at):
        rows = slice(at * BLK, (at + 1) * BLK)
        return pltpu.make_async_copy(
            out_ref.at[rows, :], out_hbm.at[rows, :], out_sem.at[at]
        )

    found = {}

    def grow(state, number):
        memory, top = state
        total = found["total"][number:number + 1, :]
        block_top = found["block_top"][number:number + 1, :]
        new_top = jnp.maximum(top + total, block_top)
        memory = jnp.exp(top + total - new_top) * memory + jnp.exp(
            block_top - new_top
        ) * locals_ref[number]
        return memory, new_top

    def diagonal():
        shape = (key_dim, value_dim)
        return iota(shape, 0) == iota(shape, 1)

    def early():
        load.start()
        for copy in inputs:
            copy.wait()
        logits = block_rows(forget_ref, lambda value, head: value + bias_ref[:, head:head + 1])
        kept = jnp.minimum(logits, 0.0) - log_one_plus(jnp.exp(-jnp.abs(logits)))
        kept = kept + block_rows(extra_ref)
        gates = block_rows(in_ref)
        upper = (iota((BLK, BLK), 0) <= iota((BLK, BLK), 1)).astype(F32)
        cumulative = jnp.dot(kept, upper, precision=exact, preferred_element_type=F32)
        total = cumulative[:, BLK - 1:BLK]
        gap = total - cumulative + gates
        block_top = jnp.max(gap, axis=1, keepdims=True)
        weight = jnp.exp(gap - block_top)
        found["total"], found["block_top"] = total, block_top
        found["cumulative"], found["shift"] = cumulative, gates - cumulative
        eye = (iota((key_dim, key_dim), 0) == iota((key_dim, key_dim), 1)).astype(F32).astype(BF16)
        for head in range(heads):
            state = (
                jnp.zeros((key_dim, 2 * value_dim), F32), jnp.full((1, 1), -1e30, F32)
            )
            decay = jnp.zeros((1, 1), F32)
            for at in range(blocks):
                number = head * blocks + at
                turned = nt(eye, key_block(head, at)) * weight[number:number + 1, :]
                high, low = halves(turned)
                values = wide_values(head, at)
                locals_ref[number] = mm(high, values) + mm(low, values)
                state = grow(state, number)
                decay = decay + total[number:number + 1, :]
            memory, top = state
            low_row = head * message
            state_send[low_row:low_row + key_dim, :] = memory[:, :value_dim]
            norm = jnp.sum(
                jnp.where(diagonal(), memory[:, value_dim:], 0.0), axis=0, keepdims=True
            )
            row = iota((STATE_ROWS, value_dim), 0)
            state_send[low_row + key_dim:low_row + message, :] = jnp.where(
                row == 0, norm, jnp.where(row == 1, top, decay)
            )

    span = place_at.depth * place_at.side
    own_at = lax.rem(ep_at, span)
    lower_half = place_at.half == 0

    def state_copy(distance, sign):
        at = lax.rem(own_at + sign * distance + span, span)
        return remote(
            state_send, state_recv.at[distance], st_send.at[distance], st_recv.at[distance],
            (place_at.half * span + at, tp_at),
        )

    low_inner = lower_half & place_at.inner
    first_inner = (place_at.depth - 1) * place_at.side

    def total_copy(stage):
        return remote(
            total_send, total_recv, tot_send.at[stage], tot_recv, place_at.beyond(stage)
        )

    def sends_to(distance):
        at = lax.rem(own_at + distance, span)
        return (own_at + distance < span) | (lower_half & (at >= first_inner))

    def takes_from(distance):
        return (own_at >= distance) | low_inner

    def u_copies(target, sender):
        place = pl.ds(pl.multiple_of(sender * own_width, own_width), own_width)
        return [
            remote(
                u_ref.at[target * share:(target + 1) * share, :], u_recv.at[:, place],
                us_send, us_recv, (ep_at, target),
            ),
            remote(
                squares_ref.at[target], squares_recv.at[sender],
                sq_send, sq_recv, (ep_at, target),
            ),
        ]

    def send_states():
        for distance in range(1, span):
            @pl.when(sends_to(distance))
            def _():
                state_copy(distance, 1).start()

    def absorb(memory_ref, max_ref, message_ref):
        for head in range(heads):
            low_row = head * message
            memory = message_ref[low_row:low_row + key_dim, :]
            extra = message_ref[low_row + key_dim:low_row + message, :]
            norm = jnp.sum(jnp.where(diagonal(), extra[0:1, :], 0.0), axis=1, keepdims=True)
            top, decay = extra[1:2, :], extra[2:3, :]
            old_top = max_ref[head, 0:1, :]
            new_top = jnp.maximum(old_top + decay, top)
            left = jnp.exp(old_top + decay - new_top)
            right = jnp.exp(top - new_top)
            memory_ref[head, :, :value_dim] = (
                left * memory_ref[head, :, :value_dim] + right * memory
            )
            memory_ref[head, :, value_dim:] = (
                left * memory_ref[head, :, value_dim:] + right * norm
            )
            max_ref[head] = jnp.broadcast_to(new_top, max_ref.shape[1:])

    def take_states():
        for distance in range(1, span):
            @pl.when(takes_from(distance))
            def _():
                state_copy(distance, 1).wait_recv()

        @pl.when(lower_half)
        def _():
            total_ref[...] = jnp.zeros_like(total_ref)
            total_max[...] = jnp.full_like(total_max, -1e30)
            for distance in range(span - 1, 0, -1):
                @pl.when(own_at >= distance)
                def _():
                    absorb(total_ref, total_max, state_recv.at[distance])
            incoming[...] = total_ref[...]
            incoming_max[...] = total_max[...]

        @pl.when(low_inner)
        def _():
            absorb(total_ref, total_max, state_send)
            for distance in range(span - 1, 0, -1):
                @pl.when(own_at < distance)
                def _():
                    absorb(total_ref, total_max, state_recv.at[distance])
            for head in range(heads):
                low_row = head * message
                total_send[low_row:low_row + key_dim, :] = total_ref[head, :, :value_dim]
                norm = jnp.sum(
                    jnp.where(diagonal(), total_ref[head, :, value_dim:], 0.0),
                    axis=0, keepdims=True,
                )
                row = iota((STATE_ROWS, value_dim), 0)
                total_send[low_row + key_dim:low_row + message, :] = jnp.where(
                    row == 0, norm, jnp.where(row == 1, total_max[head], 0.0)
                )
            for stage in range(place_at.depth):
                total_copy(stage).start()

    def take_total():
        @pl.when(jnp.logical_not(lower_half))
        def _():
            incoming[...] = jnp.zeros_like(incoming)
            incoming_max[...] = jnp.full_like(incoming_max, -1e30)
            total_copy(0).wait_recv()
            absorb(incoming, incoming_max, total_recv)
            for distance in range(span - 1, 0, -1):
                @pl.when(own_at >= distance)
                def _():
                    absorb(incoming, incoming_max, state_recv.at[distance])

    def walk(low_block, high_block):
        if low_block == 0:
            found["states"] = [
                (incoming[head], incoming_max[head, 0:1, 0:1]) for head in range(heads)
            ]
            found["columns"] = jnp.transpose(found["cumulative"])
        states, columns = found["states"], found["columns"]
        lower = iota((BLK, BLK), 0) >= iota((BLK, BLK), 1)
        ones = jnp.ones((STATE_ROWS, value_dim), F32)
        for at in range(low_block, high_block):
            squares = jnp.zeros((STATE_ROWS, BLK), F32)
            for head in range(heads):
                number = head * blocks + at
                memory, top = states[head]
                query = q_ref[at * BLK:(at + 1) * BLK, head * key_dim:(head + 1) * key_dim]
                column = columns[:, number:number + 1]
                gap = jnp.where(
                    lower, column + found["shift"][number:number + 1, :], -jnp.inf
                )
                carried = column + top
                stabilizer = jnp.maximum(carried, jnp.max(gap, axis=1, keepdims=True))
                scores = nt(query, key_block(head, at)) * scale * jnp.exp(gap - stabilizer)
                high, low = halves(scores)
                values = wide_values(head, at)
                sums = mm(high, values) + mm(low, values)
                high, low = halves(memory)
                sums = sums + (jnp.exp(carried - stabilizer) * scale) * (
                    mm(query, high) + mm(query, low)
                )
                hidden = sums[:, :value_dim] / jnp.maximum(
                    jnp.abs(sums[:, value_dim:]), jnp.exp(-stabilizer)
                )
                squares = squares + nt(ones, hidden * hidden, exact)
                place = slice(head * value_dim, (head + 1) * value_dim)
                gate = gate_ref[at * BLK:(at + 1) * BLK, place].astype(F32)
                u_ref[at * BLK:(at + 1) * BLK, place] = (
                    hidden * gain_ref[:, place] * jax.nn.sigmoid(gate)
                ).astype(BF16)
                states[head] = grow(states[head], number)
            squares_ref[at // share_blocks, at % share_blocks] = squares
            if at % share_blocks == share_blocks - 1:
                @pl.when(jnp.logical_not(place_at.inner))
                def _():
                    send_share(at // share_blocks)

    def send_share(target):
        @pl.when(tp_at != target)
        def _():
            for copy in u_copies(target, tp_at):
                copy.start()

        @pl.when(tp_at == target)
        def _():
            place = pl.ds(pl.multiple_of(tp_at * own_width, own_width), own_width)
            u_recv[:, place] = u_ref[target * share:(target + 1) * share, :]
            squares_recv[tp_at] = squares_ref[target]

    def send_u():
        @pl.when(place_at.inner)
        def _():
            for target in range(tp_count):
                send_share(target)

    def late():
        others = tp_count - 1
        region = u_recv.at[:, :others * own_width]
        remote(region, region, us_send, us_recv, place_at.proxy).wait_recv()
        region = squares_recv.at[:others]
        remote(region, region, sq_send, sq_recv, place_at.proxy).wait_recv()
        squares = squares_recv[0]
        for sender in range(1, tp_count):
            squares = squares + squares_recv[sender]
        inverse_row = lax.rsqrt(squares / (heads * tp_count * value_dim) + 1e-6)
        eye = (iota((BLK, BLK), 0) == iota((BLK, BLK), 1)).astype(F32)
        load.wait()
        width = wo.shape[1]
        for at in range(share_blocks):
            inverse = nt(eye, inverse_row[at], exact)[:, 0:1]

            @pl.loop(0, width // 512)
            def _(turn):
                place = pl.ds(pl.multiple_of(turn * 512, 512), 512)
                product = mm(u_recv[at * BLK:(at + 1) * BLK, :], wo[:, place])
                out_ref[at * BLK:(at + 1) * BLK, place] = (product * inverse).astype(BF16)

            out_copy(at).start()


    def close():
        for at in range(share_blocks):
            out_copy(at).wait()
        for distance in range(1, span):
            @pl.when(sends_to(distance))
            def _():
                state_copy(distance, 1).wait_send()

        @pl.when(low_inner)
        def _():
            for stage in range(place_at.depth):
                total_copy(stage).wait_send()

        region = u_ref.at[:(tp_count - 1) * share, :]
        remote(region, region, us_send, us_recv, place_at.proxy).wait_send()
        region = squares_ref.at[:tp_count - 1]
        remote(region, region, sq_send, sq_recv, place_at.proxy).wait_send()

    return fetch, early, send_u, send_states, take_states, take_total, walk, late, close


def settle(results):
    count = len(results)
    parts = 4

    def kernel(*refs):
        sources, targets, held = refs[:count], refs[count:2 * count], refs[2 * count:3 * count]
        in_sem, out_sem = refs[3 * count:]
        ins, outs = [], []
        for number in range(count):
            rows = held[number].shape[0] // parts
            for part in range(parts):
                place, at = slice(part * rows, (part + 1) * rows), number * parts + part
                here = held[number].at[place, :]
                ins.append(
                    pltpu.make_async_copy(sources[number].at[place, :], here, in_sem.at[at])
                )
                outs.append(
                    pltpu.make_async_copy(here, targets[number].at[place, :], out_sem.at[at])
                )
        for copy in ins:
            copy.start()
        for come, leave in zip(ins, outs):
            come.wait()
            leave.start()
        for copy in outs:
            copy.wait()

    hbm = pl.BlockSpec(memory_space=pl.ANY)
    sems = pltpu.SemaphoreType.DMA((count * parts,))
    return pl.pallas_call(
        kernel,
        out_shape=tuple(jax.ShapeDtypeStruct(array.shape, array.dtype) for array in results),
        in_specs=[hbm] * count,
        out_specs=(hbm,) * count,
        scratch_shapes=[pltpu.VMEM(array.shape, array.dtype) for array in results] + [sems, sems],
        name="settle",
    )(*results)


def on_device(
    queries,
    head_key_rows,
    head_value_rows,
    log_input_gate,
    forget_logits,
    head_forget_bias,
    extra_log_forget,
    output_gate_logits,
    head_norm_gain,
    mixer_output_weight,
    second_batch_input,
    expert_norm_gain,
    routed_expert_index,
    routed_copy_weight,
    routed_gate_weight,
    routed_up_weight,
    routed_down_weight,
    shared_gate_weight,
    shared_up_weight,
    shared_down_weight,
):
    tokens, width = second_batch_input.shape
    ep_count = lax.axis_size("ep")
    tp_count = lax.axis_size("tp")
    count = ep_count * tp_count
    top_count = routed_expert_index.shape[1]
    capacity = max(2, 3 * tokens * top_count // (2 * count))
    groups = capacity // LANE_ROWS
    step = width // PIECES
    wire = PIECES * (groups * step + step * (capacity - groups * LANE_ROWS) // LANE_ROWS)
    side = max(1, tp_count // CORES)
    near = count // 2
    span = ep_count // 2
    depth = ep_count // side // 2
    rows = near * capacity
    spots = groups + LANE_ROWS // (capacity - groups * LANE_ROWS)
    padded = -(-tokens // 128) * 128
    hidden_width = routed_gate_weight.shape[2]
    length = queries.shape[0]
    heads = head_forget_bias.shape[0]
    key_dim = queries.shape[1] // heads
    value_dim = head_value_rows.shape[1] // heads
    blocks = length // BLK
    share = length // tp_count
    dma = pltpu.SemaphoreType.DMA
    vmem = pl.BlockSpec(memory_space=pltpu.VMEM)
    hbm = pl.BlockSpec(memory_space=pl.ANY)

    block = pltpu.VMEM((tokens, width), BF16)
    meta = pltpu.VMEM((STATE_ROWS, padded), F32)
    half_slots = pltpu.VMEM((near * LANE_ROWS, wire), BF16)
    far_slots = pltpu.VMEM((depth, near * LANE_ROWS, wire), BF16)
    far_block = pltpu.VMEM((depth, tokens, width), BF16)
    slots = pltpu.VMEM((2 * near * LANE_ROWS, wire), BF16)
    moe_scratch = (
        [block, meta, far_block, pltpu.VMEM((depth, STATE_ROWS, padded), F32)]
        + [half_slots, far_slots, slots, slots, half_slots, far_slots]
        + [far_block, block]
        + [
            pltpu.VMEM(array.shape[-2:], BF16)
            for array in (
                routed_gate_weight, routed_up_weight, routed_down_weight,
                shared_gate_weight, shared_up_weight, shared_down_weight,
            )
        ]
        + [
            pltpu.VMEM((rows, width), BF16),
            pltpu.VMEM((rows, hidden_width), BF16),
            pltpu.VMEM((rows, width), BF16),
            pltpu.VMEM((rows, hidden_width), F32),
            pltpu.VMEM((rows, hidden_width), F32),
            pltpu.VMEM((tokens, width), F32),
            block,
            pltpu.VMEM((spots, 2, tokens, near * LANE_ROWS), BF16),
            block, dma,
            dma((6,)), dma, dma((PIECES,)), dma, dma((depth, PIECES)), dma, dma,
            dma((PIECES,)), dma((depth, PIECES)), dma, dma((depth, PIECES)), dma,
            dma((RESULTS,)), dma, dma((depth,)), dma((RESULTS,)),
        ]
    )
    message = heads * (key_dim + STATE_ROWS)
    mixer_scratch = [
        *[
            pltpu.VMEM(array.shape, BF16)
            for array in (queries, head_key_rows, head_value_rows, output_gate_logits)
        ],
        pltpu.VMEM((share, width), BF16), dma((4,)), dma((share // BLK,)),
        pltpu.VMEM(mixer_output_weight.shape, BF16),
        pltpu.VMEM((heads * blocks, key_dim, 2 * value_dim), F32),
        pltpu.VMEM((message, value_dim), F32),
        pltpu.VMEM((span, message, value_dim), F32),
        pltpu.VMEM((message, value_dim), F32),
        pltpu.VMEM((message, value_dim), F32),
        pltpu.VMEM((heads, key_dim, 2 * value_dim), F32),
        pltpu.VMEM((heads, STATE_ROWS, value_dim), F32),
        pltpu.VMEM((heads, key_dim, 2 * value_dim), F32),
        pltpu.VMEM((heads, STATE_ROWS, value_dim), F32),
        pltpu.VMEM((length, heads * value_dim), BF16),
        pltpu.VMEM((tp_count, share // BLK, STATE_ROWS, BLK), F32),
        pltpu.VMEM((share, tp_count * heads * value_dim), BF16),
        pltpu.VMEM((tp_count, share // BLK, STATE_ROWS, BLK), F32),
        dma, dma((span,)), dma((span,)), dma((depth,)), dma,
        dma, dma, dma, dma,
    ]

    def kernel(*refs):
        mixer_in, moe_in = refs[:10], refs[10:20]
        mixer_out, moe_out = refs[20], refs[21]
        scratch = refs[22:]
        cut = len(moe_scratch)
        place = Place(ep_count, tp_count)
        fetch, early, send_u, send_states, take_states, take_total, walk, late, close = mixer_parts(
            place, ep_count, tp_count, (*mixer_in, mixer_out, *scratch[cut:])
        )
        experts = Experts(place, capacity, (*moe_in, moe_out, *scratch[:cut]))
        depth = place.depth
        experts.open()
        fetch()
        experts.meet()
        experts.start()
        early()
        send_states()
        experts.common()
        for piece in range(PIECES):
            experts.relay(0, piece)
        experts.serve_own()
        for stage in range(depth):
            if stage + 1 < depth:
                experts.relay(stage + 1, 0)
            if stage:
                experts.mix_far(stage - 1, 0)
            experts.serve_far(stage)
            if stage + 1 < depth:
                for piece in range(1, PIECES):
                    experts.relay(stage + 1, piece)
            if stage == 0:
                experts.return_planes(place.inner)
                take_states()
        take_total()
        for piece in range(PIECES):
            walk(blocks * piece // PIECES, blocks * (piece + 1) // PIECES)
            if piece + 1 == PIECES:
                experts.return_planes(jnp.logical_not(place.inner))
            experts.mix_far(depth - 1, piece)
        send_u()
        experts.mix_own()
        late()
        experts.close()
        close()

    results = pl.pallas_call(
        kernel,
        out_shape=(
            jax.ShapeDtypeStruct((share, width), BF16),
            jax.ShapeDtypeStruct((tokens, width), BF16),
        ),
        in_specs=[hbm] * 3 + [vmem] * 4 + [hbm, vmem, hbm, hbm] + [vmem] * 3 + [hbm] * 6,
        out_specs=(hbm, hbm),
        scratch_shapes=moe_scratch + mixer_scratch,
        compiler_params=pltpu.CompilerParams(
            collective_id=0, has_side_effects=True, vmem_limit_bytes=62 * 1024 * 1024
        ),
        name="both",
    )(
        queries, head_key_rows, head_value_rows, log_input_gate.T, forget_logits.T,
        head_forget_bias[None, :], extra_log_forget.T, output_gate_logits,
        head_norm_gain[None, :], mixer_output_weight,
        second_batch_input, expert_norm_gain[None, :], routed_expert_index.T,
        routed_copy_weight.T, routed_gate_weight, routed_up_weight,
        routed_down_weight, shared_gate_weight, shared_up_weight, shared_down_weight,
    )
    return settle(results)


def solution(mesh):
    in_specs = (
        P("ep", "tp"),
        P("ep", "tp"),
        P("ep", "tp"),
        P("ep", "tp"),
        P("ep", "tp"),
        P("tp"),
        P("ep", "tp"),
        P("ep", "tp"),
        P("tp"),
        P(),
        P(("ep", "tp"), None),
        P(),
        P(("ep", "tp"), None),
        P(("ep", "tp"), None),
        P(("ep", "tp"), None, None),
        P(("ep", "tp"), None, None),
        P(("ep", "tp"), None, None),
        P(),
        P(),
        P(),
    )
    out_specs = (P(("ep", "tp"), None), P(("ep", "tp"), None))
    return jax.shard_map(
        on_device, mesh=mesh, in_specs=in_specs, out_specs=out_specs, check_vma=False
    )
```
